256 devices in a mesh: sp: 32 (over z, x), tp: 8 (over y, core).
Axes of the slice: x: 4, y: 4, z: 8, core: 2. Of those that a mesh axis runs over, the one named last changes fastest.
Arguments:
- tokens: bfloat16 [24576, 2048], P(('sp', 'tp')), may hold values from -6 to 6
- in_gain: float32 [2048], replicated, may hold values from 0.1 to 1.9
- w_query: bfloat16 [2048, 1024], P(None, 'tp'), may hold values from -0.125 to 0.125
- w_key: bfloat16 [2048, 1024], P(None, 'tp'), may hold values from -0.125 to 0.125
- w_value: bfloat16 [2048, 2048], P(None, 'tp'), may hold values from -0.125 to 0.125
- w_input_gate: bfloat16 [2048, 8], replicated, may hold values from -8 to 8
- w_forget_gate: bfloat16 [2048, 8], replicated, may hold values from -0.125 to 0.125
- forget_bias: float32 [8], replicated
- forget_extra: float32 [24576, 8], P('sp', 'tp'), may hold values from -2 to 0
- w_conv_gate: bfloat16 [2048, 2048], P(None, 'tp'), may hold values from -0.125 to 0.125
- w_conv_left: bfloat16 [2048, 2048], P(None, 'tp'), may hold values from -0.125 to 0.125
- w_conv_right: bfloat16 [2048, 2048], P(None, 'tp'), may hold values from -0.125 to 0.125
- conv_taps: float32 [3, 2048], replicated, may hold values from -3.5 to 3.5
- first_memory: float32 [8, 128, 256], P('tp'), may hold values from -5120 to 5120
- first_norm: float32 [8, 128], P('tp'), may hold values from -5120 to 5120
- w_out_memory: bfloat16 [2048, 2048], P('tp'), may hold values from -0.09375 to 0.09375
- w_out_conv: bfloat16 [2048, 2048], P('tp'), may hold values from -0.09375 to 0.09375
Outputs:
- mixed: bfloat16 [24576, 2048], P(('sp', 'tp'))
The draws below stay inside these ranges and needn't reach their ends.
All inputs are finite; a program needn't handle non-finite values.
Results may differ from the reference program's by a relative error of at most 0.015.
The reference program's roundings to bfloat16 on the way count: a program that leaves them out, or rounds other values in their place, can miss the bound.
Values may be sent and summed in bfloat16 or wider, within the bound.
A program may use at most 64 MiB of HBM per device.

```python
import math
import jax
import jax.numpy as jnp
from jax import lax

D = 2048
MEMORY_HEADS = 8
KEY_DIM = 128
VALUE_DIM = 256
CONV_CH = 2048
TAPS = 3
TOK_DEV = 768
SEQUENCE_TOKENS = 24576
QK_WIDTH = 1024
V_WIDTH = 2048
N_TP = 8


def decay_plan(key):
    base_key = jax.random.fold_in(key, 7)
    order_key, spread_key, block_key, place_key, loss_key = jax.random.split(base_key, 5)
    fast_heads = jax.random.permutation(order_key, MEMORY_HEADS) < MEMORY_HEADS // 2
    spread = jax.random.uniform(spread_key, (MEMORY_HEADS,), jnp.float32)
    head_bias = jnp.where(fast_heads, 4.0 + 1.5 * spread, math.log(SEQUENCE_TOKENS) + 1.5 + spread)
    return (head_bias, block_key, place_key, loss_key)


def draw_forget_bias(key, part):
    head_bias, block_key, place_key, loss_key = decay_plan(key)
    return head_bias.astype(jnp.float32)


def draw_forget_extra(key, part):
    head_bias, block_key, place_key, loss_key = decay_plan(key)
    head_rate = jnp.exp(-head_bias)
    factor = jax.random.uniform(block_key, (SEQUENCE_TOKENS // TOK_DEV, MEMORY_HEADS), jnp.float32, 0.0, 2.0)
    block_portion = -jnp.repeat(factor, TOK_DEV, axis=0) * head_rate[None, :]
    place_slots = jax.random.randint(place_key, (3, MEMORY_HEADS), 0, SEQUENCE_TOKENS)
    loss_values = jnp.log(jax.random.uniform(loss_key, (3, MEMORY_HEADS), jnp.float32, 0.6, 0.8))
    token_positions = jnp.arange(SEQUENCE_TOKENS, dtype=jnp.int32)
    span_total_sum = jnp.zeros((SEQUENCE_TOKENS, MEMORY_HEADS), jnp.float32)
    for token_span in range(3):
        span_total_sum = span_total_sum + jnp.where(token_positions[:, None] == place_slots[token_span][None, :], loss_values[token_span][None, :], 0.0)
    return (block_portion + span_total_sum).astype(jnp.float32)


def draw_w_input_gate(key, part):
    weights = jax.random.normal(jax.random.fold_in(key, 11), (D, MEMORY_HEADS), jnp.float32) / math.sqrt(D)
    return jnp.clip(weights, -8.0, 8.0).astype(jnp.bfloat16)


def steps_of(key, extent, cuts, least, top_value):
    loudness, own = 1.0, jax.random.fold_in(key, 6)
    for position, blocks in cuts:
        heights = jnp.exp(jax.random.uniform(jax.random.fold_in(own, position), (blocks,), jnp.float32, least / len(cuts), top_value / len(cuts)))
        loudness = loudness * jnp.repeat(heights, extent[position] // blocks).reshape([-1 if axis == position else 1 for axis in range(len(extent))])
    return loudness


def noise(own_key, shape, scale, bound, pieces=(), held_as=jnp.bfloat16):
    drawn = jax.random.normal(own_key, shape, jnp.float32) * scale
    if len(pieces) > 0:
        drawn = steps_of(own_key, shape, pieces, -0.22, 0.18) * drawn
    return jnp.clip(drawn, min=-bound, max=bound).astype(held_as)


def setup_inputs(seed: int = 0) -> dict:
    splits = jax.random.split(jax.random.key(seed), 18)
    return {
        "tokens": noise(splits[0], (SEQUENCE_TOKENS, D), 1.0, 6.0, ((0, 256),)),
        "in_gain": jnp.clip(1.0 + 0.18 * jax.random.normal(splits[1], (D,), jnp.float32), 0.1, 1.9),
        "w_query": noise(splits[2], (D, QK_WIDTH), D ** -0.5, 0.125, ((1, 8),)),
        "w_key": noise(splits[3], (D, QK_WIDTH), D ** -0.5, 0.125, ((1, 8),)),
        "w_value": noise(splits[4], (D, V_WIDTH), D ** -0.5, 0.125, ((1, 8),)),
        "w_input_gate": draw_w_input_gate(jax.random.fold_in(splits[17], 71), 0),
        "w_forget_gate": noise(splits[6], (D, MEMORY_HEADS), D ** -0.5, 0.125),
        "forget_bias": draw_forget_bias(jax.random.fold_in(splits[17], 71), 0),
        "forget_extra": draw_forget_extra(jax.random.fold_in(splits[17], 71), 0),
        "w_conv_gate": noise(splits[9], (D, CONV_CH), D ** -0.5, 0.125, ((1, 8),)),
        "w_conv_left": noise(splits[10], (D, CONV_CH), D ** -0.5, 0.125, ((1, 8),)),
        "w_conv_right": noise(splits[11], (D, CONV_CH), D ** -0.5, 0.125, ((1, 8),)),
        "conv_taps": noise(splits[12], (TAPS, CONV_CH), TAPS ** -0.5, 3.5, (), jnp.float32),
        "first_memory": noise(splits[13], (MEMORY_HEADS, KEY_DIM, VALUE_DIM), (6 * SEQUENCE_TOKENS ** 0.5), 5120.0, ((0, 8),), jnp.float32),
        "first_norm": noise(splits[14], (MEMORY_HEADS, KEY_DIM), (6 * SEQUENCE_TOKENS ** 0.5), 5120.0, ((0, 8),), jnp.float32),
        "w_out_memory": noise(splits[15], (V_WIDTH, D), (V_WIDTH + CONV_CH) ** -0.5, 0.09375, ((0, 8),)),
        "w_out_conv": noise(splits[16], (CONV_CH, D), (V_WIDTH + CONV_CH) ** -0.5, 0.09375, ((0, 8),)),
    }


epsilon = 1e-06

def rounded(values):
    return lax.optimization_barrier(values.astype(jnp.bfloat16)).astype(jnp.float32)

def mixer_block(carried_state, inputs):
    carry_max, carry_memory, carry_norm = carried_state
    query_rows, key_rows, value_rows, in_pre, log_forget = inputs
    length = query_rows.shape[0]
    query_scale = KEY_DIM ** (-0.5)
    cumulative = jnp.cumsum(log_forget, axis=0)
    decay_total = cumulative[length - 1]
    weight_log = decay_total[None, :] - cumulative + in_pre
    block_max = lax.optimization_barrier(jnp.max(weight_log, axis=0))
    keyed = key_rows.astype(jnp.float32) * jnp.exp(weight_log - block_max[None, :])[:, :, None]
    block_norm = lax.optimization_barrier(jnp.sum(keyed, axis=0))
    block_memory = jnp.einsum('shd,shv->hdv', rounded(keyed), value_rows.astype(jnp.float32))
    token_positions = jnp.arange(length, dtype=jnp.int32)
    causal = token_positions[:, None] >= token_positions[None, :]
    cum_heads = cumulative.T
    log_gap = cum_heads[:, :, None] - cum_heads[:, None, :] + in_pre.T[:, None, :]
    log_gap = jnp.where(causal[None], log_gap, -jnp.inf)
    inter_log = cum_heads + carry_max[:, None]
    row_max = jnp.maximum(inter_log, lax.optimization_barrier(jnp.max(log_gap, axis=2)))
    raw_scores = jnp.einsum('thd,shd->hts', query_rows.astype(jnp.float32), key_rows.astype(jnp.float32)) * query_scale
    mixing = raw_scores * jnp.exp(log_gap - row_max[:, :, None])
    carried = jnp.exp(inter_log - row_max).T
    scaled_query = query_rows.astype(jnp.float32) * query_scale
    from_values = jnp.einsum('hts,shv->thv', rounded(mixing), value_rows.astype(jnp.float32))
    from_memory = jnp.einsum('thd,hdv->thv', scaled_query, carry_memory, precision=lax.Precision.HIGHEST)
    from_norm = jnp.einsum('thd,hd->th', scaled_query, carry_norm, precision=lax.Precision.HIGHEST)
    numerator = from_values + carried[:, :, None] * from_memory
    denominator = lax.optimization_barrier(jnp.sum(mixing, axis=2)).T + carried * from_norm
    memory_out = numerator / jnp.maximum(jnp.abs(denominator), 1.0)[:, :, None]
    row_mean = lax.optimization_barrier(jnp.mean(memory_out * memory_out, axis=(1, 2), keepdims=True))
    heads_out = (memory_out * lax.rsqrt(row_mean + epsilon)).astype(jnp.bfloat16)
    new_max = jnp.maximum(carry_max + decay_total, block_max)
    old_scale = jnp.exp(carry_max + decay_total - new_max)
    new_scale = jnp.exp(block_max - new_max)
    new_memory = old_scale[:, None, None] * carry_memory + new_scale[:, None, None] * block_memory
    new_norm = old_scale[:, None] * carry_norm + new_scale[:, None] * block_norm
    return ((new_max, new_memory, new_norm), heads_out)

def reference(tokens, in_gain, w_query, w_key, w_value, w_input_gate, w_forget_gate, forget_bias, forget_extra, w_conv_gate, w_conv_left, w_conv_right, conv_taps, first_memory, first_norm, w_out_memory, w_out_conv):
    token_rows = tokens.astype(jnp.float32)
    scale_rows = lax.rsqrt(lax.optimization_barrier(jnp.mean(token_rows * token_rows, axis=1, keepdims=True)) + epsilon)
    normed = (token_rows * scale_rows * in_gain).astype(jnp.bfloat16)
    query_rows = jnp.dot(normed, w_query, preferred_element_type=jnp.float32).astype(jnp.bfloat16)
    key_rows = jnp.dot(normed, w_key, preferred_element_type=jnp.float32).astype(jnp.bfloat16)
    value_rows = jnp.dot(normed, w_value, preferred_element_type=jnp.float32).astype(jnp.bfloat16)
    in_pre = jnp.dot(normed, w_input_gate, preferred_element_type=jnp.float32)
    forget_pre = jnp.dot(normed, w_forget_gate, preferred_element_type=jnp.float32) + forget_bias
    log_forget = jax.nn.log_sigmoid(forget_pre) + forget_extra
    conv_gate = rounded(jnp.dot(normed, w_conv_gate, preferred_element_type=jnp.float32))
    conv_left = rounded(jnp.dot(normed, w_conv_left, preferred_element_type=jnp.float32))
    conv_right = rounded(jnp.dot(normed, w_conv_right, preferred_element_type=jnp.float32))
    product = (conv_left * conv_right).astype(jnp.bfloat16)
    padded = jnp.concatenate([jnp.zeros((TAPS - 1, CONV_CH), jnp.bfloat16), product], axis=0).astype(jnp.float32)
    filtered = conv_taps[0][None, :] * padded[0:SEQUENCE_TOKENS]
    for tap_index in range(1, TAPS):
        filtered = filtered + conv_taps[tap_index][None, :] * padded[tap_index:tap_index + SEQUENCE_TOKENS]
    conv_branch = (conv_gate * filtered).astype(jnp.bfloat16)
    blocks = SEQUENCE_TOKENS // TOK_DEV
    inputs = (query_rows.reshape(blocks, TOK_DEV, MEMORY_HEADS, KEY_DIM), key_rows.reshape(blocks, TOK_DEV, MEMORY_HEADS, KEY_DIM), value_rows.reshape(blocks, TOK_DEV, MEMORY_HEADS, VALUE_DIM), in_pre.reshape(blocks, TOK_DEV, MEMORY_HEADS), log_forget.reshape(blocks, TOK_DEV, MEMORY_HEADS))
    start_state = (jnp.zeros((MEMORY_HEADS,), jnp.float32), first_memory, first_norm)
    final_state, heads_out = lax.scan(mixer_block, start_state, inputs)
    heads_out = heads_out.reshape(SEQUENCE_TOKENS, V_WIDTH)
    head_group = V_WIDTH // N_TP
    channel_group = CONV_CH // N_TP
    mixed = jnp.zeros((SEQUENCE_TOKENS, D), jnp.float32)
    for group in range(N_TP):
        head_lo = group * head_group
        channel_lo = group * channel_group
        partial_value = jnp.dot(heads_out[:, head_lo:head_lo + head_group], w_out_memory[head_lo:head_lo + head_group], preferred_element_type=jnp.float32)
        partial_value = partial_value + jnp.dot(conv_branch[:, channel_lo:channel_lo + channel_group], w_out_conv[channel_lo:channel_lo + channel_group], preferred_element_type=jnp.float32)
        mixed = mixed + rounded(partial_value)
    return mixed.astype(jnp.bfloat16)
```

```python
import functools

import jax
import jax.numpy as jnp
from jax import lax
from jax.experimental import pallas as pl
from jax.experimental.pallas import tpu as pltpu
from jax.sharding import PartitionSpec as P

D = 2048
KEY = 128
VAL = 256
CH = 256
ROWS = 96
HALF = 48
BLK = 768
NTP = 8
TILES = 32
COLS = 1024
EPS = 1e-06
SCALE = KEY ** (-0.5)
MESH = pl.DeviceIdType.MESH
f32 = jnp.float32
bf16 = jnp.bfloat16


def nt_dot(a, b):
    return lax.dot_general(a, b, (((1,), (1,)), ((), ())), preferred_element_type=f32)


def tn_dot(a, b):
    return lax.dot_general(a, b, (((0,), (0,)), ((), ())), preferred_element_type=f32)


def dot(a, b):
    return jnp.dot(a, b, preferred_element_type=f32)


def kernel(
    n_sp,
    tok, gain, wi, wf, bias, fextra, taps, fmem, fnorm,
    wq, wk, wv, wcg, wcl, wcr, wom, woc,
    out,
    x, w_all, wg, wom_v, woc_v,
    proj, gates, urow, cmcol, st, rv, aux, cv, cr, mh, nh, cmem, pv, rs,
    mob, cbr, prod, eb, er, ss, scol,
    pb_c, x_c, fs_c, fr_c, gs_c, gr_c,
    pb_h, x_h, fs_h, fr_h, gs_h, gr_h,
    wsem, ag_s, ag_r, aux_s, aux_r, st_s, st_r, cr_s, cr_r, ed_s, ed_r, ss_s, ss_r,
    rc_s, rc_r, rh_s, rh_r,
):
    tpd = TILES // n_sp
    sp = lax.axis_index("sp")
    me = lax.axis_index("tp")
    y = me // 2
    c = lax.rem(me, 2)
    sib = me + 1 - 2 * c
    yn_y, yp_y, yo_y = lax.rem(y + 1, 4), lax.rem(y + 3, 4), lax.rem(y + 2, 4)
    yn, yp, yo = yn_y * 2 + c, yp_y * 2 + c, yo_y * 2 + c

    def to(peer):
        return (sp, peer)

    def sp_peer(k):
        return lax.rem(sp + k, n_sp)

    weights = [
        pltpu.make_async_copy(src, dst, wsem.at[i])
        for i, (src, dst) in enumerate(
            [
                (wk, w_all.at[:, pl.ds(0, 128)]),
                (wq, w_all.at[:, pl.ds(128, 128)]),
                (wv, w_all.at[:, pl.ds(256, 256)]),
                (wcl, w_all.at[:, pl.ds(512, 256)]),
                (wcr, w_all.at[:, pl.ds(768, 256)]),
                (wcg, w_all.at[:, pl.ds(1024, 256)]),
                (woc, woc_v),
                (wom, wom_v),
            ]
        )
    ]
    barrier = pltpu.get_barrier_semaphore()
    for k in range(1, NTP):
        pl.semaphore_signal(
            barrier, inc=1, device_id=(sp, lax.rem(me + k, NTP)), device_id_type=MESH
        )

    def greet(k, _):
        pl.semaphore_signal(barrier, inc=1, device_id=(sp_peer(k), me), device_id_type=MESH)
        return 0

    lax.fori_loop(1, n_sp, greet, 0)
    for w in weights:
        w.start()

    def block(idx, h, n):
        return x.at[pl.ds(pl.multiple_of(idx * ROWS + h * HALF, 16), n), :]

    t = tok[...].astype(f32)
    scale = lax.rsqrt(jnp.mean(t * t, axis=1, keepdims=True) + EPS)
    x[pl.ds(pl.multiple_of(me * ROWS, 16), ROWS), :] = (t * scale * gain[...]).astype(bf16)
    pl.semaphore_wait(barrier, NTP - 1 + n_sp - 1)

    sends = []

    def send(src, dst, ssem, rsem, peer):
        cp = pltpu.make_async_remote_copy(
            src_ref=src, dst_ref=dst, send_sem=ssem, recv_sem=rsem,
            device_id=to(peer), device_id_type=MESH,
        )
        cp.start()
        sends.append(cp)

    def got(dst, rsem):
        pltpu.make_async_remote_copy(
            src_ref=dst, dst_ref=dst, send_sem=rsem, recv_sem=rsem,
            device_id=to(sib), device_id_type=MESH,
        ).wait_recv()

    def ag(idx, h, n, k, peer):
        ref = block(idx, h, n)
        send(ref, ref, ag_s.at[k], ag_r.at[k], peer)

    ag(me, 0, HALF, 0, yn)
    ag(me, 1, HALF, 3, yp)
    ag(me, 1, HALF, 1, yn)
    ag(me, 0, HALF, 4, yp)
    ag(me, 0, ROWS, 6, sib)

    gw = jnp.concatenate(
        [wi[...].astype(f32), wf[...].astype(f32), jnp.zeros((112, D), f32)], axis=0
    )
    wg[...] = gw.T.astype(bf16)
    for i in range(6):
        weights[i].wait()

    def project(yy, lo, hi, with_gates):
        rows = pl.ds(pl.multiple_of(yy * 192, 64), 192)

        def step(i, _):
            cols = pl.ds(pl.multiple_of(i * 256, 256), 256)
            proj[rows, cols] = dot(x[rows, :], w_all[:, cols]).astype(bf16)
            return 0

        if with_gates:
            gates[rows, :] = dot(x[rows, :], wg[...])
        lax.fori_loop(lo, hi, step, 0)

    other = 1 - c
    got(block(sib, 0, ROWS), ag_r.at[6])
    project(y, 0, 5, True)
    got(block(yp, 0, HALF), ag_r.at[0])
    ag(yp, 0, HALF, 2, yn)
    ag(yp, 0, HALF, 7, sib)
    got(block(yn, 1, HALF), ag_r.at[3])
    ag(yn, 1, HALF, 5, yp)
    ag(yn, 1, HALF, 9, sib)
    got(block(yp, 1, HALF), ag_r.at[1])
    ag(yp, 1, HALF, 8, sib)
    got(block(yn, 0, HALF), ag_r.at[4])
    ag(yn, 0, HALF, 10, sib)
    got(block(yp_y * 2 + other, 0, HALF), ag_r.at[7])
    got(block(yp_y * 2 + other, 1, HALF), ag_r.at[8])
    project(yp_y, 0, 5, True)
    got(block(yn_y * 2 + other, 1, HALF), ag_r.at[9])
    got(block(yn_y * 2 + other, 0, HALF), ag_r.at[10])
    project(yn_y, 0, 5, True)
    got(block(yo, 0, HALF), ag_r.at[2])
    ag(yo, 0, HALF, 11, sib)
    got(block(yo, 1, HALF), ag_r.at[5])
    ag(yo, 1, HALF, 12, sib)
    got(block(yo_y * 2 + other, 0, HALF), ag_r.at[11])
    got(block(yo_y * 2 + other, 1, HALF), ag_r.at[12])
    project(yo_y, 0, 2, True)

    g_t = gates[...].T
    sub = lax.broadcasted_iota(jnp.int32, (8, BLK), 0)
    lane = lax.broadcasted_iota(jnp.int32, (8, BLK), 1)
    in_row = jnp.sum(jnp.where(sub == me, g_t[0:8], 0.0), axis=0, keepdims=True)
    f_row = jnp.sum(jnp.where(sub == me, g_t[8:16], 0.0), axis=0, keepdims=True)
    f_row = f_row + bias[me]
    log_forget = jnp.minimum(f_row, 0.0) - jnp.log1p(jnp.exp(-jnp.abs(f_row))) + fextra[...]
    cum = jnp.broadcast_to(log_forget, (8, BLK))
    for s in (1, 2, 4, 8, 16, 32, 64, 128, 256, 512):
        cum = cum + jnp.where(lane >= s, pltpu.roll(cum, s, 1), 0.0)
    u = in_row - cum
    top = u
    for s in (1, 2, 4, 8, 16, 32, 64, 128, 256, 512):
        top = jnp.maximum(top, jnp.where(lane >= s, pltpu.roll(top, s, 1), -jnp.inf))
    u_max = jnp.max(u, axis=1, keepdims=True)
    decay = jnp.sum(jnp.where(lane == BLK - 1, cum, 0.0), axis=1, keepdims=True)
    ew = jnp.exp(u - u_max)
    urow[...] = u
    cols = jnp.concatenate(
        [jnp.where(sub == 0, top, ew), jnp.zeros((120, BLK), f32)], axis=0
    ).T
    cmcol[...] = jnp.broadcast_to(cols[:, 0:1], (BLK, 128))
    keyed = proj[:, 0:128].astype(f32) * cols[:, 1:2]
    block_norm = jnp.sum(keyed, axis=0, keepdims=True)
    mem = tn_dot(keyed.astype(bf16), proj[:, 256:512])
    for p in range(TILES):
        i, j = p // 2, p % 2
        st[p // tpd, p % tpd] = mem[8 * i : 8 * i + 8, 128 * j : 128 * j + 128]
    d_lanes = jnp.broadcast_to(decay[0:1], (1, 128))
    m_lanes = jnp.broadcast_to(decay[0:1] + u_max[0:1], (1, 128))
    aux[sp] = jnp.concatenate([d_lanes, m_lanes, block_norm], axis=1)

    def state_copies(k):
        p = sp_peer(k)
        one = pltpu.make_async_remote_copy(
            src_ref=aux.at[sp], dst_ref=aux.at[sp], send_sem=aux_s, recv_sem=aux_r,
            device_id=(p, me), device_id_type=MESH,
        )
        two = pltpu.make_async_remote_copy(
            src_ref=st.at[p], dst_ref=rv.at[sp], send_sem=st_s, recv_sem=st_r,
            device_id=(p, me), device_id_type=MESH,
        )
        return one, two

    def send_state(k, _):
        for cp in state_copies(k):
            cp.start()
        return 0

    lax.fori_loop(1, n_sp, send_state, 0)
    rv[sp] = st[sp]

    project(yo_y, 2, 5, False)
    product = (proj[:, 512:768].astype(f32) * proj[:, 768:1024].astype(f32)).astype(bf16)
    eb[...] = product[BLK - 16 :]
    nxt = lax.rem(sp + 1, n_sp)
    edge = pltpu.make_async_remote_copy(
        src_ref=eb, dst_ref=er, send_sem=ed_s, recv_sem=ed_r,
        device_id=(nxt, me), device_id_type=MESH,
    )
    edge.start()
    prod[8:, :] = product.astype(f32)
    edge.wait_recv()
    prod[0:8, :] = jnp.where(sp > 0, er[...].astype(f32)[8:16], 0.0)
    mine = pl.ds(pl.multiple_of(me * CH, CH), CH)
    filtered = taps[0:1, mine] * prod[6 : 6 + BLK, :]
    filtered = filtered + taps[1:2, mine] * prod[7 : 7 + BLK, :]
    filtered = filtered + taps[2:3, mine] * prod[8 : 8 + BLK, :]
    cbr[...] = (proj[:, 1024:1280].astype(f32) * filtered).astype(bf16)

    def own(d):
        return pl.ds(pl.multiple_of((d * 2 + c) * ROWS, 16), ROWS)

    def his(d):
        return pl.ds(pl.multiple_of((d * 2 + 1 - c) * ROWS, 16), ROWS)

    def rs_start(a, wv_, pb, xb, fs, fr, gs, gr, s_, r_):
        for n, d in ((0, yo_y), (1, yn_y), (2, yp_y), (3, y)):
            rows = pl.ds(pl.multiple_of(d * 192, 64), 192)

            def step(i, _, rows=rows):
                cs = pl.ds(pl.multiple_of(i * 512, 512), 512)
                pb[rows, cs] = dot(a[rows, :], wv_[:, cs]).astype(bf16)
                return 0

            lax.fori_loop(0, 4, step, 0)
            send(pb.at[his(d)], xb.at[d], s_.at[n], r_.at[n], sib)
            if n == 1:
                got(xb.at[yo_y], r_.at[0])
                tot = pb[own(yo_y), :].astype(f32) + xb[yo_y].astype(f32)
                fs[0] = tot[:, :COLS].astype(bf16)
                fs[1] = tot[:, COLS:].astype(bf16)
                send(fs.at[0], fr.at[0], s_.at[4], r_.at[4], yn)
                send(fs.at[1], fr.at[1], s_.at[5], r_.at[5], yp)
        got(xb.at[yn_y], r_.at[1])
        tot = pb[own(yn_y), COLS:].astype(f32) + xb[yn_y, :, COLS:].astype(f32)
        gs[1] = tot.astype(bf16)
        send(gs.at[1], gr.at[1], s_.at[7], r_.at[7], yn)
        got(xb.at[yp_y], r_.at[2])
        tot = pb[own(yp_y), :COLS].astype(f32) + xb[yp_y, :, :COLS].astype(f32)
        gs[2] = tot.astype(bf16)
        send(gs.at[2], gr.at[2], s_.at[8], r_.at[8], yp)

    def rs_mid(a, wv_, pb, xb, fs, fr, gs, gr, s_, r_):
        got(fr.at[0], r_.at[4])
        tot = pb[own(yn_y), :COLS].astype(f32) + xb[yn_y, :, :COLS].astype(f32)
        gs[0] = (tot + fr[0].astype(f32)).astype(bf16)
        send(gs.at[0], gr.at[0], s_.at[6], r_.at[6], yn)
        got(fr.at[1], r_.at[5])
        tot = pb[own(yp_y), COLS:].astype(f32) + xb[yp_y, :, COLS:].astype(f32)
        gs[3] = (tot + fr[1].astype(f32)).astype(bf16)
        send(gs.at[3], gr.at[3], s_.at[9], r_.at[9], yp)

    def rs_end(a, wv_, pb, xb, fs, fr, gs, gr, s_, r_):
        got(xb.at[y], r_.at[3])
        for k in range(4):
            got(gr.at[k], r_.at[6 + k])

        def half(k):
            cs = pl.ds(k * COLS, COLS)
            own_sum = pb[own(y), cs].astype(f32) + xb[y, :, cs].astype(f32)
            return own_sum + gr[k].astype(f32) + gr[2 + k].astype(f32)

        return half

    conv_set = (cbr, woc_v, pb_c, x_c, fs_c, fr_c, gs_c, gr_c, rc_s, rc_r)
    head_set = (mob, wom_v, pb_h, x_h, fs_h, fr_h, gs_h, gr_h, rh_s, rh_r)
    weights[6].wait()
    weights[7].wait()
    rs_start(*conv_set)

    for rb in range(3):
        r0 = rb * 256
        q = proj[r0 : r0 + 256, 128:256]
        cm = cmcol[r0 : r0 + 256, 0:1]
        acc = jnp.zeros((256, VAL), f32)
        tot = jnp.zeros((256, 1), f32)
        for cb in range(rb + 1):
            c0 = cb * 256
            mix = nt_dot(q, proj[c0 : c0 + 256, 0:128]) * SCALE
            mix = mix * jnp.exp(urow[0:1, c0 : c0 + 256] - cm)
            if cb == rb:
                ri = lax.broadcasted_iota(jnp.int32, (256, 256), 0)
                ci = lax.broadcasted_iota(jnp.int32, (256, 256), 1)
                mix = jnp.where(ri >= ci, mix, 0.0)
            tot = tot + jnp.sum(mix, axis=1, keepdims=True)
            acc = acc + dot(mix.astype(bf16), proj[c0 : c0 + 256, 256:512])
        pv[r0 : r0 + 256, :] = acc
        rs[r0 : r0 + 256, :] = jnp.broadcast_to(tot, (256, 128))

    rest = pl.ds(0, n_sp - 1)
    got(aux.at[rest], aux_r)
    got(rv.at[rest], st_r)
    first = []
    for k in range(tpd):
        p = sp * tpd + k
        r_i = pl.ds(pl.multiple_of((p // 2) * 8, 8), 8)
        c_i = pl.ds(pl.multiple_of(lax.rem(p, 2) * 128, 128), 128)
        first.append(fmem[r_i, c_i])
    run_m = jnp.zeros((1, 128), f32)
    run_n = fnorm[...]
    for b in range(n_sp):
        for k in range(tpd):
            cv[b, k] = first[k]
        mh[b] = run_m
        nh[b] = run_n
        if b < n_sp - 1:
            row = aux[b]
            new_m = jnp.maximum(run_m + row[:, 0:128], row[:, 128:256])
            old = jnp.exp(run_m + row[:, 0:128] - new_m)
            new = jnp.exp(row[:, 128:256] - new_m)
            first = [old * first[k] + new * rv[b, k] for k in range(tpd)]
            run_n = old * run_n + new * row[:, 256:384]
            run_m = new_m

    def carry_copy(k):
        p = sp_peer(k)
        return pltpu.make_async_remote_copy(
            src_ref=cv.at[p], dst_ref=cr.at[sp], send_sem=cr_s, recv_sem=cr_r,
            device_id=(p, me), device_id_type=MESH,
        )

    def send_carry(k, _):
        carry_copy(k).start()
        return 0

    lax.fori_loop(1, n_sp, send_carry, 0)
    cr[sp] = cv[sp]
    rs_mid(*conv_set)

    got(cr.at[rest], cr_r)
    for p in range(TILES):
        i, j = p // 2, p % 2
        cmem[8 * i : 8 * i + 8, 128 * j : 128 * j + 128] = cr[p // tpd, p % tpd]
    carry = cmem[...]
    high = carry.astype(bf16)
    low = (carry - high.astype(f32)).astype(bf16)
    m_in = mh[sp][:, 0:1]
    n_in = nh[sp]
    n_1 = n_in.astype(bf16).astype(f32)
    n_2 = (n_in - n_1).astype(bf16).astype(f32)
    n_3 = n_in - n_1 - n_2
    sub16 = lax.broadcasted_iota(jnp.int32, (16, 128), 0)
    n_rows = jnp.where(
        sub16 == 0, n_1, jnp.where(sub16 == 1, n_2, jnp.where(sub16 == 2, n_3, 0.0))
    ).astype(bf16)
    squares = []
    for rb in range(3):
        r0 = rb * 256
        q = proj[r0 : r0 + 256, 128:256]
        cm = cmcol[r0 : r0 + 256, 0:1]
        peak = jnp.maximum(cm, m_in)
        f_in = jnp.exp(cm - peak)
        f_carry = jnp.exp(m_in - peak)
        from_memory = (dot(q, high) + dot(q, low)) * SCALE
        from_norm = jnp.sum(nt_dot(q, n_rows), axis=1, keepdims=True) * SCALE
        num = f_in * pv[r0 : r0 + 256, :] + f_carry * from_memory
        den = f_in * rs[r0 : r0 + 256, 0:1] + f_carry * from_norm
        memory_out = num / jnp.maximum(jnp.abs(den), 1.0)
        squares.append(jnp.sum(memory_out * memory_out, axis=1, keepdims=True))
        mob[r0 : r0 + 256, :] = memory_out.astype(bf16)
    sq = jnp.broadcast_to(jnp.concatenate(squares, axis=0), (BLK, 128)).T
    ss[me] = sq[0:1]
    for k in range(1, NTP):
        peer = lax.rem(me + k, NTP)
        send(ss.at[me], ss.at[me], ss_s.at[k], ss_r.at[k], peer)
    rs_start(*head_set)
    rs_mid(*head_set)
    for k in range(1, NTP):
        got(ss.at[lax.rem(me + NTP - k, NTP)], ss_r.at[k])
    total = ss[0]
    for k in range(1, NTP):
        total = total + ss[k]
    factor = lax.rsqrt(total / (NTP * VAL) + EPS)
    scol[...] = jnp.broadcast_to(factor, (128, BLK)).T
    conv_half = rs_end(*conv_set)
    head_half = rs_end(*head_set)
    factor = scol[pl.ds(pl.multiple_of(me * ROWS, 8), ROWS), 0:1]
    for k in range(2):
        cs = slice(k * COLS, (k + 1) * COLS)
        out[:, cs] = (factor * head_half(k) + conv_half(k)).astype(bf16)

    for cp in sends:
        cp.wait_send()
    edge.wait_send()

    def sent(ref, sem):
        pltpu.make_async_remote_copy(
            src_ref=ref, dst_ref=ref, send_sem=sem, recv_sem=sem,
            device_id=to(sib), device_id_type=MESH,
        ).wait_send()

    sent(aux.at[rest], aux_s)
    sent(st.at[rest], st_s)
    sent(cv.at[rest], cr_s)


def solution(mesh):
    n_sp = mesh.shape["sp"]
    tpd = TILES // n_sp
    vmem = pl.BlockSpec(memory_space=pltpu.VMEM)
    smem = pl.BlockSpec(memory_space=pltpu.SMEM)
    hbm = pl.BlockSpec(memory_space=pl.ANY)
    dma = pltpu.SemaphoreType.DMA

    def rs_bufs():
        return [
            pltpu.VMEM((BLK, D), bf16),
            pltpu.VMEM((4, ROWS, D), bf16),
            pltpu.VMEM((2, ROWS, COLS), bf16),
            pltpu.VMEM((2, ROWS, COLS), bf16),
            pltpu.VMEM((4, ROWS, COLS), bf16),
            pltpu.VMEM((4, ROWS, COLS), bf16),
        ]

    scratch = [
        pltpu.VMEM((BLK, D), bf16),
        pltpu.VMEM((D, 1280), bf16),
        pltpu.VMEM((D, 128), bf16),
        pltpu.VMEM((VAL, D), bf16),
        pltpu.VMEM((CH, D), bf16),
        pltpu.VMEM((BLK, 1280), bf16),
        pltpu.VMEM((BLK, 128), f32),
        pltpu.VMEM((8, BLK), f32),
        pltpu.VMEM((BLK, 128), f32),
        pltpu.VMEM((n_sp, tpd, 8, 128), f32),
        pltpu.VMEM((n_sp, tpd, 8, 128), f32),
        pltpu.VMEM((n_sp, 1, 384), f32),
        pltpu.VMEM((n_sp, tpd, 8, 128), f32),
        pltpu.VMEM((n_sp, tpd, 8, 128), f32),
        pltpu.VMEM((n_sp, 1, 128), f32),
        pltpu.VMEM((n_sp, 1, 128), f32),
        pltpu.VMEM((KEY, VAL), f32),
        pltpu.VMEM((BLK, VAL), f32),
        pltpu.VMEM((BLK, 128), f32),
        pltpu.VMEM((BLK, VAL), bf16),
        pltpu.VMEM((BLK, CH), bf16),
        pltpu.VMEM((BLK + 8, CH), f32),
        pltpu.VMEM((16, CH), bf16),
        pltpu.VMEM((16, CH), bf16),
        pltpu.VMEM((NTP, 1, BLK), f32),
        pltpu.VMEM((BLK, 128), f32),
        *rs_bufs(),
        *rs_bufs(),
        dma((8,)),
        dma((13,)),
        dma((13,)),
        dma(()),
        dma(()),
        dma(()),
        dma(()),
        dma(()),
        dma(()),
        dma(()),
        dma(()),
        dma((NTP,)),
        dma((NTP,)),
        dma((10,)),
        dma((10,)),
        dma((10,)),
        dma((10,)),
    ]

    def per_device(
        tokens, in_gain, w_query, w_key, w_value, w_input_gate, w_forget_gate, forget_bias,
        forget_extra, w_conv_gate, w_conv_left, w_conv_right, conv_taps, first_memory,
        first_norm, w_out_memory, w_out_conv,
    ):
        return pl.pallas_call(
            functools.partial(kernel, n_sp),
            out_shape=jax.ShapeDtypeStruct((ROWS, D), bf16),
            in_specs=[vmem] * 4 + [smem] + [vmem] * 4 + [hbm] * 8,
            out_specs=vmem,
            scratch_shapes=scratch,
            compiler_params=pltpu.CompilerParams(
                collective_id=0, has_side_effects=True, vmem_limit_bytes=60 * 1024 * 1024
            ),
        )(
            tokens, in_gain.reshape(1, D), w_input_gate.T, w_forget_gate.T, forget_bias,
            forget_extra.reshape(1, BLK), conv_taps, first_memory.reshape(KEY, VAL), first_norm,
            w_query, w_key, w_value, w_conv_gate, w_conv_left, w_conv_right,
            w_out_memory, w_out_conv,
        )

    placed = (
        P(("sp", "tp"), None),
        P(),
        P(None, "tp"),
        P(None, "tp"),
        P(None, "tp"),
        P(),
        P(),
        P(),
        P("sp", "tp"),
        P(None, "tp"),
        P(None, "tp"),
        P(None, "tp"),
        P(),
        P("tp", None, None),
        P("tp", None),
        P("tp", None),
        P("tp", None),
    )
    return jax.shard_map(
        per_device, mesh=mesh, in_specs=placed, out_specs=P(("sp", "tp"), None), check_vma=False
    )
```

```python
import functools

import jax
import jax.numpy as jnp
from jax import lax
from jax.experimental import pallas as pl
from jax.experimental.pallas import tpu as pltpu
from jax.sharding import PartitionSpec as P

D = 2048
KEY = 128
VAL = 256
CH = 256
ROWS = 96
HALF = 48
BLK = 768
NTP = 8
TILES = 32
COLS = 1024
EPS = 1e-06
SCALE = KEY ** (-0.5)
MESH = pl.DeviceIdType.MESH
f32 = jnp.float32
bf16 = jnp.bfloat16


def nt_dot(a, b):
    return lax.dot_general(a, b, (((1,), (1,)), ((), ())), preferred_element_type=f32)


def dot(a, b):
    return jnp.dot(a, b, preferred_element_type=f32)


def kernel(
    n_sp,
    tok_h, gain_h, wi_h, wf_h, bias_h, fextra_h, taps_h, fmem_h, fnorm_h,
    wq, wk, wv, wcg, wcl, wcr, wom, woc,
    out,
    tok, gain, wi, wf, bias, fextra, taps, fmem, fnorm,
    x, w_all, wom_v, woc_v,
    proj, gates, urow, cmcol, st, rv, aux, cv, cr, mh, nh, cmem, pv, rs,
    mob, cbr, prod, eb, er, ss, scol, sqcol, fin,
    pb_c, x_c, fs_c, fr_c, gs_c, gr_c,
    pb_h, x_h, fs_h, fr_h, gs_h, gr_h,
    wsem, isem, ag_s, ag_r, aux_s, aux_r, st_s, st_r, cr_s, cr_r, ed_s, ed_r, ss_s, ss_r,
    rc_s, rc_r, rh_s, rh_r,
):
    tpd = TILES // n_sp
    scope = jax.named_scope
    sp = lax.axis_index("sp")
    me = lax.axis_index("tp")
    y = me // 2
    c = lax.rem(me, 2)
    sib = me + 1 - 2 * c
    yn_y, yp_y, yo_y = lax.rem(y + 1, 4), lax.rem(y + 3, 4), lax.rem(y + 2, 4)
    yn, yp = yn_y * 2 + c, yp_y * 2 + c

    def sp_peer(k):
        return lax.rem(sp + k, n_sp)

    inputs = [
        pltpu.make_async_copy(src, dst, isem.at[i])
        for i, (src, dst) in enumerate(
            [
                (tok_h, tok), (gain_h, gain), (wi_h, wi), (wf_h, wf), (bias_h, bias),
                (fextra_h, fextra), (taps_h, taps), (fmem_h, fmem), (fnorm_h, fnorm),
            ]
        )
    ]
    weights = [
        pltpu.make_async_copy(src, dst, wsem.at[i])
        for i, (src, dst) in enumerate(
            [
                (wk, w_all.at[:, pl.ds(0, 128)]),
                (wq, w_all.at[:, pl.ds(128, 128)]),
                (wv, w_all.at[:, pl.ds(256, 256)]),
                (wcl, w_all.at[:, pl.ds(512, 256)]),
                (wcr, w_all.at[:, pl.ds(768, 256)]),
                (wcg, w_all.at[:, pl.ds(1024, 256)]),
                (woc, woc_v),
                (wom, wom_v),
            ]
        )
    ]
    for cp in inputs[:4]:
        cp.start()
    barrier = pltpu.get_barrier_semaphore()
    for k in range(1, NTP):
        pl.semaphore_signal(
            barrier, inc=1, device_id=(sp, lax.rem(me + k, NTP)), device_id_type=MESH
        )

    def greet(k, _):
        pl.semaphore_signal(barrier, inc=1, device_id=(sp_peer(k), me), device_id_type=MESH)
        return 0

    lax.fori_loop(1, n_sp, greet, 0)
    for cp in inputs[4:]:
        cp.start()
    for w in weights:
        w.start()

    def slots(s, n=1):
        return x.at[pl.ds(pl.multiple_of(s * HALF, 16), n * HALF), :]

    with scope("norm"):
        inputs[0].wait()
        inputs[1].wait()
        t = tok[...].astype(f32)
        scale = lax.rsqrt(jnp.mean(t * t, axis=1, keepdims=True) + EPS)
        x[pl.ds(pl.multiple_of(c * ROWS, 16), ROWS), :] = (t * scale * gain[...]).astype(bf16)
    with scope("w_barrier"):
        pl.semaphore_wait(barrier, NTP - 1 + n_sp - 1)

    sends = []

    def send(src, dst, ssem, rsem, peer):
        cp = pltpu.make_async_remote_copy(
            src_ref=src, dst_ref=dst, send_sem=ssem, recv_sem=rsem,
            device_id=(sp, peer), device_id_type=MESH,
        )
        cp.start()
        sends.append(cp)

    def got(dst, rsem, name="w"):
        with scope(name):
            pltpu.make_async_remote_copy(
                src_ref=dst, dst_ref=dst, send_sem=rsem, recv_sem=rsem,
                device_id=(sp, sib), device_id_type=MESH,
            ).wait_recv()

    def ag(src, dst, k, peer, n=1):
        send(slots(src, n), slots(dst, n), ag_s.at[k], ag_r.at[k], peer)

    other = 1 - c
    ag(2 * c, 4 + c, 0, yn)
    ag(2 * c + 1, 6 + c, 3, yp)
    ag(2 * c + 1, 8 + c, 1, yn)
    ag(2 * c, 10 + c, 4, yp)
    ag(2 * c, 2 * c, 6, sib, 2)

    inputs[2].wait()
    inputs[3].wait()
    gw = jnp.concatenate(
        [wi[...].astype(f32), wf[...].astype(f32), jnp.zeros((112, D), f32)], axis=0
    )
    w_all[:, 1280:1408] = gw.T.astype(bf16)
    with scope("w_weights"):
        for i in range(6):
            weights[i].wait()

    def project(stage, bases, parts):
        xs = x[stage * 192 : stage * 192 + 192, :]
        for lo, hi in parts:
            res = dot(xs, w_all[:, lo:hi])
            for k, base in enumerate(bases):
                rows = pl.ds(pl.multiple_of(base, 16), HALF)
                piece = res[k * HALF : (k + 1) * HALF]
                if hi <= 1280:
                    proj[rows, lo:hi] = piece.astype(bf16)
                else:
                    gates[rows, :] = piece[:, 1280 - lo :]
                    if lo < 1280:
                        proj[rows, lo:1280] = piece[:, : 1280 - lo].astype(bf16)

    every = ((0, 512), (512, 1024), (1024, 1408))
    got(slots(2 * other, 2), ag_r.at[6], "w_ag6")
    with scope("proj_0"):
        project(0, [y * 192 + HALF * k for k in range(4)], every)
    got(slots(4 + c), ag_r.at[0], "w_ag0")
    ag(4 + c, 12 + c, 2, yn)
    ag(4 + c, 4 + c, 7, sib)
    got(slots(6 + c), ag_r.at[3], "w_ag3")
    ag(6 + c, 14 + c, 5, yp)
    ag(6 + c, 6 + c, 8, sib)
    got(slots(4 + other), ag_r.at[7], "w_ag7")
    got(slots(6 + other), ag_r.at[8], "w_ag8")
    with scope("proj_1"):
        project(
            1,
            [yp_y * 192, yp_y * 192 + ROWS, yn_y * 192 + HALF, yn_y * 192 + ROWS + HALF],
            every,
        )
    got(slots(8 + c), ag_r.at[1], "w_ag1")
    ag(8 + c, 8 + c, 9, sib)
    got(slots(10 + c), ag_r.at[4], "w_ag4")
    ag(10 + c, 10 + c, 10, sib)
    got(slots(8 + other), ag_r.at[9], "w_ag9")
    got(slots(10 + other), ag_r.at[10], "w_ag10")
    with scope("proj_2"):
        project(
            2,
            [yp_y * 192 + HALF, yp_y * 192 + ROWS + HALF, yn_y * 192, yn_y * 192 + ROWS],
            every,
        )
    got(slots(12 + c), ag_r.at[2], "w_ag2")
    ag(12 + c, 12 + c, 11, sib)
    got(slots(14 + c), ag_r.at[5], "w_ag5")
    ag(14 + c, 14 + c, 12, sib)
    got(slots(12 + other), ag_r.at[11], "w_ag11")
    got(slots(14 + other), ag_r.at[12], "w_ag12")
    last = [yo_y * 192, yo_y * 192 + ROWS, yo_y * 192 + HALF, yo_y * 192 + ROWS + HALF]
    with scope("proj_3"):
        project(3, last, ((1280, 1408), (0, 512)))

    for cp in inputs[4:]:
        cp.wait()
    with scope("state"):
        g_t = gates[...].T
        sub = lax.broadcasted_iota(jnp.int32, (8, BLK), 0)
        lane = lax.broadcasted_iota(jnp.int32, (8, BLK), 1)
        in_row = jnp.sum(jnp.where(sub == me, g_t[0:8], 0.0), axis=0, keepdims=True)
        f_row = jnp.sum(jnp.where(sub == me, g_t[8:16], 0.0), axis=0, keepdims=True)
        lane8 = lax.broadcasted_iota(jnp.int32, (1, NTP), 1)
        f_row = f_row + jnp.sum(jnp.where(lane8 == me, bias[...], 0.0), axis=1, keepdims=True)
        log_forget = (
            jnp.minimum(f_row, 0.0) - jnp.log1p(jnp.exp(-jnp.abs(f_row))) + fextra[...]
        )

        def stacked(row):
            parts = [row[:, 128 * k : 128 * k + 128] for k in range(6)]
            return jnp.concatenate(parts + [jnp.zeros((2, 128), f32)], axis=0)

        lf6 = stacked(log_forget)
        l_1 = lf6.astype(bf16).astype(f32)
        l_2 = (lf6 - l_1).astype(bf16).astype(f32)
        l_3 = lf6 - l_1 - l_2
        upto = lax.broadcasted_iota(jnp.int32, (128, 128), 0) <= lax.broadcasted_iota(
            jnp.int32, (128, 128), 1
        )
        sums = dot(
            jnp.concatenate([l_1, l_2, l_3, jnp.zeros((8, 128), f32)], axis=0).astype(bf16),
            jnp.where(upto, 1.0, 0.0).astype(bf16),
        )
        inside = sums[0:8] + sums[8:16] + sums[16:24]
        sub8 = lax.broadcasted_iota(jnp.int32, (8, 128), 0)
        ends = jnp.broadcast_to(inside[:, 127:128], (8, 128))
        before = jnp.where(sub8 >= 1, pltpu.roll(ends, 1, 0), 0.0)
        for s in (1, 2, 4):
            before = before + jnp.where(sub8 >= s, pltpu.roll(before, s, 0), 0.0)
        cum6 = inside + before
        u6 = jnp.where(sub8 < 6, stacked(in_row) - cum6, -jnp.inf)
        u_max = jnp.max(jnp.max(u6, axis=1, keepdims=True), axis=0, keepdims=True)
        decay = cum6[5:6, 127:128]

        def unstacked(a):
            return jnp.concatenate([a[k : k + 1] for k in range(6)], axis=1)

        u_row = unstacked(u6)
        k_t = proj[:, 0:128].astype(f32).T
        keyed = k_t * jnp.exp(u_row - u_max)
        mem = dot(keyed.astype(bf16), proj[:, 256:512])
        norm_col = jnp.sum(keyed, axis=1, keepdims=True)
        block_norm = jnp.broadcast_to(norm_col, (128, 128)).T[0:1]
        d_lanes = jnp.broadcast_to(decay, (1, 128))
        m_lanes = jnp.broadcast_to(decay + u_max, (1, 128))
        aux[sp] = jnp.concatenate([d_lanes, m_lanes, block_norm], axis=1)
        for p in range(TILES):
            i, j = p // 2, p % 2
            st[p // tpd, p % tpd] = mem[8 * i : 8 * i + 8, 128 * j : 128 * j + 128]

    def over_peers(start):
        half = n_sp // 2
        start(half)

        def both(i, _):
            start(half + i)
            start(half - i)
            return 0

        lax.fori_loop(1, half, both, 0)

    def start_state(k):
        p = sp_peer(k)
        pltpu.make_async_remote_copy(
            src_ref=st.at[p], dst_ref=rv.at[sp], send_sem=st_s, recv_sem=st_r,
            device_id=(p, me), device_id_type=MESH,
        ).start()
        pltpu.make_async_remote_copy(
            src_ref=aux.at[sp], dst_ref=aux.at[sp], send_sem=aux_s, recv_sem=aux_r,
            device_id=(p, me), device_id_type=MESH,
        ).start()

    with scope("send_state"):
        over_peers(start_state)
    rv[sp] = st[sp]

    with scope("proj_lr"):
        project(3, last, ((512, 1024),))
        product = (proj[:, 512:768].astype(f32) * proj[:, 768:1024].astype(f32)).astype(bf16)
        eb[...] = product[BLK - 16 :]
        prod[8:, :] = product.astype(f32)
    edge = pltpu.make_async_remote_copy(
        src_ref=eb, dst_ref=er, send_sem=ed_s, recv_sem=ed_r,
        device_id=(sp_peer(1), me), device_id_type=MESH,
    )
    edge.start()
    with scope("proj_g"):
        project(3, last, ((1024, 1280),))

    with scope("mixing"):
        top = jnp.broadcast_to(u_row, (8, BLK))
        urow[...] = top
        for s in (1, 2, 4, 8, 16, 32, 64, 128, 256, 512):
            top = jnp.maximum(top, jnp.where(lane >= s, pltpu.roll(top, s, 1), -jnp.inf))
        cols = jnp.concatenate([top, jnp.zeros((120, BLK), f32)], axis=0).T
        cmcol[...] = jnp.broadcast_to(cols[:, 0:1], (BLK, 128))
        for rb in range(3):
            r0 = rb * 256
            q = proj[r0 : r0 + 256, 128:256]
            cm = cmcol[r0 : r0 + 256, 0:1]
            acc = jnp.zeros((256, VAL), f32)
            tot = jnp.zeros((256, 1), f32)
            for cb in range(rb + 1):
                c0 = cb * 256
                mix = nt_dot(q, proj[c0 : c0 + 256, 0:128]) * SCALE
                mix = mix * jnp.exp(urow[0:1, c0 : c0 + 256] - cm)
                if cb == rb:
                    ri = lax.broadcasted_iota(jnp.int32, (256, 256), 0)
                    ci = lax.broadcasted_iota(jnp.int32, (256, 256), 1)
                    mix = jnp.where(ri >= ci, mix, 0.0)
                tot = tot + jnp.sum(mix, axis=1, keepdims=True)
                acc = acc + dot(mix.astype(bf16), proj[c0 : c0 + 256, 256:512])
            pv[r0 : r0 + 256, :] = acc
            rs[r0 : r0 + 256, :] = jnp.broadcast_to(tot, (256, 128))

    with scope("w_edge"):
        edge.wait_recv()
    with scope("filter"):
        prod[0:8, :] = jnp.where(sp > 0, er[...].astype(f32)[8:16], 0.0)
        mine = pl.ds(pl.multiple_of(me * CH, CH), CH)
        filtered = taps[0:1, mine] * prod[6 : 6 + BLK, :]
        filtered = filtered + taps[1:2, mine] * prod[7 : 7 + BLK, :]
        filtered = filtered + taps[2:3, mine] * prod[8 : 8 + BLK, :]
        cbr[...] = (proj[:, 1024:1280].astype(f32) * filtered).astype(bf16)

    def own(d):
        return pl.ds(pl.multiple_of((d * 2 + c) * ROWS, 16), ROWS)

    def his(d):
        return pl.ds(pl.multiple_of((d * 2 + 1 - c) * ROWS, 16), ROWS)

    def rs_start(a, wv_, pb, xb, fs, fr, gs, gr, s_, r_, prepare=None):
        for n, d in ((0, yo_y), (1, yn_y), (2, yp_y), (3, y)):
            rows = pl.ds(pl.multiple_of(d * 192, 64), 192)
            if prepare is not None:
                prepare(rows)
            for lo in range(0, D, COLS):
                pb[rows, lo : lo + COLS] = dot(a[rows, :], wv_[:, lo : lo + COLS]).astype(bf16)
            send(pb.at[his(d)], xb.at[d], s_.at[n], r_.at[n], sib)
            if n == 1:
                got(xb.at[yo_y], r_.at[0], "w_x0")
                tot = pb[own(yo_y), :].astype(f32) + xb[yo_y].astype(f32)
                fs[0] = tot[:, :COLS].astype(bf16)
                fs[1] = tot[:, COLS:].astype(bf16)
                send(fs.at[0], fr.at[0], s_.at[4], r_.at[4], yn)
                send(fs.at[1], fr.at[1], s_.at[5], r_.at[5], yp)
        got(xb.at[yn_y], r_.at[1], "w_x1")
        tot = pb[own(yn_y), COLS:].astype(f32) + xb[yn_y, :, COLS:].astype(f32)
        gs[1] = tot.astype(bf16)
        send(gs.at[1], gr.at[1], s_.at[7], r_.at[7], yn)
        got(xb.at[yp_y], r_.at[2], "w_x2")
        tot = pb[own(yp_y), :COLS].astype(f32) + xb[yp_y, :, :COLS].astype(f32)
        gs[2] = tot.astype(bf16)
        send(gs.at[2], gr.at[2], s_.at[8], r_.at[8], yp)

    def rs_mid(a, wv_, pb, xb, fs, fr, gs, gr, s_, r_):
        got(fr.at[0], r_.at[4], "w_f0")
        tot = pb[own(yn_y), :COLS].astype(f32) + xb[yn_y, :, :COLS].astype(f32)
        gs[0] = (tot + fr[0].astype(f32)).astype(bf16)
        send(gs.at[0], gr.at[0], s_.at[6], r_.at[6], yn)
        got(fr.at[1], r_.at[5], "w_f1")
        tot = pb[own(yp_y), COLS:].astype(f32) + xb[yp_y, :, COLS:].astype(f32)
        gs[3] = (tot + fr[1].astype(f32)).astype(bf16)
        send(gs.at[3], gr.at[3], s_.at[9], r_.at[9], yp)

    def here(pb, xb, cs):
        return pb[own(y), cs].astype(f32) + xb[y, :, cs].astype(f32)

    conv_set = (cbr, woc_v, pb_c, x_c, fs_c, fr_c, gs_c, gr_c, rc_s, rc_r)
    head_set = (mob, wom_v, pb_h, x_h, fs_h, fr_h, gs_h, gr_h, rh_s, rh_r)
    weights[6].wait()
    weights[7].wait()
    with scope("rs_start_conv"):
        rs_start(*conv_set)

    rest = pl.ds(0, n_sp - 1)
    got(aux.at[rest], aux_r, "w_aux")
    got(rv.at[rest], st_r, "w_state")
    first = []
    for k in range(tpd):
        p = sp * tpd + k
        r_i = pl.ds(pl.multiple_of((p // 2) * 8, 8), 8)
        c_i = pl.ds(pl.multiple_of(lax.rem(p, 2) * 128, 128), 128)
        first.append(fmem[r_i, c_i])
    run_m = jnp.zeros((1, 128), f32)
    run_n = fnorm[...]
    for b in range(n_sp):
        for k in range(tpd):
            cv[b, k] = first[k]
        mh[b] = run_m
        nh[b] = run_n
        if b < n_sp - 1:
            row = aux[b]
            new_m = jnp.maximum(run_m + row[:, 0:128], row[:, 128:256])
            old = jnp.exp(run_m + row[:, 0:128] - new_m)
            new = jnp.exp(row[:, 128:256] - new_m)
            first = [old * first[k] + new * rv[b, k] for k in range(tpd)]
            run_n = old * run_n + new * row[:, 256:384]
            run_m = new_m

    def start_carry(k):
        p = sp_peer(k)
        pltpu.make_async_remote_copy(
            src_ref=cv.at[p], dst_ref=cr.at[sp], send_sem=cr_s, recv_sem=cr_r,
            device_id=(p, me), device_id_type=MESH,
        ).start()

    with scope("send_carry"):
        over_peers(start_carry)
    cr[sp] = cv[sp]
    with scope("rs_mid_conv"):
        rs_mid(*conv_set)

    got(cr.at[rest], cr_r, "w_carry")
    with scope("carry"):
        for p in range(TILES):
            i, j = p // 2, p % 2
            cmem[8 * i : 8 * i + 8, 128 * j : 128 * j + 128] = cr[p // tpd, p % tpd]
        carry = cmem[...]
        high = carry.astype(bf16)
        low = (carry - high.astype(f32)).astype(bf16)
        m_in = mh[sp][:, 0:1]
        n_in = nh[sp]
        n_1 = n_in.astype(bf16).astype(f32)
        n_2 = (n_in - n_1).astype(bf16).astype(f32)
        n_3 = n_in - n_1 - n_2
        sub16 = lax.broadcasted_iota(jnp.int32, (16, 128), 0)
        n_rows = jnp.where(
            sub16 == 0, n_1, jnp.where(sub16 == 1, n_2, jnp.where(sub16 == 2, n_3, 0.0))
        ).astype(bf16)

    def heads(rows):
        q = proj[rows, 128:256]
        cm = cmcol[rows, 0:1]
        peak = jnp.maximum(cm, m_in)
        f_in = jnp.exp(cm - peak)
        f_carry = jnp.exp(m_in - peak)
        from_memory = (dot(q, high) + dot(q, low)) * SCALE
        from_norm = jnp.sum(nt_dot(q, n_rows), axis=1, keepdims=True) * SCALE
        num = f_in * pv[rows, :] + f_carry * from_memory
        den = f_in * rs[rows, 0:1] + f_carry * from_norm
        memory_out = num / jnp.maximum(jnp.abs(den), 1.0)
        squares = jnp.sum(memory_out * memory_out, axis=1, keepdims=True)
        sqcol[rows, :] = jnp.broadcast_to(squares, (192, 128))
        mob[rows, :] = memory_out.astype(bf16)

    with scope("rs_start_head"):
        rs_start(*head_set, prepare=heads)
    ss[me] = sqcol[...].T[0:1]
    for k in range(1, NTP):
        send(ss.at[me], ss.at[me], ss_s.at[k], ss_r.at[k], lax.rem(me + k, NTP))
    with scope("rs_mid_head"):
        rs_mid(*head_set)
    for k in range(1, NTP):
        got(ss.at[lax.rem(me + NTP - k, NTP)], ss_r.at[k], "w_ss")
    total = ss[0]
    for k in range(1, NTP):
        total = total + ss[k]
    factor = lax.rsqrt(total / (NTP * VAL) + EPS)
    scol[...] = jnp.broadcast_to(factor, (128, BLK)).T
    got(x_c.at[y], rc_r.at[3])
    for k in range(4):
        got(gr_c.at[k], rc_r.at[6 + k], "w_gc")
    got(x_h.at[y], rh_r.at[3])
    factor = scol[pl.ds(pl.multiple_of(me * ROWS, 8), ROWS), 0:1]
    for k in range(2):
        cs = slice(k * COLS, (k + 1) * COLS)
        conv_sum = here(pb_c, x_c, cs) + gr_c[k].astype(f32) + gr_c[2 + k].astype(f32)
        fin[:, cs] = conv_sum + factor * here(pb_h, x_h, cs)
    for k in (1, 2, 0, 3):
        got(gr_h.at[k], rh_r.at[6 + k], "w_gh")
    with scope("final"):
        for k in range(2):
            cs = slice(k * COLS, (k + 1) * COLS)
            rest_sum = gr_h[k].astype(f32) + gr_h[2 + k].astype(f32)
            out[:, cs] = (fin[:, cs] + factor * rest_sum).astype(bf16)

    for cp in sends:
        cp.wait_send()
    edge.wait_send()

    def sent(ref, sem):
        pltpu.make_async_remote_copy(
            src_ref=ref, dst_ref=ref, send_sem=sem, recv_sem=sem,
            device_id=(sp, sib), device_id_type=MESH,
        ).wait_send()

    sent(aux.at[rest], aux_s)
    sent(st.at[rest], st_s)
    sent(cv.at[rest], cr_s)


def solution(mesh):
    n_sp = mesh.shape["sp"]
    tpd = TILES // n_sp
    vmem = pl.BlockSpec(memory_space=pltpu.VMEM)
    hbm = pl.BlockSpec(memory_space=pl.ANY)
    dma = pltpu.SemaphoreType.DMA

    def rs_bufs():
        return [
            pltpu.VMEM((BLK, D), bf16),
            pltpu.VMEM((4, ROWS, D), bf16),
            pltpu.VMEM((2, ROWS, COLS), bf16),
            pltpu.VMEM((2, ROWS, COLS), bf16),
            pltpu.VMEM((4, ROWS, COLS), bf16),
            pltpu.VMEM((4, ROWS, COLS), bf16),
        ]

    scratch = [
        pltpu.VMEM((ROWS, D), bf16),
        pltpu.VMEM((1, D), f32),
        pltpu.VMEM((NTP, D), bf16),
        pltpu.VMEM((NTP, D), bf16),
        pltpu.VMEM((1, NTP), f32),
        pltpu.VMEM((1, BLK), f32),
        pltpu.VMEM((3, NTP * CH), f32),
        pltpu.VMEM((KEY, VAL), f32),
        pltpu.VMEM((1, KEY), f32),
        pltpu.VMEM((BLK, D), bf16),
        pltpu.VMEM((D, 1408), bf16),
        pltpu.VMEM((VAL, D), bf16),
        pltpu.VMEM((CH, D), bf16),
        pltpu.VMEM((BLK, 1280), bf16),
        pltpu.VMEM((BLK, 128), f32),
        pltpu.VMEM((8, BLK), f32),
        pltpu.VMEM((BLK, 128), f32),
        pltpu.VMEM((n_sp, tpd, 8, 128), f32),
        pltpu.VMEM((n_sp, tpd, 8, 128), f32),
        pltpu.VMEM((n_sp, 1, 384), f32),
        pltpu.VMEM((n_sp, tpd, 8, 128), f32),
        pltpu.VMEM((n_sp, tpd, 8, 128), f32),
        pltpu.VMEM((n_sp, 1, 128), f32),
        pltpu.VMEM((n_sp, 1, 128), f32),
        pltpu.VMEM((KEY, VAL), f32),
        pltpu.VMEM((BLK, VAL), f32),
        pltpu.VMEM((BLK, 128), f32),
        pltpu.VMEM((BLK, VAL), bf16),
        pltpu.VMEM((BLK, CH), bf16),
        pltpu.VMEM((BLK + 8, CH), f32),
        pltpu.VMEM((16, CH), bf16),
        pltpu.VMEM((16, CH), bf16),
        pltpu.VMEM((NTP, 1, BLK), f32),
        pltpu.VMEM((BLK, 128), f32),
        pltpu.VMEM((BLK, 128), f32),
        pltpu.VMEM((ROWS, D), f32),
        *rs_bufs(),
        *rs_bufs(),
        dma((8,)),
        dma((9,)),
        dma((13,)),
        dma((13,)),
        dma(()),
        dma(()),
        dma(()),
        dma(()),
        dma(()),
        dma(()),
        dma(()),
        dma(()),
        dma((NTP,)),
        dma((NTP,)),
        dma((10,)),
        dma((10,)),
        dma((10,)),
        dma((10,)),
    ]

    def per_device(
        tokens, in_gain, w_query, w_key, w_value, w_input_gate, w_forget_gate, forget_bias,
        forget_extra, w_conv_gate, w_conv_left, w_conv_right, conv_taps, first_memory,
        first_norm, w_out_memory, w_out_conv,
    ):
        return pl.pallas_call(
            functools.partial(kernel, n_sp),
            out_shape=jax.ShapeDtypeStruct((ROWS, D), bf16),
            in_specs=[hbm] * 17,
            out_specs=vmem,
            scratch_shapes=scratch,
            compiler_params=pltpu.CompilerParams(
                collective_id=0, has_side_effects=True, vmem_limit_bytes=60 * 1024 * 1024
            ),
        )(
            tokens, in_gain.reshape(1, D), w_input_gate.T, w_forget_gate.T,
            forget_bias.reshape(1, NTP),
            forget_extra.reshape(1, BLK), conv_taps, first_memory.reshape(KEY, VAL), first_norm,
            w_query, w_key, w_value, w_conv_gate, w_conv_left, w_conv_right,
            w_out_memory, w_out_conv,
        )

    placed = (
        P(("sp", "tp"), None),
        P(),
        P(None, "tp"),
        P(None, "tp"),
        P(None, "tp"),
        P(),
        P(),
        P(),
        P("sp", "tp"),
        P(None, "tp"),
        P(None, "tp"),
        P(None, "tp"),
        P(),
        P("tp", None, None),
        P("tp", None),
        P("tp", None),
        P("tp", None),
    )
    return jax.shard_map(
        per_device, mesh=mesh, in_specs=placed, out_specs=P(("sp", "tp"), None), check_vma=False
    )
```

```python
import functools

import jax
import jax.numpy as jnp
from jax import lax
from jax.experimental import pallas as pl
from jax.experimental.pallas import tpu as pltpu
from jax.sharding import PartitionSpec as P

D = 2048
KEY = 128
VAL = 256
CH = 256
ROWS = 96
HALF = 48
BLK = 768
NTP = 8
TILES = 32
COLS = 1024
EPS = 1e-06
SCALE = KEY ** (-0.5)
MESH = pl.DeviceIdType.MESH
f32 = jnp.float32
bf16 = jnp.bfloat16


def nt_dot(a, b):
    return lax.dot_general(a, b, (((1,), (1,)), ((), ())), preferred_element_type=f32)


def groups_of(n_sp):
    if n_sp == 32:
        return ((0, 8), (8, 16), (16, 32))
    if n_sp == 4:
        return ((0, 2), (2, 4))
    return ((0, n_sp),)


def dot(a, b):
    return jnp.dot(a, b, preferred_element_type=f32)


def kernel(
    n_sp,
    tok_h, gain_h, wi_h, wf_h, bias_h, fextra_h, taps_h, fmem_h, fnorm_h,
    wq, wk, wv, wcg, wcl, wcr, wom, woc,
    out,
    tok, gain, wi, wf, bias, fextra, taps, fmem, fnorm,
    x, w_all, wom_v, woc_v,
    proj, gates, urow, cmcol, st, rv, aux, cv, cr, mh, nh, m_at, n_at,
    ex, ea, px, pa, cmem, pv, rs,
    mob, cbr, prod, eb, er, ss, scol, sqcol, fin,
    pb_c, x_c, fs_c, fr_c, gs_c, gr_c,
    pb_h, x_h, fs_h, fr_h, gs_h, gr_h,
    wsem, isem, ag_s, ag_r, aux_s, aux_r, st_s, st_r, cr_s, cr_r, ed_s, ed_r, ss_s, ss_r,
    rc_s, rc_r, rh_s, rh_r, ex_s, px_r, ea_s, pa_r, ready, ready_edge,
):
    groups = groups_of(n_sp)
    scope = jax.named_scope
    sp = lax.axis_index("sp")
    me = lax.axis_index("tp")
    y = me // 2
    c = lax.rem(me, 2)
    sib = me + 1 - 2 * c
    yn_y, yp_y, yo_y = lax.rem(y + 1, 4), lax.rem(y + 3, 4), lax.rem(y + 2, 4)
    yn, yp = yn_y * 2 + c, yp_y * 2 + c

    def in_group(g):
        return jnp.logical_and(sp >= groups[g][0], sp < groups[g][1])

    def mates(g, start):
        lo, hi = groups[g]
        n = hi - lo
        for k in range(1, n):
            far = n // 2 + (k // 2 if k % 2 else -(k // 2))
            start(lo + lax.rem(sp - lo + far, n))

    def following(g):
        lo, hi = groups[g]
        if g + 1 == len(groups):
            return []
        at, end = groups[g + 1]
        ratio = (end - at) // (hi - lo)
        return [at + (sp - lo) * ratio + q for q in range(ratio)]

    def preceding(g):
        lo, hi = groups[g]
        at, end = groups[g - 1]
        return at + (sp - lo) // ((hi - lo) // (end - at))

    inputs = [
        pltpu.make_async_copy(src, dst, isem.at[i])
        for i, (src, dst) in enumerate(
            [
                (tok_h, tok), (gain_h, gain), (wi_h, wi), (wf_h, wf), (bias_h, bias),
                (fextra_h, fextra), (taps_h, taps), (fmem_h, fmem), (fnorm_h, fnorm),
            ]
        )
    ]
    weights = [
        pltpu.make_async_copy(src, dst, wsem.at[i])
        for i, (src, dst) in enumerate(
            [
                (wk, w_all.at[:, pl.ds(0, 128)]),
                (wq, w_all.at[:, pl.ds(128, 128)]),
                (wv, w_all.at[:, pl.ds(256, 256)]),
                (wcl, w_all.at[:, pl.ds(512, 256)]),
                (wcr, w_all.at[:, pl.ds(768, 256)]),
                (wcg, w_all.at[:, pl.ds(1024, 256)]),
                (woc, woc_v),
                (wom, wom_v),
            ]
        )
    ]
    for cp in inputs[:4]:
        cp.start()
    barrier = pltpu.get_barrier_semaphore()
    for k in range(1, NTP):
        pl.semaphore_signal(
            barrier, inc=1, device_id=(sp, lax.rem(me + k, NTP)), device_id_type=MESH
        )

    def greet(p):
        pl.semaphore_signal(barrier, inc=1, device_id=(p, me), device_id_type=MESH)

    for g, (lo, hi) in enumerate(groups):

        @pl.when(in_group(g))
        def _(g=g):
            mates(g, greet)
            for p in following(g):
                greet(p)

        if hi < n_sp:

            @pl.when(sp == hi - 1)
            def _():
                greet(sp + 1)

    for cp in inputs[4:]:
        cp.start()
    for w in weights:
        w.start()

    def slots(s, n=1):
        return x.at[pl.ds(pl.multiple_of(s * HALF, 16), n * HALF), :]

    with scope("norm"):
        inputs[0].wait()
        inputs[1].wait()
        t = tok[...].astype(f32)
        scale = lax.rsqrt(jnp.mean(t * t, axis=1, keepdims=True) + EPS)
        x[pl.ds(pl.multiple_of(c * ROWS, 16), ROWS), :] = (t * scale * gain[...]).astype(bf16)
    prod[0:8, :] = jnp.zeros((8, CH), f32)

    with scope("w_barrier"):
        for g, (lo, hi) in enumerate(groups):
            count = NTP - 1 + hi - lo - 1 + (1 if lo else 0)

            @pl.when(jnp.logical_and(in_group(g), jnp.logical_or(sp != lo, lo == 0)))
            def _(count=count):
                pl.semaphore_wait(barrier, count)

            if lo:

                @pl.when(sp == lo)
                def _(count=count):
                    pl.semaphore_wait(barrier, count + 1)

    sends = []

    def send(src, dst, ssem, rsem, peer):
        cp = pltpu.make_async_remote_copy(
            src_ref=src, dst_ref=dst, send_sem=ssem, recv_sem=rsem,
            device_id=(sp, peer), device_id_type=MESH,
        )
        cp.start()
        sends.append(cp)

    def got(dst, rsem, name="w"):
        with scope(name):
            pltpu.make_async_remote_copy(
                src_ref=dst, dst_ref=dst, send_sem=rsem, recv_sem=rsem,
                device_id=(sp, sib), device_id_type=MESH,
            ).wait_recv()

    def ag(src, dst, k, peer, n=1):
        send(slots(src, n), slots(dst, n), ag_s.at[k], ag_r.at[k], peer)

    other = 1 - c
    ag(2 * c, 4 + c, 0, yn)
    ag(2 * c + 1, 6 + c, 3, yp)
    ag(2 * c + 1, 8 + c, 1, yn)
    ag(2 * c, 10 + c, 4, yp)
    ag(2 * c, 2 * c, 6, sib, 2)
    def tell(sem, p):
        pl.semaphore_signal(sem, inc=1, device_id=(p, me), device_id_type=MESH)

    for g, (lo, hi) in enumerate(groups):
        if lo:

            @pl.when(in_group(g))
            def _(g=g):
                tell(ready, preceding(g))

            @pl.when(sp == lo)
            def _():
                tell(ready_edge, sp - 1)

    inputs[2].wait()
    inputs[3].wait()
    gw = jnp.concatenate(
        [wi[...].astype(f32), wf[...].astype(f32), jnp.zeros((112, D), f32)], axis=0
    )
    w_all[:, 1280:1408] = gw.T.astype(bf16)
    with scope("w_weights"):
        for i in range(6):
            weights[i].wait()

    def project(stage, bases, parts):
        xs = x[stage * 192 : stage * 192 + 192, :]
        for lo, hi in parts:
            res = dot(xs, w_all[:, lo:hi])
            for k, base in enumerate(bases):
                rows = pl.ds(pl.multiple_of(base, 16), HALF)
                piece = res[k * HALF : (k + 1) * HALF]
                if lo == 512:
                    left = piece[:, :CH].astype(bf16).astype(f32)
                    right = piece[:, CH:].astype(bf16).astype(f32)
                    at = pl.ds(pl.multiple_of(base + 8, 8), HALF)
                    prod[at, :] = (left * right).astype(bf16).astype(f32)
                elif hi <= 1280:
                    proj[rows, lo:hi] = piece.astype(bf16)
                else:
                    gates[rows, :] = piece[:, 1280 - lo :]
                    if lo < 1280:
                        proj[rows, lo:1280] = piece[:, : 1280 - lo].astype(bf16)

    edge = pltpu.make_async_remote_copy(
        src_ref=eb, dst_ref=er, send_sem=ed_s, recv_sem=ed_r,
        device_id=(lax.rem(sp + 1, n_sp), me), device_id_type=MESH,
    )

    def send_edge(where):
        @pl.when(jnp.logical_and(y == where, sp < n_sp - 1))
        def _():
            eb[...] = prod[BLK - 8 :, :].astype(bf16)
            for lo, hi in groups[:-1]:

                @pl.when(sp == hi - 1)
                def _():
                    pl.semaphore_wait(ready_edge, 1)

            edge.start()

    every = ((0, 512), (512, 1024), (1024, 1408))
    got(slots(2 * other, 2), ag_r.at[6], "w_ag6")
    with scope("proj_0"):
        project(0, [y * 192 + HALF * k for k in range(4)], every)
        send_edge(3)
    got(slots(4 + c), ag_r.at[0], "w_ag0")
    ag(4 + c, 12 + c, 2, yn)
    ag(4 + c, 4 + c, 7, sib)
    got(slots(6 + c), ag_r.at[3], "w_ag3")
    ag(6 + c, 14 + c, 5, yp)
    ag(6 + c, 6 + c, 8, sib)
    got(slots(4 + other), ag_r.at[7], "w_ag7")
    got(slots(6 + other), ag_r.at[8], "w_ag8")
    with scope("proj_1"):
        project(
            1,
            [yp_y * 192, yp_y * 192 + ROWS, yn_y * 192 + HALF, yn_y * 192 + ROWS + HALF],
            every,
        )
        send_edge(2)
    got(slots(8 + c), ag_r.at[1], "w_ag1")
    ag(8 + c, 8 + c, 9, sib)
    got(slots(10 + c), ag_r.at[4], "w_ag4")
    ag(10 + c, 10 + c, 10, sib)
    got(slots(8 + other), ag_r.at[9], "w_ag9")
    got(slots(10 + other), ag_r.at[10], "w_ag10")
    with scope("proj_2"):
        project(
            2,
            [yp_y * 192 + HALF, yp_y * 192 + ROWS + HALF, yn_y * 192, yn_y * 192 + ROWS],
            every,
        )
        send_edge(0)
    got(slots(12 + c), ag_r.at[2], "w_ag2")
    ag(12 + c, 12 + c, 11, sib)
    got(slots(14 + c), ag_r.at[5], "w_ag5")
    ag(14 + c, 14 + c, 12, sib)
    got(slots(12 + other), ag_r.at[11], "w_ag11")
    got(slots(14 + other), ag_r.at[12], "w_ag12")
    last = [yo_y * 192, yo_y * 192 + ROWS, yo_y * 192 + HALF, yo_y * 192 + ROWS + HALF]
    with scope("proj_3"):
        project(3, last, ((1280, 1408), (0, 512)))

    for cp in inputs[4:]:
        cp.wait()
    with scope("state"):
        g_t = gates[...].T
        sub = lax.broadcasted_iota(jnp.int32, (8, BLK), 0)
        lane = lax.broadcasted_iota(jnp.int32, (8, BLK), 1)
        in_row = jnp.sum(jnp.where(sub == me, g_t[0:8], 0.0), axis=0, keepdims=True)
        f_row = jnp.sum(jnp.where(sub == me, g_t[8:16], 0.0), axis=0, keepdims=True)
        lane8 = lax.broadcasted_iota(jnp.int32, (1, NTP), 1)
        f_row = f_row + jnp.sum(jnp.where(lane8 == me, bias[...], 0.0), axis=1, keepdims=True)
        log_forget = (
            jnp.minimum(f_row, 0.0) - jnp.log1p(jnp.exp(-jnp.abs(f_row))) + fextra[...]
        )

        def stacked(row):
            parts = [row[:, 128 * k : 128 * k + 128] for k in range(6)]
            return jnp.concatenate(parts + [jnp.zeros((2, 128), f32)], axis=0)

        lf6 = stacked(log_forget)
        l_1 = lf6.astype(bf16).astype(f32)
        l_2 = (lf6 - l_1).astype(bf16).astype(f32)
        l_3 = lf6 - l_1 - l_2
        upto = lax.broadcasted_iota(jnp.int32, (128, 128), 0) <= lax.broadcasted_iota(
            jnp.int32, (128, 128), 1
        )
        sums = dot(
            jnp.concatenate([l_1, l_2, l_3, jnp.zeros((8, 128), f32)], axis=0).astype(bf16),
            jnp.where(upto, 1.0, 0.0).astype(bf16),
        )
        inside = sums[0:8] + sums[8:16] + sums[16:24]
        sub8 = lax.broadcasted_iota(jnp.int32, (8, 128), 0)
        ends = jnp.broadcast_to(inside[:, 127:128], (8, 128))
        before = jnp.where(sub8 >= 1, pltpu.roll(ends, 1, 0), 0.0)
        for s in (1, 2, 4):
            before = before + jnp.where(sub8 >= s, pltpu.roll(before, s, 0), 0.0)
        cum6 = inside + before
        u6 = jnp.where(sub8 < 6, stacked(in_row) - cum6, -jnp.inf)
        u_max = jnp.max(jnp.max(u6, axis=1, keepdims=True), axis=0, keepdims=True)
        decay = cum6[5:6, 127:128]

        def unstacked(a):
            return jnp.concatenate([a[k : k + 1] for k in range(6)], axis=1)

        u_row = unstacked(u6)
        k_t = proj[:, 0:128].astype(f32).T
        keyed = k_t * jnp.exp(u_row - u_max)
        mem = dot(keyed.astype(bf16), proj[:, 256:512])
        norm_col = jnp.sum(keyed, axis=1, keepdims=True)
        block_norm = jnp.broadcast_to(norm_col, (128, 128)).T[0:1]
        d_lanes = jnp.broadcast_to(decay, (1, 128))
        m_lanes = jnp.broadcast_to(decay + u_max, (1, 128))
        aux[sp] = jnp.concatenate([d_lanes, m_lanes, block_norm], axis=1)
        for p in range(TILES):
            i, j = p // 2, p % 2
            st[p] = mem[8 * i : 8 * i + 8, 128 * j : 128 * j + 128]

    def start_state(g, p):
        lo, hi = groups[g]
        n = TILES // (hi - lo)
        pltpu.make_async_remote_copy(
            src_ref=st.at[pl.ds((p - lo) * n, n)], dst_ref=rv.at[sp - lo, pl.ds(0, n)],
            send_sem=st_s, recv_sem=st_r, device_id=(p, me), device_id_type=MESH,
        ).start()
        pltpu.make_async_remote_copy(
            src_ref=aux.at[sp], dst_ref=aux.at[sp], send_sem=aux_s, recv_sem=aux_r,
            device_id=(p, me), device_id_type=MESH,
        ).start()

    with scope("send_state"):
        for g, (lo, hi) in enumerate(groups):

            @pl.when(in_group(g))
            def _(g=g, lo=lo, hi=hi):
                mates(g, functools.partial(start_state, g))
                n = TILES // (hi - lo)
                for k in range(n):
                    rv[sp - lo, k] = st[(sp - lo) * n + k]

    with scope("proj_lrg"):
        project(3, last, ((512, 1024),))
        send_edge(1)
        project(3, last, ((1024, 1280),))

    def own(d):
        return pl.ds(pl.multiple_of((d * 2 + c) * ROWS, 16), ROWS)

    def his(d):
        return pl.ds(pl.multiple_of((d * 2 + 1 - c) * ROWS, 16), ROWS)

    def rs_rows(n, d, a, wv_, pb, xb, s_, r_, prepare):
        rows = pl.ds(pl.multiple_of(d * 192, 64), 192)
        prepare(n, d)
        for lo in range(0, D, COLS):
            pb[rows, lo : lo + COLS] = dot(a[rows, :], wv_[:, lo : lo + COLS]).astype(bf16)
        send(pb.at[his(d)], xb.at[d], s_.at[n], r_.at[n], sib)

    def rs_first(a, wv_, pb, xb, fs, fr, gs, gr, s_, r_, prepare):
        rs_rows(0, yo_y, a, wv_, pb, xb, s_, r_, prepare)
        rs_rows(1, yn_y, a, wv_, pb, xb, s_, r_, prepare)
        got(xb.at[yo_y], r_.at[0], "w_x0")
        tot = pb[own(yo_y), :].astype(f32) + xb[yo_y].astype(f32)
        fs[0] = tot[:, :COLS].astype(bf16)
        fs[1] = tot[:, COLS:].astype(bf16)
        send(fs.at[0], fr.at[0], s_.at[4], r_.at[4], yn)
        send(fs.at[1], fr.at[1], s_.at[5], r_.at[5], yp)

    def rs_second(a, wv_, pb, xb, fs, fr, gs, gr, s_, r_, prepare):
        rs_rows(2, yp_y, a, wv_, pb, xb, s_, r_, prepare)
        rs_rows(3, y, a, wv_, pb, xb, s_, r_, prepare)
        got(xb.at[yn_y], r_.at[1], "w_x1")
        tot = pb[own(yn_y), COLS:].astype(f32) + xb[yn_y, :, COLS:].astype(f32)
        gs[1] = tot.astype(bf16)
        send(gs.at[1], gr.at[1], s_.at[7], r_.at[7], yn)
        got(xb.at[yp_y], r_.at[2], "w_x2")
        tot = pb[own(yp_y), :COLS].astype(f32) + xb[yp_y, :, :COLS].astype(f32)
        gs[2] = tot.astype(bf16)
        send(gs.at[2], gr.at[2], s_.at[8], r_.at[8], yp)

    def rs_mid(a, wv_, pb, xb, fs, fr, gs, gr, s_, r_):
        got(fr.at[0], r_.at[4], "w_f0")
        tot = pb[own(yn_y), :COLS].astype(f32) + xb[yn_y, :, :COLS].astype(f32)
        gs[0] = (tot + fr[0].astype(f32)).astype(bf16)
        send(gs.at[0], gr.at[0], s_.at[6], r_.at[6], yn)
        got(fr.at[1], r_.at[5], "w_f1")
        tot = pb[own(yp_y), COLS:].astype(f32) + xb[yp_y, :, COLS:].astype(f32)
        gs[3] = (tot + fr[1].astype(f32)).astype(bf16)
        send(gs.at[3], gr.at[3], s_.at[9], r_.at[9], yp)

    def here(pb, xb, cs):
        return pb[own(y), cs].astype(f32) + xb[y, :, cs].astype(f32)

    def filtered(n, d):
        @pl.when(jnp.logical_and(d == 0, sp > 0))
        def _():
            with scope("w_edge"):
                edge.wait_recv()
            prod[0:8, :] = er[8:16, :].astype(f32)

        rows = pl.ds(pl.multiple_of(d * 192, 64), 192)
        mine = pl.ds(pl.multiple_of(me * CH, CH), CH)
        near = prod[pl.ds(pl.multiple_of(d * 192, 64), 200), :]
        f = taps[0:1, mine] * near[6:198]
        f = f + taps[1:2, mine] * near[7:199]
        f = f + taps[2:3, mine] * near[8:200]
        cbr[rows, :] = (proj[rows, 1024:1280].astype(f32) * f).astype(bf16)

    conv_set = (cbr, woc_v, pb_c, x_c, fs_c, fr_c, gs_c, gr_c, rc_s, rc_r)
    head_set = (mob, wom_v, pb_h, x_h, fs_h, fr_h, gs_h, gr_h, rh_s, rh_r)
    weights[6].wait()
    weights[7].wait()
    def start_carry(g, p):
        lo, hi = groups[g]
        n = TILES // (hi - lo)
        pltpu.make_async_remote_copy(
            src_ref=cv.at[p - lo, pl.ds(0, n)], dst_ref=cr.at[pl.ds((sp - lo) * n, n)],
            send_sem=cr_s, recv_sem=cr_r, device_id=(p, me), device_id_type=MESH,
        ).start()

    def pass_on(g):
        lo, hi = groups[g]
        out_ = []
        for q, p in enumerate(following(g)):
            n = TILES // (groups[g + 1][1] - groups[g + 1][0])
            out_ += [
                pltpu.make_async_remote_copy(
                    src_ref=ex.at[pl.ds(q * n, n)], dst_ref=px.at[pl.ds(0, n)],
                    send_sem=ex_s.at[q], recv_sem=px_r, device_id=(p, me), device_id_type=MESH,
                ),
                pltpu.make_async_remote_copy(
                    src_ref=ea, dst_ref=pa, send_sem=ea_s.at[q], recv_sem=pa_r,
                    device_id=(p, me), device_id_type=MESH,
                ),
            ]
        return out_

    def recurrence(g):
        lo, hi = groups[g]
        n = TILES // (hi - lo)
        with scope("w_state"):
            if hi - lo > 1:
                got(aux.at[pl.ds(0, hi - lo - 1)], aux_r)
                got(rv.at[pl.ds(0, hi - lo - 1), pl.ds(0, n)], st_r)
        if lo:
            with scope("w_prefix"):
                got(px.at[pl.ds(0, n)], px_r)
                got(pa, pa_r)
            tiles = [px[k] for k in range(n)]
            run_m = pa[:, 0:128]
            run_n = pa[:, 128:256]
        else:
            tiles = []
            for k in range(n):
                p = (sp - lo) * n + k
                r_i = pl.ds(pl.multiple_of((p // 2) * 8, 8), 8)
                c_i = pl.ds(pl.multiple_of(lax.rem(p, 2) * 128, 128), 128)
                tiles.append(fmem[r_i, c_i])
            run_m = jnp.zeros((1, 128), f32)
            run_n = fnorm[...]
        last_one = hi == n_sp
        for b in range(lo, hi):
            for k in range(n):
                cv[b - lo, k] = tiles[k]
            mh[b - lo] = run_m
            nh[b - lo] = run_n
            if b < hi - 1 or not last_one:
                row = aux[b]
                new_m = jnp.maximum(run_m + row[:, 0:128], row[:, 128:256])
                old = jnp.exp(run_m + row[:, 0:128] - new_m)
                new = jnp.exp(row[:, 128:256] - new_m)
                tiles = [old * tiles[k] + new * rv[b - lo, k] for k in range(n)]
                run_n = old * run_n + new * row[:, 256:384]
                run_m = new_m
        if not last_one:
            for k in range(n):
                ex[k] = tiles[k]
            ea[...] = jnp.concatenate([run_m, run_n], axis=1)
            with scope("w_ready"):
                pl.semaphore_wait(ready, len(following(g)))
            for cp in pass_on(g):
                cp.start()
        with scope("send_carry"):
            mates(g, functools.partial(start_carry, g))
        for k in range(n):
            cr[(sp - lo) * n + k] = cv[sp - lo, k]
        m_at[...] = mh[sp - lo]
        n_at[...] = nh[sp - lo]

    def take(g):
        @pl.when(in_group(g))
        def _():
            recurrence(g)

    with scope("rs_first_conv"):
        rs_first(*conv_set, filtered)
    take(0)
    with scope("rs_second_conv"):
        rs_second(*conv_set, filtered)

    with scope("mixing"):
        top = jnp.broadcast_to(u_row, (8, BLK))
        urow[...] = top
        for s in (1, 2, 4, 8, 16, 32, 64, 128, 256, 512):
            top = jnp.maximum(top, jnp.where(lane >= s, pltpu.roll(top, s, 1), -jnp.inf))
        cols = jnp.concatenate([top, jnp.zeros((120, BLK), f32)], axis=0).T
        cmcol[...] = jnp.broadcast_to(cols[:, 0:1], (BLK, 128))
        for rb in range(3):
            r0 = rb * 256
            q = proj[r0 : r0 + 256, 128:256]
            cm = cmcol[r0 : r0 + 256, 0:1]
            acc = jnp.zeros((256, VAL), f32)
            tot = jnp.zeros((256, 1), f32)
            for cb in range(rb + 1):
                c0 = cb * 256
                mix = nt_dot(q, proj[c0 : c0 + 256, 0:128]) * SCALE
                mix = mix * jnp.exp(urow[0:1, c0 : c0 + 256] - cm)
                if cb == rb:
                    ri = lax.broadcasted_iota(jnp.int32, (256, 256), 0)
                    ci = lax.broadcasted_iota(jnp.int32, (256, 256), 1)
                    mix = jnp.where(ri >= ci, mix, 0.0)
                tot = tot + jnp.sum(mix, axis=1, keepdims=True)
                acc = acc + dot(mix.astype(bf16), proj[c0 : c0 + 256, 256:512])
            pv[r0 : r0 + 256, :] = acc
            rs[r0 : r0 + 256, :] = jnp.broadcast_to(tot, (256, 128))

    for g in range(1, len(groups)):
        take(g)
    with scope("rs_mid_conv"):
        rs_mid(*conv_set)

    for g, (lo, hi) in enumerate(groups):

        @pl.when(in_group(g))
        def _(lo=lo, hi=hi):
            got(cr.at[pl.ds(0, TILES - TILES // (hi - lo))], cr_r, "w_carry")

    with scope("carry"):
        for p in range(TILES):
            i, j = p // 2, p % 2
            cmem[8 * i : 8 * i + 8, 128 * j : 128 * j + 128] = cr[p]
        carry = cmem[...]
        high = carry.astype(bf16)
        low = (carry - high.astype(f32)).astype(bf16)
        m_in = m_at[:, 0:1]
        n_in = n_at[...]
        n_1 = n_in.astype(bf16).astype(f32)
        n_2 = (n_in - n_1).astype(bf16).astype(f32)
        n_3 = n_in - n_1 - n_2
        sub16 = lax.broadcasted_iota(jnp.int32, (16, 128), 0)
        n_rows = jnp.where(
            sub16 == 0, n_1, jnp.where(sub16 == 1, n_2, jnp.where(sub16 == 2, n_3, 0.0))
        ).astype(bf16)

    def heads(n, d):
        rows = pl.ds(pl.multiple_of(d * 192, 64), 192)
        q = proj[rows, 128:256]
        cm = cmcol[rows, 0:1]
        peak = jnp.maximum(cm, m_in)
        f_in = jnp.exp(cm - peak)
        f_carry = jnp.exp(m_in - peak)
        from_memory = (dot(q, high) + dot(q, low)) * SCALE
        from_norm = jnp.sum(nt_dot(q, n_rows), axis=1, keepdims=True) * SCALE
        num = f_in * pv[rows, :] + f_carry * from_memory
        den = f_in * rs[rows, 0:1] + f_carry * from_norm
        memory_out = num / jnp.maximum(jnp.abs(den), 1.0)
        squares = jnp.sum(memory_out * memory_out, axis=1, keepdims=True)
        sqcol[rows, :] = jnp.broadcast_to(squares, (192, 128))
        mob[rows, :] = memory_out.astype(bf16)

    with scope("rs_first_head"):
        rs_first(*head_set, heads)
    with scope("rs_second_head"):
        rs_second(*head_set, heads)
    ss[me] = sqcol[...].T[0:1]
    for k in range(1, NTP):
        send(ss.at[me], ss.at[me], ss_s.at[k], ss_r.at[k], lax.rem(me + k, NTP))
    with scope("rs_mid_head"):
        rs_mid(*head_set)
    for k in range(1, NTP):
        got(ss.at[lax.rem(me + NTP - k, NTP)], ss_r.at[k], "w_ss")
    total = ss[0]
    for k in range(1, NTP):
        total = total + ss[k]
    factor = lax.rsqrt(total / (NTP * VAL) + EPS)
    scol[...] = jnp.broadcast_to(factor, (128, BLK)).T
    got(x_c.at[y], rc_r.at[3])
    for k in range(4):
        got(gr_c.at[k], rc_r.at[6 + k], "w_gc")
    got(x_h.at[y], rh_r.at[3])
    factor = scol[pl.ds(pl.multiple_of(me * ROWS, 8), ROWS), 0:1]
    for k in range(2):
        cs = slice(k * COLS, (k + 1) * COLS)
        conv_sum = here(pb_c, x_c, cs) + gr_c[k].astype(f32) + gr_c[2 + k].astype(f32)
        fin[:, cs] = conv_sum + factor * here(pb_h, x_h, cs)
    for k in (1, 2, 0, 3):
        got(gr_h.at[k], rh_r.at[6 + k], "w_gh")
    with scope("final"):
        for k in range(2):
            cs = slice(k * COLS, (k + 1) * COLS)
            rest_sum = gr_h[k].astype(f32) + gr_h[2 + k].astype(f32)
            out[:, cs] = (fin[:, cs] + factor * rest_sum).astype(bf16)

    for cp in sends:
        cp.wait_send()
    def sent(ref, sem):
        pltpu.make_async_remote_copy(
            src_ref=ref, dst_ref=ref, send_sem=sem, recv_sem=sem,
            device_id=(sp, sib), device_id_type=MESH,
        ).wait_send()

    @pl.when(sp < n_sp - 1)
    def _():
        edge.wait_send()

    for g, (lo, hi) in enumerate(groups):

        @pl.when(in_group(g))
        def _(g=g, lo=lo, hi=hi):
            if hi - lo > 1:
                rest = pl.ds(0, TILES - TILES // (hi - lo))
                sent(st.at[rest], st_s)
                sent(aux.at[pl.ds(0, hi - lo - 1)], aux_s)
                sent(cr.at[rest], cr_s)
            for cp in pass_on(g):
                cp.wait_send()


def solution(mesh):
    n_sp = mesh.shape["sp"]
    groups = groups_of(n_sp)
    gmax = max(hi - lo for lo, hi in groups)
    tmax = max(TILES // (hi - lo) for lo, hi in groups)
    vmem = pl.BlockSpec(memory_space=pltpu.VMEM)
    hbm = pl.BlockSpec(memory_space=pl.ANY)
    dma = pltpu.SemaphoreType.DMA

    def rs_bufs():
        return [
            pltpu.VMEM((BLK, D), bf16),
            pltpu.VMEM((4, ROWS, D), bf16),
            pltpu.VMEM((2, ROWS, COLS), bf16),
            pltpu.VMEM((2, ROWS, COLS), bf16),
            pltpu.VMEM((4, ROWS, COLS), bf16),
            pltpu.VMEM((4, ROWS, COLS), bf16),
        ]

    scratch = [
        pltpu.VMEM((ROWS, D), bf16),
        pltpu.VMEM((1, D), f32),
        pltpu.VMEM((NTP, D), bf16),
        pltpu.VMEM((NTP, D), bf16),
        pltpu.VMEM((1, NTP), f32),
        pltpu.VMEM((1, BLK), f32),
        pltpu.VMEM((3, NTP * CH), f32),
        pltpu.VMEM((KEY, VAL), f32),
        pltpu.VMEM((1, KEY), f32),
        pltpu.VMEM((BLK, D), bf16),
        pltpu.VMEM((D, 1408), bf16),
        pltpu.VMEM((VAL, D), bf16),
        pltpu.VMEM((CH, D), bf16),
        pltpu.VMEM((BLK, 1280), bf16),
        pltpu.VMEM((BLK, 128), f32),
        pltpu.VMEM((8, BLK), f32),
        pltpu.VMEM((BLK, 128), f32),
        pltpu.VMEM((TILES, 8, 128), f32),
        pltpu.VMEM((gmax, tmax, 8, 128), f32),
        pltpu.VMEM((n_sp, 1, 384), f32),
        pltpu.VMEM((gmax, tmax, 8, 128), f32),
        pltpu.VMEM((TILES, 8, 128), f32),
        pltpu.VMEM((gmax, 1, 128), f32),
        pltpu.VMEM((gmax, 1, 128), f32),
        pltpu.VMEM((1, 128), f32),
        pltpu.VMEM((1, 128), f32),
        pltpu.VMEM((tmax, 8, 128), f32),
        pltpu.VMEM((1, 256), f32),
        pltpu.VMEM((tmax, 8, 128), f32),
        pltpu.VMEM((1, 256), f32),
        pltpu.VMEM((KEY, VAL), f32),
        pltpu.VMEM((BLK, VAL), f32),
        pltpu.VMEM((BLK, 128), f32),
        pltpu.VMEM((BLK, VAL), bf16),
        pltpu.VMEM((BLK, CH), bf16),
        pltpu.VMEM((BLK + 8, CH), f32),
        pltpu.VMEM((16, CH), bf16),
        pltpu.VMEM((16, CH), bf16),
        pltpu.VMEM((NTP, 1, BLK), f32),
        pltpu.VMEM((BLK, 128), f32),
        pltpu.VMEM((BLK, 128), f32),
        pltpu.VMEM((ROWS, D), f32),
        *rs_bufs(),
        *rs_bufs(),
        dma((8,)),
        dma((9,)),
        dma((13,)),
        dma((13,)),
        dma(()),
        dma(()),
        dma(()),
        dma(()),
        dma(()),
        dma(()),
        dma(()),
        dma(()),
        dma((NTP,)),
        dma((NTP,)),
        dma((10,)),
        dma((10,)),
        dma((10,)),
        dma((10,)),
        dma((4,)),
        dma(()),
        dma((4,)),
        dma(()),
        pltpu.SemaphoreType.REGULAR,
        pltpu.SemaphoreType.REGULAR,
    ]

    def per_device(
        tokens, in_gain, w_query, w_key, w_value, w_input_gate, w_forget_gate, forget_bias,
        forget_extra, w_conv_gate, w_conv_left, w_conv_right, conv_taps, first_memory,
        first_norm, w_out_memory, w_out_conv,
    ):
        return pl.pallas_call(
            functools.partial(kernel, n_sp),
            out_shape=jax.ShapeDtypeStruct((ROWS, D), bf16),
            in_specs=[hbm] * 17,
            out_specs=vmem,
            scratch_shapes=scratch,
            compiler_params=pltpu.CompilerParams(
                collective_id=0, has_side_effects=True, vmem_limit_bytes=60 * 1024 * 1024
            ),
        )(
            tokens, in_gain.reshape(1, D), w_input_gate.T, w_forget_gate.T,
            forget_bias.reshape(1, NTP),
            forget_extra.reshape(1, BLK), conv_taps, first_memory.reshape(KEY, VAL), first_norm,
            w_query, w_key, w_value, w_conv_gate, w_conv_left, w_conv_right,
            w_out_memory, w_out_conv,
        )

    placed = (
        P(("sp", "tp"), None),
        P(),
        P(None, "tp"),
        P(None, "tp"),
        P(None, "tp"),
        P(),
        P(),
        P(),
        P("sp", "tp"),
        P(None, "tp"),
        P(None, "tp"),
        P(None, "tp"),
        P(),
        P("tp", None, None),
        P("tp", None),
        P("tp", None),
        P("tp", None),
    )
    return jax.shard_map(
        per_device, mesh=mesh, in_specs=placed, out_specs=P(("sp", "tp"), None), check_vma=False
    )
```

```python
import functools

import jax
import jax.numpy as jnp
from jax import lax
from jax.experimental import pallas as pl
from jax.experimental.pallas import tpu as pltpu
from jax.sharding import PartitionSpec as P

D = 2048
KEY = 128
VAL = 256
CH = 256
ROWS = 96
HALF = 48
BLK = 768
NTP = 8
TILES = 16
COLS = 1024
EPS = 1e-06
SCALE = KEY ** (-0.5)
MESH = pl.DeviceIdType.MESH
f32 = jnp.float32
bf16 = jnp.bfloat16


def nt_dot(a, b):
    return lax.dot_general(a, b, (((1,), (1,)), ((), ())), preferred_element_type=f32)


def groups_of(n_sp):
    if n_sp == 32:
        return ((0, 8), (8, 16), (16, 32))
    if n_sp == 4:
        return ((0, 2), (2, 4))
    return ((0, n_sp),)


def dot(a, b):
    return jnp.dot(a, b, preferred_element_type=f32)


def kernel(
    n_sp,
    tok_h, gain_h, wi_h, wf_h, bias_h, fextra_h, taps_h, fmem_h, fnorm_h,
    wq, wk, wv, wcg, wcl, wcr, wom, woc,
    out,
    tok, gain, wi, wf, bias, fextra, taps, fmem, fnorm,
    x, w_all, wom_v, woc_v,
    proj, gates, urow, cmcol, st, rv, aux, cv, cr, mh, nh, m_at, n_at,
    ex, ea, px, pa, cmem, pv, rs,
    mob, cbr, prod, eb, er, ss, scol, sqcol, own_c, own_h, part,
    x_c, fs_c, fr_c, gs_c, gr_c,
    x_h, fs_h, fr_h, gs_h, gr_h,
    wsem, isem, ag_s, ag_r, aux_s, aux_r, st_s, st_r, cr_s, cr_r, ed_s, ed_r, ss_s, ss_r,
    rc_s, rc_r, rh_s, rh_r, ex_s, px_r, ea_s, pa_r, ready, ready_edge, ow_s, ow_r,
):
    groups = groups_of(n_sp)
    scope = jax.named_scope
    sp = lax.axis_index("sp")
    me = lax.axis_index("tp")
    y = me // 2
    c = lax.rem(me, 2)
    sib = me + 1 - 2 * c
    yn_y, yp_y, yo_y = lax.rem(y + 1, 4), lax.rem(y + 3, 4), lax.rem(y + 2, 4)
    yn, yp = yn_y * 2 + c, yp_y * 2 + c

    def in_group(g):
        return jnp.logical_and(sp >= groups[g][0], sp < groups[g][1])

    def mates(g, start):
        lo, hi = groups[g]
        n = hi - lo
        for k in range(1, n):
            far = n // 2 + (k // 2 if k % 2 else -(k // 2))
            start(lo + lax.rem(sp - lo + far, n))

    def following(g):
        lo, hi = groups[g]
        if g + 1 == len(groups):
            return []
        at, end = groups[g + 1]
        ratio = (end - at) // (hi - lo)
        return [at + (sp - lo) * ratio + q for q in range(ratio)]

    def preceding(g):
        lo, hi = groups[g]
        at, end = groups[g - 1]
        return at + (sp - lo) // ((hi - lo) // (end - at))

    inputs = [
        pltpu.make_async_copy(src, dst, isem.at[i])
        for i, (src, dst) in enumerate(
            [
                (tok_h, tok), (gain_h, gain), (wi_h, wi), (wf_h, wf), (bias_h, bias),
                (fextra_h, fextra), (taps_h, taps), (fmem_h, fmem), (fnorm_h, fnorm),
            ]
        )
    ]
    weights = [
        pltpu.make_async_copy(src, dst, wsem.at[i])
        for i, (src, dst) in enumerate(
            [
                (wk, w_all.at[:, pl.ds(0, 128)]),
                (wq, w_all.at[:, pl.ds(128, 128)]),
                (wv, w_all.at[:, pl.ds(256, 256)]),
                (wcl, w_all.at[:, pl.ds(512, 256)]),
                (wcr, w_all.at[:, pl.ds(768, 256)]),
                (wcg, w_all.at[:, pl.ds(1024, 256)]),
                (woc, woc_v.at[pl.ds(0, CH), :]),
                (wom, wom_v.at[pl.ds(0, VAL), :]),
            ]
        )
    ]
    for cp in inputs[:4]:
        cp.start()
    barrier = pltpu.get_barrier_semaphore()
    for k in range(1, NTP):
        pl.semaphore_signal(
            barrier, inc=1, device_id=(sp, lax.rem(me + k, NTP)), device_id_type=MESH
        )

    def greet(p):
        pl.semaphore_signal(barrier, inc=1, device_id=(p, me), device_id_type=MESH)

    for g, (lo, hi) in enumerate(groups):

        @pl.when(in_group(g))
        def _(g=g):
            mates(g, greet)
            for p in following(g):
                greet(p)

        if hi < n_sp:

            @pl.when(sp == hi - 1)
            def _():
                greet(sp + 1)

    for cp in inputs[4:]:
        cp.start()
    for w in weights:
        w.start()

    def slots(s, n=1):
        return x.at[pl.ds(pl.multiple_of(s * HALF, 16), n * HALF), :]

    with scope("norm"):
        inputs[0].wait()
        inputs[1].wait()
        t = tok[...].astype(f32)
        scale = lax.rsqrt(jnp.mean(t * t, axis=1, keepdims=True) + EPS)
        x[pl.ds(pl.multiple_of(c * ROWS, 16), ROWS), :] = (t * scale * gain[...]).astype(bf16)
    prod[0:8, :] = jnp.zeros((8, CH), f32)

    with scope("w_barrier"):
        for g, (lo, hi) in enumerate(groups):
            count = NTP - 1 + hi - lo - 1 + (1 if lo else 0)

            @pl.when(jnp.logical_and(in_group(g), jnp.logical_or(sp != lo, lo == 0)))
            def _(count=count):
                pl.semaphore_wait(barrier, count)

            if lo:

                @pl.when(sp == lo)
                def _(count=count):
                    pl.semaphore_wait(barrier, count + 1)

    sends = []

    def send(src, dst, ssem, rsem, peer):
        cp = pltpu.make_async_remote_copy(
            src_ref=src, dst_ref=dst, send_sem=ssem, recv_sem=rsem,
            device_id=(sp, peer), device_id_type=MESH,
        )
        cp.start()
        sends.append(cp)

    def got(dst, rsem, name="w"):
        with scope(name):
            pltpu.make_async_remote_copy(
                src_ref=dst, dst_ref=dst, send_sem=rsem, recv_sem=rsem,
                device_id=(sp, sib), device_id_type=MESH,
            ).wait_recv()

    def ag(src, dst, k, peer, n=1):
        send(slots(src, n), slots(dst, n), ag_s.at[k], ag_r.at[k], peer)

    other = 1 - c
    ag(2 * c, 4 + c, 0, yn)
    ag(2 * c + 1, 6 + c, 3, yp)
    ag(2 * c + 1, 8 + c, 1, yn)
    ag(2 * c, 10 + c, 4, yp)
    ag(2 * c, 2 * c, 6, sib, 2)
    send(woc, woc_v.at[pl.ds(CH, CH), :], ow_s.at[0], ow_r.at[0], sib)
    send(wom, wom_v.at[pl.ds(VAL, VAL), :], ow_s.at[1], ow_r.at[1], sib)
    def tell(sem, p):
        pl.semaphore_signal(sem, inc=1, device_id=(p, me), device_id_type=MESH)

    for g, (lo, hi) in enumerate(groups):
        if lo:

            @pl.when(in_group(g))
            def _(g=g):
                tell(ready, preceding(g))

            @pl.when(sp == lo)
            def _():
                tell(ready_edge, sp - 1)

    for cp in inputs[2:]:
        cp.wait()
    gw = jnp.concatenate(
        [wi[...].astype(f32), wf[...].astype(f32), jnp.zeros((112, D), f32)], axis=0
    )
    w_all[:, 1280:1408] = gw.T.astype(bf16)
    with scope("w_weights"):
        for i in range(6):
            weights[i].wait()

    def project(stage, bases, parts):
        xs = x[stage * 192 : stage * 192 + 192, :]
        for lo, hi in parts:
            res = dot(xs, w_all[:, lo:hi])
            for k, base in enumerate(bases):
                rows = pl.ds(pl.multiple_of(base, 16), HALF)
                piece = res[k * HALF : (k + 1) * HALF]
                if lo == 512:
                    left = piece[:, :CH].astype(bf16).astype(f32)
                    right = piece[:, CH:].astype(bf16).astype(f32)
                    at = pl.ds(pl.multiple_of(base + 8, 8), HALF)
                    prod[at, :] = (left * right).astype(bf16).astype(f32)
                elif hi <= 1280:
                    proj[rows, lo:hi] = piece.astype(bf16)
                else:
                    gates[rows, :] = piece[:, 1280 - lo :]
                    if lo < 1280:
                        proj[rows, lo:1280] = piece[:, : 1280 - lo].astype(bf16)

    edge = pltpu.make_async_remote_copy(
        src_ref=eb, dst_ref=er, send_sem=ed_s, recv_sem=ed_r,
        device_id=(lax.rem(sp + 1, n_sp), me), device_id_type=MESH,
    )

    def send_edge(where):
        @pl.when(jnp.logical_and(y == where, sp < n_sp - 1))
        def _():
            eb[...] = prod[BLK - 8 :, :].astype(bf16)
            for lo, hi in groups[:-1]:

                @pl.when(sp == hi - 1)
                def _():
                    pl.semaphore_wait(ready_edge, 1)

            edge.start()

    def own(d):
        return pl.ds(pl.multiple_of((d * 2 + c) * ROWS, 16), ROWS)

    def his(d):
        return pl.ds(pl.multiple_of((d * 2 + 1 - c) * ROWS, 16), ROWS)

    order = (yo_y, yn_y, yp_y, y)

    def rs_part(n, a, w, xb, s_, r_, prepare, kept=True):
        prepare(n, order[n])
        send(a.at[his(order[n])], xb.at[n], s_.at[n], r_.at[n], sib)
        if not kept:
            sends.pop()

    def both(n, a, xb):
        return jnp.concatenate([a[own(order[n]), :], xb[n]], axis=1)

    def rs_first(a, w, xb, fs, fr, gs, gr, kept, s_, r_):
        got(xb.at[0], r_.at[0], "w_x0")
        lhs = both(0, a, xb)
        for k, peer in ((0, yn), (1, yp)):
            fs[k] = dot(lhs, w[:, k * COLS : (k + 1) * COLS]).astype(bf16)
            send(fs.at[k], fr.at[k], s_.at[4 + k], r_.at[4 + k], peer)

    def rs_second(a, w, xb, fs, fr, gs, gr, kept, s_, r_):
        for n in (1, 2, 3):
            got(xb.at[n], r_.at[n], "w_x123")
        lhs = jnp.concatenate([both(n, a, xb) for n in (1, 2, 3)], axis=0)
        res = dot(lhs, w[:, COLS:])
        gs[1] = res[0:ROWS].astype(bf16)
        send(gs.at[1], gr.at[1], s_.at[7], r_.at[7], yn)
        part[1] = res[ROWS : 2 * ROWS]
        kept[:, COLS:] = res[2 * ROWS :]
        res = dot(lhs, w[:, :COLS])
        gs[2] = res[ROWS : 2 * ROWS].astype(bf16)
        send(gs.at[2], gr.at[2], s_.at[8], r_.at[8], yp)
        part[0] = res[0:ROWS]
        kept[:, :COLS] = res[2 * ROWS :]

    def rs_mid(a, w, xb, fs, fr, gs, gr, kept, s_, r_):
        got(fr.at[0], r_.at[4], "w_f0")
        gs[0] = (part[0] + fr[0].astype(f32)).astype(bf16)
        send(gs.at[0], gr.at[0], s_.at[6], r_.at[6], yn)
        got(fr.at[1], r_.at[5], "w_f1")
        gs[3] = (part[1] + fr[1].astype(f32)).astype(bf16)
        send(gs.at[3], gr.at[3], s_.at[9], r_.at[9], yp)

    def filtered(n, d):
        @pl.when(jnp.logical_and(d == 0, sp > 0))
        def _():
            with scope("w_edge"):
                edge.wait_recv()
            prod[0:8, :] = er[8:16, :].astype(f32)

        rows = pl.ds(pl.multiple_of(d * 192, 64), 192)
        mine = pl.ds(pl.multiple_of(me * CH, CH), CH)
        near = prod[pl.ds(pl.multiple_of(d * 192, 64), 200), :]
        f = taps[0:1, mine] * near[6:198]
        f = f + taps[1:2, mine] * near[7:199]
        f = f + taps[2:3, mine] * near[8:200]
        cbr[rows, :] = (proj[rows, 1024:1280].astype(f32) * f).astype(bf16)

    conv_set = (cbr, woc_v, x_c, fs_c, fr_c, gs_c, gr_c, own_c, rc_s, rc_r)
    head_set = (mob, wom_v, x_h, fs_h, fr_h, gs_h, gr_h, own_h, rh_s, rh_r)

    def conv_part(n, kept=True):
        rs_part(n, cbr, woc_v, x_c, rc_s, rc_r, filtered, kept)

    every = ((0, 512), (512, 1024), (1024, 1408))
    got(slots(2 * other, 2), ag_r.at[6], "w_ag6")
    with scope("proj_0"):
        project(0, [y * 192 + HALF * k for k in range(4)], every)
        send_edge(3)
    got(slots(4 + c), ag_r.at[0], "w_ag0")
    ag(4 + c, 12 + c, 2, yn)
    ag(4 + c, 4 + c, 7, sib)
    got(slots(6 + c), ag_r.at[3], "w_ag3")
    ag(6 + c, 14 + c, 5, yp)
    ag(6 + c, 6 + c, 8, sib)
    got(slots(4 + other), ag_r.at[7], "w_ag7")
    got(slots(6 + other), ag_r.at[8], "w_ag8")
    with scope("proj_1"):
        project(
            1,
            [yp_y * 192, yp_y * 192 + ROWS, yn_y * 192 + HALF, yn_y * 192 + ROWS + HALF],
            every,
        )
        send_edge(2)
    got(slots(8 + c), ag_r.at[1], "w_ag1")
    ag(8 + c, 8 + c, 9, sib)
    got(slots(10 + c), ag_r.at[4], "w_ag4")
    ag(10 + c, 10 + c, 10, sib)
    got(slots(8 + other), ag_r.at[9], "w_ag9")
    got(slots(10 + other), ag_r.at[10], "w_ag10")
    with scope("proj_2"):
        project(
            2,
            [yp_y * 192 + HALF, yp_y * 192 + ROWS + HALF, yn_y * 192, yn_y * 192 + ROWS],
            every,
        )
        send_edge(0)
    got(slots(12 + c), ag_r.at[2], "w_ag2")
    ag(12 + c, 12 + c, 11, sib)
    got(slots(14 + c), ag_r.at[5], "w_ag5")
    ag(14 + c, 14 + c, 12, sib)
    with scope("conv_early"):
        conv_part(1)
    got(slots(12 + other), ag_r.at[11], "w_ag11")
    got(slots(14 + other), ag_r.at[12], "w_ag12")
    last = [yo_y * 192, yo_y * 192 + ROWS, yo_y * 192 + HALF, yo_y * 192 + ROWS + HALF]
    with scope("proj_3"):
        project(3, last, ((1280, 1408), (0, 512)))

    with scope("state"):
        g_t = gates[...].T
        sub = lax.broadcasted_iota(jnp.int32, (8, BLK), 0)
        lane = lax.broadcasted_iota(jnp.int32, (8, BLK), 1)
        in_row = jnp.sum(jnp.where(sub == me, g_t[0:8], 0.0), axis=0, keepdims=True)
        f_row = jnp.sum(jnp.where(sub == me, g_t[8:16], 0.0), axis=0, keepdims=True)
        lane8 = lax.broadcasted_iota(jnp.int32, (1, NTP), 1)
        f_row = f_row + jnp.sum(jnp.where(lane8 == me, bias[...], 0.0), axis=1, keepdims=True)
        log_forget = (
            jnp.minimum(f_row, 0.0) - jnp.log1p(jnp.exp(-jnp.abs(f_row))) + fextra[...]
        )

        def stacked(row):
            parts = [row[:, 128 * k : 128 * k + 128] for k in range(6)]
            return jnp.concatenate(parts + [jnp.zeros((2, 128), f32)], axis=0)

        lf6 = stacked(log_forget)
        l_1 = lf6.astype(bf16).astype(f32)
        l_2 = (lf6 - l_1).astype(bf16).astype(f32)
        l_3 = lf6 - l_1 - l_2
        upto = lax.broadcasted_iota(jnp.int32, (128, 128), 0) <= lax.broadcasted_iota(
            jnp.int32, (128, 128), 1
        )
        sums = dot(
            jnp.concatenate([l_1, l_2, l_3, jnp.zeros((8, 128), f32)], axis=0).astype(bf16),
            jnp.where(upto, 1.0, 0.0).astype(bf16),
        )
        inside = sums[0:8] + sums[8:16] + sums[16:24]
        sub8 = lax.broadcasted_iota(jnp.int32, (8, 128), 0)
        ends = jnp.broadcast_to(inside[:, 127:128], (8, 128))
        before = jnp.where(sub8 >= 1, pltpu.roll(ends, 1, 0), 0.0)
        for s in (1, 2, 4):
            before = before + jnp.where(sub8 >= s, pltpu.roll(before, s, 0), 0.0)
        cum6 = inside + before
        u6 = jnp.where(sub8 < 6, stacked(in_row) - cum6, -jnp.inf)
        u_max = jnp.max(jnp.max(u6, axis=1, keepdims=True), axis=0, keepdims=True)
        decay = cum6[5:6, 127:128]

        def unstacked(a):
            return jnp.concatenate([a[k : k + 1] for k in range(6)], axis=1)

        u_row = unstacked(u6)
        k_t = proj[:, 0:128].astype(f32).T
        keyed = k_t * jnp.exp(u_row - u_max)
        mem = dot(keyed.astype(bf16), proj[:, 256:512])
        norm_col = jnp.sum(keyed, axis=1, keepdims=True)
        block_norm = jnp.broadcast_to(norm_col, (128, 128)).T[0:1]
        d_lanes = jnp.broadcast_to(decay, (1, 128))
        m_lanes = jnp.broadcast_to(decay + u_max, (1, 128))
        aux[sp] = jnp.concatenate([d_lanes, m_lanes, block_norm], axis=1)
        for p in range(TILES):
            i, j = p // 2, p % 2
            st[p] = mem[16 * i : 16 * i + 16, 128 * j : 128 * j + 128].astype(bf16)

    def start_state(g, p):
        lo, hi = groups[g]
        n = TILES // (hi - lo)
        pltpu.make_async_remote_copy(
            src_ref=st.at[pl.ds((p - lo) * n, n)], dst_ref=rv.at[sp - lo, pl.ds(0, n)],
            send_sem=st_s, recv_sem=st_r, device_id=(p, me), device_id_type=MESH,
        ).start()
        pltpu.make_async_remote_copy(
            src_ref=aux.at[sp], dst_ref=aux.at[sp], send_sem=aux_s, recv_sem=aux_r,
            device_id=(p, me), device_id_type=MESH,
        ).start()

    with scope("send_state"):
        for g, (lo, hi) in enumerate(groups):

            @pl.when(in_group(g))
            def _(g=g, lo=lo, hi=hi):
                mates(g, functools.partial(start_state, g))
                n = TILES // (hi - lo)
                for k in range(n):
                    rv[sp - lo, k] = st[(sp - lo) * n + k]

    with scope("proj_lrg"):
        project(3, last, ((512, 1024),))
        send_edge(1)
        project(3, last, ((1024, 1280),))

    def start_carry(g, p):
        lo, hi = groups[g]
        n = TILES // (hi - lo)
        pltpu.make_async_remote_copy(
            src_ref=cv.at[p - lo, pl.ds(0, n)], dst_ref=cr.at[pl.ds((sp - lo) * n, n)],
            send_sem=cr_s, recv_sem=cr_r, device_id=(p, me), device_id_type=MESH,
        ).start()

    def pass_on(g):
        lo, hi = groups[g]
        out_ = []
        for q, p in enumerate(following(g)):
            n = TILES // (groups[g + 1][1] - groups[g + 1][0])
            out_ += [
                pltpu.make_async_remote_copy(
                    src_ref=ex.at[pl.ds(q * n, n)], dst_ref=px.at[pl.ds(0, n)],
                    send_sem=ex_s.at[q], recv_sem=px_r, device_id=(p, me), device_id_type=MESH,
                ),
                pltpu.make_async_remote_copy(
                    src_ref=ea, dst_ref=pa, send_sem=ea_s.at[q], recv_sem=pa_r,
                    device_id=(p, me), device_id_type=MESH,
                ),
            ]
        return out_

    def recurrence(g):
        lo, hi = groups[g]
        n = TILES // (hi - lo)
        with scope("w_state"):
            if hi - lo > 1:
                got(aux.at[pl.ds(0, hi - lo - 1)], aux_r)
                got(rv.at[pl.ds(0, hi - lo - 1), pl.ds(0, n)], st_r)
        if lo:
            with scope("w_prefix"):
                got(px.at[pl.ds(0, n)], px_r)
                got(pa, pa_r)
            tiles = [px[k] for k in range(n)]
            run_m = pa[:, 0:128]
            run_n = pa[:, 128:256]
        else:
            tiles = []
            for k in range(n):
                p = (sp - lo) * n + k
                r_i = pl.ds(pl.multiple_of((p // 2) * 16, 16), 16)
                c_i = pl.ds(pl.multiple_of(lax.rem(p, 2) * 128, 128), 128)
                tiles.append(fmem[r_i, c_i])
            run_m = jnp.zeros((1, 128), f32)
            run_n = fnorm[...]
        last_one = hi == n_sp
        for b in range(lo, hi):
            for k in range(n):
                cv[b - lo, k] = tiles[k].astype(bf16)
            mh[b - lo] = run_m
            nh[b - lo] = run_n
            if b < hi - 1 or not last_one:
                row = aux[b]
                new_m = jnp.maximum(run_m + row[:, 0:128], row[:, 128:256])
                old = jnp.exp(run_m + row[:, 0:128] - new_m)
                new = jnp.exp(row[:, 128:256] - new_m)
                tiles = [old * tiles[k] + new * rv[b - lo, k].astype(f32) for k in range(n)]
                run_n = old * run_n + new * row[:, 256:384]
                run_m = new_m
        if not last_one:
            for k in range(n):
                ex[k] = tiles[k]
            ea[...] = jnp.concatenate([run_m, run_n], axis=1)
            with scope("w_ready"):
                pl.semaphore_wait(ready, len(following(g)))
            for cp in pass_on(g):
                cp.start()
        with scope("send_carry"):
            mates(g, functools.partial(start_carry, g))
        for k in range(n):
            cr[(sp - lo) * n + k] = cv[sp - lo, k]
        m_at[...] = mh[sp - lo]
        n_at[...] = nh[sp - lo]

    def take(g):
        @pl.when(in_group(g))
        def _():
            recurrence(g)

    with scope("rs_first_conv"):
        conv_part(0)
        conv_part(3)
        weights[6].wait()
        weights[7].wait()
        got(woc_v.at[pl.ds(CH, CH), :], ow_r.at[0])
        got(wom_v.at[pl.ds(VAL, VAL), :], ow_r.at[1])
        top = jnp.broadcast_to(u_row, (8, BLK))
        urow[...] = top
        for s in (1, 2, 4, 8, 16, 32, 64, 128, 256, 512):
            top = jnp.maximum(top, jnp.where(lane >= s, pltpu.roll(top, s, 1), -jnp.inf))
        cols = jnp.concatenate([top, jnp.zeros((120, BLK), f32)], axis=0).T
        cmcol[...] = jnp.broadcast_to(cols[:, 0:1], (BLK, 128))
        rs_first(*conv_set)
    for g in range(len(groups)):
        if g + 1 < len(groups):
            take(g)

            @pl.when(in_group(g))
            def _():
                conv_part(2, False)

    with scope("mixing"):
        for rb in range(3):
            r0 = rb * 256
            q = proj[r0 : r0 + 256, 128:256]
            cm = cmcol[r0 : r0 + 256, 0:1]
            acc = jnp.zeros((256, VAL), f32)
            tot = jnp.zeros((256, 1), f32)
            for cb in range(rb + 1):
                c0 = cb * 256
                mix = nt_dot(q, proj[c0 : c0 + 256, 0:128]) * SCALE
                mix = mix * jnp.exp(urow[0:1, c0 : c0 + 256] - cm)
                if cb == rb:
                    ri = lax.broadcasted_iota(jnp.int32, (256, 256), 0)
                    ci = lax.broadcasted_iota(jnp.int32, (256, 256), 1)
                    mix = jnp.where(ri >= ci, mix, 0.0)
                tot = tot + jnp.sum(mix, axis=1, keepdims=True)
                acc = acc + dot(mix.astype(bf16), proj[c0 : c0 + 256, 256:512])
            pv[r0 : r0 + 256, :] = acc
            rs[r0 : r0 + 256, :] = jnp.broadcast_to(tot, (256, 128))

    with scope("rs_second_conv"):

        @pl.when(in_group(len(groups) - 1))
        def _():
            conv_part(2, False)

        sends.append(
            pltpu.make_async_remote_copy(
                src_ref=cbr.at[his(order[2])], dst_ref=x_c.at[2], send_sem=rc_s.at[2],
                recv_sem=rc_r.at[2], device_id=(sp, sib), device_id_type=MESH,
            )
        )
        rs_second(*conv_set)
    take(len(groups) - 1)
    with scope("rs_mid_conv"):
        rs_mid(*conv_set)

    for g, (lo, hi) in enumerate(groups):

        @pl.when(in_group(g))
        def _(lo=lo, hi=hi):
            got(cr.at[pl.ds(0, TILES - TILES // (hi - lo))], cr_r, "w_carry")

    with scope("carry"):
        for p in range(TILES):
            i, j = p // 2, p % 2
            cmem[16 * i : 16 * i + 16, 128 * j : 128 * j + 128] = cr[p]
        carry = cmem[...]
        m_in = m_at[:, 0:1]
        n_in = n_at[...]
        n_1 = n_in.astype(bf16).astype(f32)
        n_2 = (n_in - n_1).astype(bf16).astype(f32)
        n_3 = n_in - n_1 - n_2
        sub16 = lax.broadcasted_iota(jnp.int32, (16, 128), 0)
        n_rows = jnp.where(
            sub16 == 0, n_1, jnp.where(sub16 == 1, n_2, jnp.where(sub16 == 2, n_3, 0.0))
        ).astype(bf16)

    def heads(n, d):
        rows = pl.ds(pl.multiple_of(d * 192, 64), 192)
        q = proj[rows, 128:256]
        cm = cmcol[rows, 0:1]
        peak = jnp.maximum(cm, m_in)
        f_in = jnp.exp(cm - peak)
        f_carry = jnp.exp(m_in - peak)
        from_memory = dot(q, carry) * SCALE
        from_norm = jnp.sum(nt_dot(q, n_rows), axis=1, keepdims=True) * SCALE
        num = f_in * pv[rows, :] + f_carry * from_memory
        den = f_in * rs[rows, 0:1] + f_carry * from_norm
        memory_out = num / jnp.maximum(jnp.abs(den), 1.0)
        squares = jnp.sum(memory_out * memory_out, axis=1, keepdims=True)
        sqcol[rows, :] = jnp.broadcast_to(squares, (192, 128))
        mob[rows, :] = memory_out.astype(bf16)

    with scope("rs_first_head"):
        for n in (0, 1, 2):
            rs_part(n, mob, wom_v, x_h, rh_s, rh_r, heads)
        rs_first(*head_set)
    with scope("rs_second_head"):
        rs_part(3, mob, wom_v, x_h, rh_s, rh_r, heads)
        rs_second(*head_set)
    ss[me] = sqcol[...].T[0:1]
    for k in range(1, NTP):
        send(ss.at[me], ss.at[me], ss_s.at[k], ss_r.at[k], lax.rem(me + k, NTP))
    with scope("rs_mid_head"):
        rs_mid(*head_set)
    for k in range(1, NTP):
        got(ss.at[lax.rem(me + NTP - k, NTP)], ss_r.at[k], "w_ss")
    total = ss[0]
    for k in range(1, NTP):
        total = total + ss[k]
    factor = lax.rsqrt(total / (NTP * VAL) + EPS)
    scol[...] = jnp.broadcast_to(factor, (128, BLK)).T
    for k in range(4):
        got(gr_c.at[k], rc_r.at[6 + k], "w_gc")
    factor = scol[pl.ds(pl.multiple_of(me * ROWS, 8), ROWS), 0:1]
    for k in range(2):
        cs = slice(k * COLS, (k + 1) * COLS)
        conv_sum = own_c[:, cs] + gr_c[k].astype(f32) + gr_c[2 + k].astype(f32)
        own_c[:, cs] = conv_sum + factor * own_h[:, cs]
    for k in (1, 2, 0, 3):
        got(gr_h.at[k], rh_r.at[6 + k], "w_gh")
    with scope("final"):
        for k in range(2):
            cs = slice(k * COLS, (k + 1) * COLS)
            rest_sum = gr_h[k].astype(f32) + gr_h[2 + k].astype(f32)
            out[:, cs] = (own_c[:, cs] + factor * rest_sum).astype(bf16)

    for cp in sends:
        cp.wait_send()
    def sent(ref, sem):
        pltpu.make_async_remote_copy(
            src_ref=ref, dst_ref=ref, send_sem=sem, recv_sem=sem,
            device_id=(sp, sib), device_id_type=MESH,
        ).wait_send()

    @pl.when(sp < n_sp - 1)
    def _():
        edge.wait_send()

    for g, (lo, hi) in enumerate(groups):

        @pl.when(in_group(g))
        def _(g=g, lo=lo, hi=hi):
            if hi - lo > 1:
                rest = pl.ds(0, TILES - TILES // (hi - lo))
                sent(st.at[rest], st_s)
                sent(aux.at[pl.ds(0, hi - lo - 1)], aux_s)
                sent(cr.at[rest], cr_s)
            for cp in pass_on(g):
                cp.wait_send()


def solution(mesh):
    n_sp = mesh.shape["sp"]
    groups = groups_of(n_sp)
    gmax = max(hi - lo for lo, hi in groups)
    tmax = max(TILES // (hi - lo) for lo, hi in groups)
    vmem = pl.BlockSpec(memory_space=pltpu.VMEM)
    hbm = pl.BlockSpec(memory_space=pl.ANY)
    dma = pltpu.SemaphoreType.DMA

    def rs_bufs():
        return [
            pltpu.VMEM((4, ROWS, CH), bf16),
            pltpu.VMEM((2, ROWS, COLS), bf16),
            pltpu.VMEM((2, ROWS, COLS), bf16),
            pltpu.VMEM((4, ROWS, COLS), bf16),
            pltpu.VMEM((4, ROWS, COLS), bf16),
        ]

    scratch = [
        pltpu.VMEM((ROWS, D), bf16),
        pltpu.VMEM((1, D), f32),
        pltpu.VMEM((NTP, D), bf16),
        pltpu.VMEM((NTP, D), bf16),
        pltpu.VMEM((1, NTP), f32),
        pltpu.VMEM((1, BLK), f32),
        pltpu.VMEM((3, NTP * CH), f32),
        pltpu.VMEM((KEY, VAL), f32),
        pltpu.VMEM((1, KEY), f32),
        pltpu.VMEM((BLK, D), bf16),
        pltpu.VMEM((D, 1408), bf16),
        pltpu.VMEM((2 * VAL, D), bf16),
        pltpu.VMEM((2 * CH, D), bf16),
        pltpu.VMEM((BLK, 1280), bf16),
        pltpu.VMEM((BLK, 128), f32),
        pltpu.VMEM((8, BLK), f32),
        pltpu.VMEM((BLK, 128), f32),
        pltpu.VMEM((TILES, 16, 128), bf16),
        pltpu.VMEM((gmax, tmax, 16, 128), bf16),
        pltpu.VMEM((n_sp, 1, 384), f32),
        pltpu.VMEM((gmax, tmax, 16, 128), bf16),
        pltpu.VMEM((TILES, 16, 128), bf16),
        pltpu.VMEM((gmax, 1, 128), f32),
        pltpu.VMEM((gmax, 1, 128), f32),
        pltpu.VMEM((1, 128), f32),
        pltpu.VMEM((1, 128), f32),
        pltpu.VMEM((tmax, 16, 128), f32),
        pltpu.VMEM((1, 256), f32),
        pltpu.VMEM((tmax, 16, 128), f32),
        pltpu.VMEM((1, 256), f32),
        pltpu.VMEM((KEY, VAL), bf16),
        pltpu.VMEM((BLK, VAL), f32),
        pltpu.VMEM((BLK, 128), f32),
        pltpu.VMEM((BLK, VAL), bf16),
        pltpu.VMEM((BLK, CH), bf16),
        pltpu.VMEM((BLK + 8, CH), f32),
        pltpu.VMEM((16, CH), bf16),
        pltpu.VMEM((16, CH), bf16),
        pltpu.VMEM((NTP, 1, BLK), f32),
        pltpu.VMEM((BLK, 128), f32),
        pltpu.VMEM((BLK, 128), f32),
        pltpu.VMEM((ROWS, D), f32),
        pltpu.VMEM((ROWS, D), f32),
        pltpu.VMEM((2, ROWS, COLS), f32),
        *rs_bufs(),
        *rs_bufs(),
        dma((8,)),
        dma((9,)),
        dma((13,)),
        dma((13,)),
        dma(()),
        dma(()),
        dma(()),
        dma(()),
        dma(()),
        dma(()),
        dma(()),
        dma(()),
        dma((NTP,)),
        dma((NTP,)),
        dma((10,)),
        dma((10,)),
        dma((10,)),
        dma((10,)),
        dma((4,)),
        dma(()),
        dma((4,)),
        dma(()),
        pltpu.SemaphoreType.REGULAR,
        pltpu.SemaphoreType.REGULAR,
        dma((2,)),
        dma((2,)),
    ]

    def per_device(
        tokens, in_gain, w_query, w_key, w_value, w_input_gate, w_forget_gate, forget_bias,
        forget_extra, w_conv_gate, w_conv_left, w_conv_right, conv_taps, first_memory,
        first_norm, w_out_memory, w_out_conv,
    ):
        return pl.pallas_call(
            functools.partial(kernel, n_sp),
            out_shape=jax.ShapeDtypeStruct((ROWS, D), bf16),
            in_specs=[hbm] * 17,
            out_specs=vmem,
            scratch_shapes=scratch,
            compiler_params=pltpu.CompilerParams(
                collective_id=0, has_side_effects=True, vmem_limit_bytes=60 * 1024 * 1024
            ),
        )(
            tokens, in_gain.reshape(1, D), w_input_gate.T, w_forget_gate.T,
            forget_bias.reshape(1, NTP),
            forget_extra.reshape(1, BLK), conv_taps, first_memory.reshape(KEY, VAL), first_norm,
            w_query, w_key, w_value, w_conv_gate, w_conv_left, w_conv_right,
            w_out_memory, w_out_conv,
        )

    placed = (
        P(("sp", "tp"), None),
        P(),
        P(None, "tp"),
        P(None, "tp"),
        P(None, "tp"),
        P(),
        P(),
        P(),
        P("sp", "tp"),
        P(None, "tp"),
        P(None, "tp"),
        P(None, "tp"),
        P(),
        P("tp", None, None),
        P("tp", None),
        P("tp", None),
        P("tp", None),
    )
    return jax.shard_map(
        per_device, mesh=mesh, in_specs=placed, out_specs=P(("sp", "tp"), None), check_vma=False
    )
```

```python
import functools

import jax
import jax.numpy as jnp
from jax import lax
from jax.experimental import pallas as pl
from jax.experimental.pallas import tpu as pltpu
from jax.sharding import PartitionSpec as P

D = 2048
KEY = 128
VAL = 256
CH = 256
ROWS = 96
HALF = 48
BLK = 768
NTP = 8
TILES = 16
COLS = 1024
AG_SLOT = (0, 1, 2, 3, 4, 5, 6, 7, 7, 8, 8, 9, 9)
EPS = 1e-06
SCALE = KEY ** (-0.5)
MESH = pl.DeviceIdType.MESH
f32 = jnp.float32
bf16 = jnp.bfloat16


def nt_dot(a, b):
    return lax.dot_general(a, b, (((1,), (1,)), ((), ())), preferred_element_type=f32)


def groups_of(n_sp):
    if n_sp == 32:
        return ((0, 8), (8, 16), (16, 32))
    if n_sp == 4:
        return ((0, 2), (2, 4))
    return ((0, n_sp),)


def dot(a, b):
    return jnp.dot(a, b, preferred_element_type=f32)


def kernel(
    n_sp,
    tok_h, gain_h, wi_h, wf_h, bias_h, fextra_h, taps_h, fmem_h, fnorm_h,
    wq, wk, wv, wcg, wcl, wcr, wom, woc,
    out_h,
    tok, gain, wi, wf, bias, fextra, taps, fmem, fnorm,
    x, w_all, wom_v, woc_v,
    proj, gates, urow, cmcol, st, rv, aux, cv, cr, mh, nh, m_at, n_at,
    ex, ea, px, pa, cmem, pv, rs,
    mob, cbr, prod, eb, er, ss, scol, sqcol, own_c, own_h, part, out,
    x_c, fs_c, fr_c, gs_c, gr_c,
    x_h, fs_h, fr_h, gs_h, gr_h,
    wsem, isem, ag_s, ag_r, aux_s, aux_r, st_s, st_r, cr_s, cr_r, ed_s, ed_r, ss_s, ss_r,
    rc_s, rc_r, rh_s, rh_r, ex_s, px_r, ea_s, pa_r, ready, ready_edge, ow_s, ow_r, out_s,
):
    groups = groups_of(n_sp)
    scope = jax.named_scope
    sp = lax.axis_index("sp")
    me = lax.axis_index("tp")
    y = me // 2
    c = lax.rem(me, 2)
    sib = me + 1 - 2 * c
    yn_y, yp_y, yo_y = lax.rem(y + 1, 4), lax.rem(y + 3, 4), lax.rem(y + 2, 4)
    yn, yp = yn_y * 2 + c, yp_y * 2 + c

    def in_group(g):
        return jnp.logical_and(sp >= groups[g][0], sp < groups[g][1])

    def mates(g, start):
        lo, hi = groups[g]
        n = hi - lo
        for k in range(1, n):
            far = n // 2 + (k // 2 if k % 2 else -(k // 2))
            start(lo + lax.rem(sp - lo + far, n))

    def following(g):
        lo, hi = groups[g]
        if g + 1 == len(groups):
            return []
        at, end = groups[g + 1]
        ratio = (end - at) // (hi - lo)
        return [at + (sp - lo) * ratio + q for q in range(ratio)]

    def preceding(g):
        lo, hi = groups[g]
        at, end = groups[g - 1]
        return at + (sp - lo) // ((hi - lo) // (end - at))

    inputs = [
        pltpu.make_async_copy(src, dst, isem.at[i])
        for i, (src, dst) in enumerate(
            [
                (tok_h, tok), (gain_h, gain), (wi_h, wi), (wf_h, wf), (bias_h, bias),
                (fextra_h, fextra), (taps_h, taps), (fmem_h, fmem), (fnorm_h, fnorm),
            ]
        )
    ]
    weights = [
        pltpu.make_async_copy(src, dst, wsem.at[i // 6])
        for i, (src, dst) in enumerate(
            [
                (wk, w_all.at[:, pl.ds(0, 128)]),
                (wq, w_all.at[:, pl.ds(128, 128)]),
                (wv, w_all.at[:, pl.ds(256, 256)]),
                (wcl, w_all.at[:, pl.ds(512, 256)]),
                (wcr, w_all.at[:, pl.ds(768, 256)]),
                (wcg, w_all.at[:, pl.ds(1024, 256)]),
                (woc, woc_v.at[pl.ds(0, CH), :]),
                (wom, wom_v.at[pl.ds(0, VAL), :]),
            ]
        )
    ]
    for cp in inputs[:4]:
        cp.start()
    barrier = pltpu.get_barrier_semaphore()
    for k in range(1, NTP):
        pl.semaphore_signal(
            barrier, inc=1, device_id=(sp, lax.rem(me + k, NTP)), device_id_type=MESH
        )

    def greet(p):
        pl.semaphore_signal(barrier, inc=1, device_id=(p, me), device_id_type=MESH)

    for g, (lo, hi) in enumerate(groups):

        @pl.when(in_group(g))
        def _(g=g):
            mates(g, greet)
            for p in following(g):
                greet(p)

        if hi < n_sp:

            @pl.when(sp == hi - 1)
            def _():
                greet(sp + 1)

    for cp in inputs[4:]:
        cp.start()
    for w in weights:
        w.start()

    def slots(s, n=1):
        return x.at[pl.ds(pl.multiple_of(s * HALF, 16), n * HALF), :]

    with scope("norm"):
        inputs[0].wait()
        inputs[1].wait()
        t = tok[...].astype(f32)
        scale = lax.rsqrt(jnp.mean(t * t, axis=1, keepdims=True) + EPS)
        x[pl.ds(pl.multiple_of(c * ROWS, 16), ROWS), :] = (t * scale * gain[...]).astype(bf16)
    prod[0:8, :] = jnp.zeros((8, CH), f32)

    with scope("w_barrier"):
        for g, (lo, hi) in enumerate(groups):
            count = NTP - 1 + hi - lo - 1 + (1 if lo else 0)

            @pl.when(jnp.logical_and(in_group(g), jnp.logical_or(sp != lo, lo == 0)))
            def _(count=count):
                pl.semaphore_wait(barrier, count)

            if lo:

                @pl.when(sp == lo)
                def _(count=count):
                    pl.semaphore_wait(barrier, count + 1)

    def send(src, dst, ssem, rsem, peer):
        cp = pltpu.make_async_remote_copy(
            src_ref=src, dst_ref=dst, send_sem=ssem, recv_sem=rsem,
            device_id=(sp, peer), device_id_type=MESH,
        )
        cp.start()

    def got(dst, rsem, name="w"):
        with scope(name):
            pltpu.make_async_remote_copy(
                src_ref=dst, dst_ref=dst, send_sem=rsem, recv_sem=rsem,
                device_id=(sp, sib), device_id_type=MESH,
            ).wait_recv()

    def ag(src, dst, k, peer, n=1):
        send(slots(src, n), slots(dst, n), ag_s, ag_r.at[AG_SLOT[k]], peer)

    other = 1 - c
    ag(2 * c, 4 + c, 0, yn)
    ag(2 * c + 1, 6 + c, 3, yp)
    ag(2 * c + 1, 8 + c, 1, yn)
    ag(2 * c, 10 + c, 4, yp)
    ag(2 * c, 2 * c, 6, sib, 2)
    send(woc, woc_v.at[pl.ds(CH, CH), :], ow_s, ow_r, sib)
    send(wom, wom_v.at[pl.ds(VAL, VAL), :], ow_s, ow_r, sib)
    def tell(sem, p):
        pl.semaphore_signal(sem, inc=1, device_id=(p, me), device_id_type=MESH)

    for g, (lo, hi) in enumerate(groups):
        if lo:

            @pl.when(in_group(g))
            def _(g=g):
                tell(ready, preceding(g))

            @pl.when(sp == lo)
            def _():
                tell(ready_edge, sp - 1)

    for cp in inputs[2:]:
        cp.wait()
    gw = jnp.concatenate(
        [wi[...].astype(f32), wf[...].astype(f32), jnp.zeros((112, D), f32)], axis=0
    )
    w_all[:, 1280:1408] = gw.T.astype(bf16)
    with scope("w_weights"):
        pltpu.make_async_copy(w_all.at[:, 0:1280], w_all.at[:, 0:1280], wsem.at[0]).wait()

    def project_rows(xs, bases, n, parts):
        for lo, hi in parts:
            res = dot(xs, w_all[:, lo:hi])
            for k, base in enumerate(bases):
                rows = pl.ds(pl.multiple_of(base, 16), n)
                piece = res[k * n : (k + 1) * n]
                if lo == 512:
                    left = piece[:, :CH].astype(bf16).astype(f32)
                    right = piece[:, CH:].astype(bf16).astype(f32)
                    at = pl.ds(pl.multiple_of(base + 8, 8), n)
                    prod[at, :] = (left * right).astype(bf16).astype(f32)
                elif hi <= 1280:
                    proj[rows, lo:hi] = piece.astype(bf16)
                else:
                    gates[rows, :] = piece[:, 1280 - lo :]
                    if lo < 1280:
                        proj[rows, lo:1280] = piece[:, : 1280 - lo].astype(bf16)

    def project(stage, bases, parts):
        project_rows(x[stage * 192 : stage * 192 + 192, :], bases, HALF, parts)

    edge = pltpu.make_async_remote_copy(
        src_ref=eb, dst_ref=er, send_sem=ed_s, recv_sem=ed_r,
        device_id=(lax.rem(sp + 1, n_sp), me), device_id_type=MESH,
    )

    def send_edge(where):
        @pl.when(jnp.logical_and(y == where, sp < n_sp - 1))
        def _():
            eb[...] = prod[BLK - 8 :, :].astype(bf16)
            for lo, hi in groups[:-1]:

                @pl.when(sp == hi - 1)
                def _():
                    pl.semaphore_wait(ready_edge, 1)

            edge.start()

    def own(d):
        return pl.ds(pl.multiple_of((d * 2 + c) * ROWS, 16), ROWS)

    def his(d):
        return pl.ds(pl.multiple_of((d * 2 + 1 - c) * ROWS, 16), ROWS)

    order = (yo_y, yn_y, yp_y, y)

    def rs_part(n, a, w, xb, s_, r_, prepare):
        prepare(order[n], other)
        send(a.at[his(order[n])], xb.at[n], s_, r_.at[0 if n == 0 else 1], sib)
        prepare(order[n], c)

    def both(n, a, xb):
        return jnp.concatenate([a[own(order[n]), :], xb[n]], axis=1)

    def rs_first(a, w, xb, fs, fr, gs, gr, kept, s_, r_):
        got(xb.at[0], r_.at[0], "w_x0")
        lhs = both(0, a, xb)
        for k, peer in ((0, yn), (1, yp)):
            fs[k] = dot(lhs, w[:, k * COLS : (k + 1) * COLS]).astype(bf16)
            send(fs.at[k], fr.at[k], s_, r_.at[2 + k], peer)

    def rs_second(a, w, xb, fs, fr, gs, gr, kept, s_, r_):
        got(xb.at[pl.ds(1, 3)], r_.at[1], "w_x123")
        lhs = jnp.concatenate([both(n, a, xb) for n in (1, 2, 3)], axis=0)
        res = dot(lhs, w[:, COLS:])
        gs[1] = res[0:ROWS].astype(bf16)
        send(gs.at[1], gr.at[1], s_, r_.at[4], yn)
        part[1] = res[ROWS : 2 * ROWS]
        kept[:, COLS:] = res[2 * ROWS :]
        res = dot(lhs, w[:, :COLS])
        gs[2] = res[ROWS : 2 * ROWS].astype(bf16)
        send(gs.at[2], gr.at[2], s_, r_.at[4], yp)
        part[0] = res[0:ROWS]
        kept[:, :COLS] = res[2 * ROWS :]

    def rs_mid(a, w, xb, fs, fr, gs, gr, kept, s_, r_):
        got(fr.at[0], r_.at[2], "w_f0")
        gs[0] = (part[0] + fr[0].astype(f32)).astype(bf16)
        send(gs.at[0], gr.at[0], s_, r_.at[4], yn)
        got(fr.at[1], r_.at[3], "w_f1")
        gs[3] = (part[1] + fr[1].astype(f32)).astype(bf16)
        send(gs.at[3], gr.at[3], s_, r_.at[4], yp)

    def filtered(d, core):
        @pl.when(jnp.logical_and(jnp.logical_and(d == 0, core == 0), sp > 0))
        def _():
            with scope("w_edge"):
                edge.wait_recv()
            prod[0:8, :] = er[8:16, :].astype(f32)

        at = (d * 2 + core) * ROWS
        rows = pl.ds(pl.multiple_of(at, 16), ROWS)
        mine = pl.ds(pl.multiple_of(me * CH, CH), CH)
        near = prod[pl.ds(pl.multiple_of(at, 16), ROWS + 8), :]
        f = taps[0:1, mine] * near[6 : 6 + ROWS]
        f = f + taps[1:2, mine] * near[7 : 7 + ROWS]
        f = f + taps[2:3, mine] * near[8 : 8 + ROWS]
        cbr[rows, :] = (proj[rows, 1024:1280].astype(f32) * f).astype(bf16)

    conv_set = (cbr, woc_v, x_c, fs_c, fr_c, gs_c, gr_c, own_c, rc_s, rc_r)
    head_set = (mob, wom_v, x_h, fs_h, fr_h, gs_h, gr_h, own_h, rh_s, rh_r)

    def conv_part(n):
        rs_part(n, cbr, woc_v, x_c, rc_s, rc_r, filtered)

    every = ((0, 512), (512, 1024), (1024, 1408))
    got(slots(2 * other, 2), ag_r.at[6], "w_ag6")
    with scope("proj_0"):
        project(0, [y * 192 + HALF * k for k in range(4)], every)
        send_edge(3)
    got(slots(4 + c), ag_r.at[0], "w_ag0")
    ag(4 + c, 12 + 2 * c, 2, yn)
    ag(4 + c, 4 + c, 7, sib)
    got(slots(6 + c), ag_r.at[3], "w_ag3")
    ag(6 + c, 13 + 2 * c, 5, yp)
    ag(6 + c, 6 + c, 8, sib)
    got(slots(0, 2), ag_r.at[7], "w_ag7")
    with scope("proj_1"):
        project(
            1,
            [yp_y * 192, yp_y * 192 + ROWS, yn_y * 192 + HALF, yn_y * 192 + ROWS + HALF],
            every,
        )
        send_edge(2)
    got(slots(8 + c), ag_r.at[1], "w_ag1")
    ag(8 + c, 8 + c, 9, sib)
    got(slots(10 + c), ag_r.at[4], "w_ag4")
    ag(10 + c, 10 + c, 10, sib)
    got(slots(0, 2), ag_r.at[8], "w_ag9")
    with scope("proj_2"):
        project(
            2,
            [yp_y * 192 + HALF, yp_y * 192 + ROWS + HALF, yn_y * 192, yn_y * 192 + ROWS],
            every,
        )
        send_edge(0)
    got(slots(12 + 2 * c), ag_r.at[2], "w_ag2")
    ag(12 + 2 * c, 12 + 2 * c, 11, sib)
    got(slots(13 + 2 * c), ag_r.at[5], "w_ag5")
    ag(13 + 2 * c, 13 + 2 * c, 12, sib)
    with scope("conv_early"):
        conv_part(1)
    keys, rest = ((1280, 1408), (0, 512)), ((512, 1024), (1024, 1280))

    def project_last(core, parts):
        xs = x[pl.ds(pl.multiple_of(576 + core * ROWS, 16), ROWS), :]
        project_rows(xs, [yo_y * 192 + core * ROWS], ROWS, parts)

    with scope("proj_3own"):
        project_last(c, keys + rest)
    got(slots(0, 2), ag_r.at[9], "w_ag12")
    with scope("proj_3"):
        project_last(other, keys)

    with scope("state"):
        g_t = gates[...].T
        sub = lax.broadcasted_iota(jnp.int32, (8, BLK), 0)
        lane = lax.broadcasted_iota(jnp.int32, (8, BLK), 1)
        in_row = jnp.sum(jnp.where(sub == me, g_t[0:8], 0.0), axis=0, keepdims=True)
        f_row = jnp.sum(jnp.where(sub == me, g_t[8:16], 0.0), axis=0, keepdims=True)
        lane8 = lax.broadcasted_iota(jnp.int32, (1, NTP), 1)
        f_row = f_row + jnp.sum(jnp.where(lane8 == me, bias[...], 0.0), axis=1, keepdims=True)
        log_forget = (
            jnp.minimum(f_row, 0.0) - jnp.log1p(jnp.exp(-jnp.abs(f_row))) + fextra[...]
        )

        def stacked(row):
            parts = [row[:, 128 * k : 128 * k + 128] for k in range(6)]
            return jnp.concatenate(parts + [jnp.zeros((2, 128), f32)], axis=0)

        lf6 = stacked(log_forget)
        l_1 = lf6.astype(bf16).astype(f32)
        l_2 = (lf6 - l_1).astype(bf16).astype(f32)
        l_3 = lf6 - l_1 - l_2
        upto = lax.broadcasted_iota(jnp.int32, (128, 128), 0) <= lax.broadcasted_iota(
            jnp.int32, (128, 128), 1
        )
        sums = dot(
            jnp.concatenate([l_1, l_2, l_3, jnp.zeros((8, 128), f32)], axis=0).astype(bf16),
            jnp.where(upto, 1.0, 0.0).astype(bf16),
        )
        inside = sums[0:8] + sums[8:16] + sums[16:24]
        sub8 = lax.broadcasted_iota(jnp.int32, (8, 128), 0)
        ends = jnp.broadcast_to(inside[:, 127:128], (8, 128))
        before = jnp.where(sub8 >= 1, pltpu.roll(ends, 1, 0), 0.0)
        for s in (1, 2, 4):
            before = before + jnp.where(sub8 >= s, pltpu.roll(before, s, 0), 0.0)
        cum6 = inside + before
        u6 = jnp.where(sub8 < 6, stacked(in_row) - cum6, -jnp.inf)
        u_max = jnp.max(jnp.max(u6, axis=1, keepdims=True), axis=0, keepdims=True)
        decay = cum6[5:6, 127:128]

        def unstacked(a):
            return jnp.concatenate([a[k : k + 1] for k in range(6)], axis=1)

        u_row = unstacked(u6)
        k_t = proj[:, 0:128].astype(f32).T
        keyed = k_t * jnp.exp(u_row - u_max)
        mem = dot(keyed.astype(bf16), proj[:, 256:512])
        norm_col = jnp.sum(keyed, axis=1, keepdims=True)
        block_norm = jnp.broadcast_to(norm_col, (128, 128)).T[0:1]
        d_lanes = jnp.broadcast_to(decay, (1, 128))
        m_lanes = jnp.broadcast_to(decay + u_max, (1, 128))
        aux[sp] = jnp.concatenate([d_lanes, m_lanes, block_norm], axis=1)
        for p in range(TILES):
            i, j = p // 2, p % 2
            st[p] = mem[16 * i : 16 * i + 16, 128 * j : 128 * j + 128].astype(bf16)

    def start_state(g, p):
        lo, hi = groups[g]
        n = TILES // (hi - lo)
        pltpu.make_async_remote_copy(
            src_ref=st.at[pl.ds((p - lo) * n, n)], dst_ref=rv.at[sp - lo, pl.ds(0, n)],
            send_sem=st_s, recv_sem=st_r, device_id=(p, me), device_id_type=MESH,
        ).start()
        pltpu.make_async_remote_copy(
            src_ref=aux.at[sp], dst_ref=aux.at[sp], send_sem=aux_s, recv_sem=aux_r,
            device_id=(p, me), device_id_type=MESH,
        ).start()

    with scope("send_state"):
        for g, (lo, hi) in enumerate(groups):

            @pl.when(in_group(g))
            def _(g=g, lo=lo, hi=hi):
                mates(g, functools.partial(start_state, g))
                n = TILES // (hi - lo)
                for k in range(n):
                    rv[sp - lo, k] = st[(sp - lo) * n + k]

    with scope("proj_lrg"):
        project_last(other, rest)
        send_edge(1)

    def start_carry(g, p):
        lo, hi = groups[g]
        n = TILES // (hi - lo)
        pltpu.make_async_remote_copy(
            src_ref=cv.at[p - lo, pl.ds(0, n)], dst_ref=cr.at[pl.ds((sp - lo) * n, n)],
            send_sem=cr_s, recv_sem=cr_r, device_id=(p, me), device_id_type=MESH,
        ).start()

    def pass_on(g):
        lo, hi = groups[g]
        out_ = []
        for q, p in enumerate(following(g)):
            n = TILES // (groups[g + 1][1] - groups[g + 1][0])
            out_ += [
                pltpu.make_async_remote_copy(
                    src_ref=ex.at[pl.ds(q * n, n)], dst_ref=px.at[pl.ds(0, n)],
                    send_sem=ex_s.at[q], recv_sem=px_r, device_id=(p, me), device_id_type=MESH,
                ),
                pltpu.make_async_remote_copy(
                    src_ref=ea, dst_ref=pa, send_sem=ea_s.at[q], recv_sem=pa_r,
                    device_id=(p, me), device_id_type=MESH,
                ),
            ]
        return out_

    def recurrence(g):
        lo, hi = groups[g]
        n = TILES // (hi - lo)
        with scope("w_state"):
            if hi - lo > 1:
                got(aux.at[pl.ds(0, hi - lo - 1)], aux_r)
                got(rv.at[pl.ds(0, hi - lo - 1), pl.ds(0, n)], st_r)
        if lo:
            with scope("w_prefix"):
                got(px.at[pl.ds(0, n)], px_r)
                got(pa, pa_r)
            tiles = [px[k] for k in range(n)]
            run_m = pa[:, 0:128]
            run_n = pa[:, 128:256]
        else:
            tiles = []
            for k in range(n):
                p = (sp - lo) * n + k
                r_i = pl.ds(pl.multiple_of((p // 2) * 16, 16), 16)
                c_i = pl.ds(pl.multiple_of(lax.rem(p, 2) * 128, 128), 128)
                tiles.append(fmem[r_i, c_i])
            run_m = jnp.zeros((1, 128), f32)
            run_n = fnorm[...]
        last_one = hi == n_sp
        for b in range(lo, hi):
            for k in range(n):
                cv[b - lo, k] = tiles[k].astype(bf16)
            mh[b - lo] = run_m
            nh[b - lo] = run_n
            if b < hi - 1 or not last_one:
                row = aux[b]
                new_m = jnp.maximum(run_m + row[:, 0:128], row[:, 128:256])
                old = jnp.exp(run_m + row[:, 0:128] - new_m)
                new = jnp.exp(row[:, 128:256] - new_m)
                tiles = [old * tiles[k] + new * rv[b - lo, k].astype(f32) for k in range(n)]
                run_n = old * run_n + new * row[:, 256:384]
                run_m = new_m
        if not last_one:
            for k in range(n):
                ex[k] = tiles[k]
            ea[...] = jnp.concatenate([run_m, run_n], axis=1)
            with scope("w_ready"):
                pl.semaphore_wait(ready, len(following(g)))
            for cp in pass_on(g):
                cp.start()
        with scope("send_carry"):
            mates(g, functools.partial(start_carry, g))
        for k in range(n):
            cr[(sp - lo) * n + k] = cv[sp - lo, k]
        m_at[...] = mh[sp - lo]
        n_at[...] = nh[sp - lo]

    def take(g):
        @pl.when(in_group(g))
        def _():
            recurrence(g)

    with scope("rs_first_conv"):
        conv_part(0)
        conv_part(3)
        pltpu.make_async_copy(woc_v, woc_v, wsem.at[1]).wait()
        got(woc_v, ow_r)
        top = jnp.broadcast_to(u_row, (8, BLK))
        urow[...] = top
        for s in (1, 2, 4, 8, 16, 32, 64, 128, 256, 512):
            top = jnp.maximum(top, jnp.where(lane >= s, pltpu.roll(top, s, 1), -jnp.inf))
        cols = jnp.concatenate([top, jnp.zeros((120, BLK), f32)], axis=0).T
        cmcol[...] = jnp.broadcast_to(cols[:, 0:1], (BLK, 128))
        rs_first(*conv_set)
    def mixing():
        for rb in range(3):
            r0 = rb * 256
            q = proj[r0 : r0 + 256, 128:256]
            cm = cmcol[r0 : r0 + 256, 0:1]
            acc = jnp.zeros((256, VAL), f32)
            tot = jnp.zeros((256, 1), f32)
            for cb in range(rb + 1):
                c0 = cb * 256
                mix = nt_dot(q, proj[c0 : c0 + 256, 0:128]) * SCALE
                mix = mix * jnp.exp(urow[0:1, c0 : c0 + 256] - cm)
                if cb == rb:
                    ri = lax.broadcasted_iota(jnp.int32, (256, 256), 0)
                    ci = lax.broadcasted_iota(jnp.int32, (256, 256), 1)
                    mix = jnp.where(ri >= ci, mix, 0.0)
                tot = tot + jnp.sum(mix, axis=1, keepdims=True)
                acc = acc + dot(mix.astype(bf16), proj[c0 : c0 + 256, 256:512])
            pv[r0 : r0 + 256, :] = acc
            rs[r0 : r0 + 256, :] = jnp.broadcast_to(tot, (256, 128))

    last_group = in_group(len(groups) - 1)
    for g in range(len(groups) - 1):
        take(g)

    @pl.when(last_group)
    def _():
        with scope("mixing"):
            mixing()

    with scope("rs_second_conv"):
        conv_part(2)
        rs_second(*conv_set)

    @pl.when(jnp.logical_not(last_group))
    def _():
        with scope("mixing"):
            mixing()

    take(len(groups) - 1)
    with scope("rs_mid_conv"):
        rs_mid(*conv_set)

    for g, (lo, hi) in enumerate(groups):

        @pl.when(in_group(g))
        def _(lo=lo, hi=hi):
            got(cr.at[pl.ds(0, TILES - TILES // (hi - lo))], cr_r, "w_carry")

    with scope("carry"):
        for p in range(TILES):
            i, j = p // 2, p % 2
            cmem[16 * i : 16 * i + 16, 128 * j : 128 * j + 128] = cr[p]
        carry = cmem[...]
        m_in = m_at[:, 0:1]
        n_in = n_at[...]
        n_1 = n_in.astype(bf16).astype(f32)
        n_2 = (n_in - n_1).astype(bf16).astype(f32)
        n_3 = n_in - n_1 - n_2
        sub16 = lax.broadcasted_iota(jnp.int32, (16, 128), 0)
        n_rows = jnp.where(
            sub16 == 0, n_1, jnp.where(sub16 == 1, n_2, jnp.where(sub16 == 2, n_3, 0.0))
        ).astype(bf16)

    def heads(d, core):
        rows = pl.ds(pl.multiple_of((d * 2 + core) * ROWS, 16), ROWS)
        q = proj[rows, 128:256]
        cm = cmcol[rows, 0:1]
        peak = jnp.maximum(cm, m_in)
        f_in = jnp.exp(cm - peak)
        f_carry = jnp.exp(m_in - peak)
        from_memory = dot(q, carry) * SCALE
        from_norm = jnp.sum(nt_dot(q, n_rows), axis=1, keepdims=True) * SCALE
        num = f_in * pv[rows, :] + f_carry * from_memory
        den = f_in * rs[rows, 0:1] + f_carry * from_norm
        memory_out = num / jnp.maximum(jnp.abs(den), 1.0)
        squares = jnp.sum(memory_out * memory_out, axis=1, keepdims=True)
        sqcol[rows, :] = jnp.broadcast_to(squares, (ROWS, 128))
        mob[rows, :] = memory_out.astype(bf16)

    with scope("rs_first_head"):
        for n in (0, 1, 2):
            rs_part(n, mob, wom_v, x_h, rh_s, rh_r, heads)
        rs_first(*head_set)
    with scope("rs_second_head"):
        rs_part(3, mob, wom_v, x_h, rh_s, rh_r, heads)
        rs_second(*head_set)
    ss[me] = sqcol[...].T[0:1]
    for k in range(1, NTP):
        send(ss.at[me], ss.at[me], ss_s, ss_r, lax.rem(me + k, NTP))
    with scope("rs_mid_head"):
        rs_mid(*head_set)
    got(ss.at[pl.ds(0, NTP - 1)], ss_r, "w_ss")
    total = ss[0]
    for k in range(1, NTP):
        total = total + ss[k]
    factor = lax.rsqrt(total / (NTP * VAL) + EPS)
    scol[...] = jnp.broadcast_to(factor, (128, BLK)).T
    got(gr_c, rc_r.at[4], "w_gc")
    factor = scol[pl.ds(pl.multiple_of(me * ROWS, 8), ROWS), 0:1]
    for k in range(2):
        cs = slice(k * COLS, (k + 1) * COLS)
        conv_sum = own_c[:, cs] + gr_c[k].astype(f32) + gr_c[2 + k].astype(f32)
        own_c[:, cs] = conv_sum + factor * own_h[:, cs]
    got(gr_h, rh_r.at[4], "w_gh")
    outs = []
    with scope("final"):
        for k in range(2):
            cs = slice(k * COLS, (k + 1) * COLS)
            rest_sum = gr_h[k].astype(f32) + gr_h[2 + k].astype(f32)
            out[:, cs] = (own_c[:, cs] + factor * rest_sum).astype(bf16)
            outs.append(pltpu.make_async_copy(out.at[:, cs], out_h.at[:, cs], out_s.at[k]))
            outs[k].start()

    def sent(ref, sem):
        pltpu.make_async_remote_copy(
            src_ref=ref, dst_ref=ref, send_sem=sem, recv_sem=sem,
            device_id=(sp, sib), device_id_type=MESH,
        ).wait_send()

    with scope("w_sends"):
        sent(x.at[pl.ds(0, 14 * HALF), :], ag_s)
        sent(woc_v, ow_s)
        sent(x.at[pl.ds(0, 336), :], rc_s)
        sent(x.at[pl.ds(0, 336), :], rh_s)
        sent(ss.at[pl.ds(0, NTP - 1)], ss_s)

    @pl.when(sp < n_sp - 1)
    def _():
        edge.wait_send()

    for g, (lo, hi) in enumerate(groups):

        @pl.when(in_group(g))
        def _(g=g, lo=lo, hi=hi):
            if hi - lo > 1:
                rest = pl.ds(0, TILES - TILES // (hi - lo))
                sent(st.at[rest], st_s)
                sent(aux.at[pl.ds(0, hi - lo - 1)], aux_s)
                sent(cr.at[rest], cr_s)
            for cp in pass_on(g):
                cp.wait_send()

    with scope("w_out"):
        for cp in outs:
            cp.wait()


def solution(mesh):
    n_sp = mesh.shape["sp"]
    groups = groups_of(n_sp)
    gmax = max(hi - lo for lo, hi in groups)
    tmax = max(TILES // (hi - lo) for lo, hi in groups)
    hbm = pl.BlockSpec(memory_space=pl.ANY)
    dma = pltpu.SemaphoreType.DMA

    def rs_bufs():
        return [
            pltpu.VMEM((4, ROWS, CH), bf16),
            pltpu.VMEM((2, ROWS, COLS), bf16),
            pltpu.VMEM((2, ROWS, COLS), bf16),
            pltpu.VMEM((4, ROWS, COLS), bf16),
            pltpu.VMEM((4, ROWS, COLS), bf16),
        ]

    scratch = [
        pltpu.VMEM((ROWS, D), bf16),
        pltpu.VMEM((1, D), f32),
        pltpu.VMEM((NTP, D), bf16),
        pltpu.VMEM((NTP, D), bf16),
        pltpu.VMEM((1, NTP), f32),
        pltpu.VMEM((1, BLK), f32),
        pltpu.VMEM((3, NTP * CH), f32),
        pltpu.VMEM((KEY, VAL), f32),
        pltpu.VMEM((1, KEY), f32),
        pltpu.VMEM((BLK, D), bf16),
        pltpu.VMEM((D, 1408), bf16),
        pltpu.VMEM((2 * VAL, D), bf16),
        pltpu.VMEM((2 * CH, D), bf16),
        pltpu.VMEM((BLK, 1280), bf16),
        pltpu.VMEM((BLK, 128), f32),
        pltpu.VMEM((8, BLK), f32),
        pltpu.VMEM((BLK, 128), f32),
        pltpu.VMEM((TILES, 16, 128), bf16),
        pltpu.VMEM((gmax, tmax, 16, 128), bf16),
        pltpu.VMEM((n_sp, 1, 384), f32),
        pltpu.VMEM((gmax, tmax, 16, 128), bf16),
        pltpu.VMEM((TILES, 16, 128), bf16),
        pltpu.VMEM((gmax, 1, 128), f32),
        pltpu.VMEM((gmax, 1, 128), f32),
        pltpu.VMEM((1, 128), f32),
        pltpu.VMEM((1, 128), f32),
        pltpu.VMEM((tmax, 16, 128), f32),
        pltpu.VMEM((1, 256), f32),
        pltpu.VMEM((tmax, 16, 128), f32),
        pltpu.VMEM((1, 256), f32),
        pltpu.VMEM((KEY, VAL), bf16),
        pltpu.VMEM((BLK, VAL), f32),
        pltpu.VMEM((BLK, 128), f32),
        pltpu.VMEM((BLK, VAL), bf16),
        pltpu.VMEM((BLK, CH), bf16),
        pltpu.VMEM((BLK + 8, CH), f32),
        pltpu.VMEM((16, CH), bf16),
        pltpu.VMEM((16, CH), bf16),
        pltpu.VMEM((NTP, 1, BLK), f32),
        pltpu.VMEM((BLK, 128), f32),
        pltpu.VMEM((BLK, 128), f32),
        pltpu.VMEM((ROWS, D), f32),
        pltpu.VMEM((ROWS, D), f32),
        pltpu.VMEM((2, ROWS, COLS), f32),
        pltpu.VMEM((ROWS, D), bf16),
        *rs_bufs(),
        *rs_bufs(),
        dma((2,)),
        dma((9,)),
        dma(()),
        dma((10,)),
        *[dma(()) for _ in range(8)],
        dma(()),
        dma(()),
        dma(()),
        dma((5,)),
        dma(()),
        dma((5,)),
        dma((2,)),
        dma(()),
        dma((2,)),
        dma(()),
        pltpu.SemaphoreType.REGULAR,
        pltpu.SemaphoreType.REGULAR,
        dma(()),
        dma(()),
        dma((2,)),
    ]

    def per_device(
        tokens, in_gain, w_query, w_key, w_value, w_input_gate, w_forget_gate, forget_bias,
        forget_extra, w_conv_gate, w_conv_left, w_conv_right, conv_taps, first_memory,
        first_norm, w_out_memory, w_out_conv,
    ):
        return pl.pallas_call(
            functools.partial(kernel, n_sp),
            out_shape=jax.ShapeDtypeStruct((ROWS, D), bf16),
            in_specs=[hbm] * 17,
            out_specs=hbm,
            scratch_shapes=scratch,
            compiler_params=pltpu.CompilerParams(
                collective_id=0, has_side_effects=True, vmem_limit_bytes=60 * 1024 * 1024
            ),
        )(
            tokens, in_gain.reshape(1, D), w_input_gate.T, w_forget_gate.T,
            forget_bias.reshape(1, NTP),
            forget_extra.reshape(1, BLK), conv_taps, first_memory.reshape(KEY, VAL), first_norm,
            w_query, w_key, w_value, w_conv_gate, w_conv_left, w_conv_right,
            w_out_memory, w_out_conv,
        )

    placed = (
        P(("sp", "tp"), None),
        P(),
        P(None, "tp"),
        P(None, "tp"),
        P(None, "tp"),
        P(),
        P(),
        P(),
        P("sp", "tp"),
        P(None, "tp"),
        P(None, "tp"),
        P(None, "tp"),
        P(),
        P("tp", None, None),
        P("tp", None),
        P("tp", None),
        P("tp", None),
    )
    return jax.shard_map(
        per_device, mesh=mesh, in_specs=placed, out_specs=P(("sp", "tp"), None), check_vma=False
    )
```

```python
import functools

import jax
import jax.numpy as jnp
from jax import lax
from jax.experimental import pallas as pl
from jax.experimental.pallas import tpu as pltpu
from jax.sharding import PartitionSpec as P

D = 2048
KEY = 128
VAL = 256
CH = 256
ROWS = 96
HALF = 48
BLK = 768
NTP = 8
TILES = 16
COLS = 1024
CUT = 1280
AG_SLOT = (0, 1, 2, 3, 4, 5, 6, 7, 7, 8, 8, 9, 9)
EPS = 1e-06
SCALE = KEY ** (-0.5)
MESH = pl.DeviceIdType.MESH
f32 = jnp.float32
bf16 = jnp.bfloat16


def nt_dot(a, b):
    return lax.dot_general(a, b, (((1,), (1,)), ((), ())), preferred_element_type=f32)


def groups_of(n_sp):
    if n_sp == 32:
        return ((0, 8), (8, 16), (16, 32))
    if n_sp == 4:
        return ((0, 2), (2, 4))
    return ((0, n_sp),)


def dot(a, b):
    return jnp.dot(a, b, preferred_element_type=f32)


def kernel(
    n_sp,
    tok_h, gain_h, wi_h, wf_h, bias_h, fextra_h, taps_h, fmem_h, fnorm_h,
    wq, wk, wv, wcg, wcl, wcr, wom, woc,
    out_h,
    tok, gain, wi, wf, bias, fextra, taps, fmem, fnorm,
    x, w_all, wom_v, woc_v,
    proj, gates, urow, cmcol, st, rv, aux, cv, cr, mh, nh, m_at, n_at,
    ex, ea, px, pa, cmem, pv, rs,
    mob, cbr, prod, eb, er, ss, scol, sqcol, own_c, own_h, part, out,
    x_c, fs_c, fr_c, gs_c, gr_c,
    x_h, fs_h, fr_h, gs_h, gr_h,
    wsem, isem, ag_s, ag_r, aux_s, aux_r, st_s, st_r, cr_s, cr_r, ed_s, ed_r, ss_s, ss_r,
    rc_s, rc_r, rh_s, rh_r, ex_s, px_r, ea_s, pa_r, ready, ready_edge, ow_s, ow_r, out_s,
):
    groups = groups_of(n_sp)
    scope = jax.named_scope
    sp = lax.axis_index("sp")
    me = lax.axis_index("tp")
    y = me // 2
    c = lax.rem(me, 2)
    sib = me + 1 - 2 * c
    yn_y, yp_y, yo_y = lax.rem(y + 1, 4), lax.rem(y + 3, 4), lax.rem(y + 2, 4)
    yn, yp = yn_y * 2 + c, yp_y * 2 + c

    def in_group(g):
        return jnp.logical_and(sp >= groups[g][0], sp < groups[g][1])

    def mates(g, start):
        lo, hi = groups[g]
        n = hi - lo
        for k in range(1, n):
            far = n // 2 + (k // 2 if k % 2 else -(k // 2))
            start(lo + lax.rem(sp - lo + far, n))

    def following(g):
        lo, hi = groups[g]
        if g + 1 == len(groups):
            return []
        at, end = groups[g + 1]
        ratio = (end - at) // (hi - lo)
        return [at + (sp - lo) * ratio + q for q in range(ratio)]

    def preceding(g):
        lo, hi = groups[g]
        at, end = groups[g - 1]
        return at + (sp - lo) // ((hi - lo) // (end - at))

    inputs = [
        pltpu.make_async_copy(src, dst, isem.at[i])
        for i, (src, dst) in enumerate(
            [
                (tok_h, tok), (gain_h, gain), (wi_h, wi), (wf_h, wf), (bias_h, bias),
                (fextra_h, fextra), (taps_h, taps), (fmem_h, fmem), (fnorm_h, fnorm),
            ]
        )
    ]
    weights = [
        pltpu.make_async_copy(src, dst, wsem.at[i // 6])
        for i, (src, dst) in enumerate(
            [
                (wk, w_all.at[:, pl.ds(0, 128)]),
                (wq, w_all.at[:, pl.ds(128, 128)]),
                (wv, w_all.at[:, pl.ds(256, 256)]),
                (wcl, w_all.at[:, pl.ds(512, 256)]),
                (wcr, w_all.at[:, pl.ds(768, 256)]),
                (wcg, w_all.at[:, pl.ds(1024, 256)]),
                (woc, woc_v.at[pl.ds(0, CH), :]),
                (wom, wom_v.at[pl.ds(0, VAL), :]),
            ]
        )
    ]
    for cp in inputs[:4]:
        cp.start()
    barrier = pltpu.get_barrier_semaphore()
    for k in range(1, NTP):
        pl.semaphore_signal(
            barrier, inc=1, device_id=(sp, lax.rem(me + k, NTP)), device_id_type=MESH
        )

    def greet(p):
        pl.semaphore_signal(barrier, inc=1, device_id=(p, me), device_id_type=MESH)

    for g, (lo, hi) in enumerate(groups):

        @pl.when(in_group(g))
        def _(g=g):
            mates(g, greet)
            for p in following(g):
                greet(p)

        if hi < n_sp:

            @pl.when(sp == hi - 1)
            def _():
                greet(sp + 1)

    for cp in inputs[4:]:
        cp.start()
    for w in weights:
        w.start()

    def slots(s, n=1):
        return x.at[pl.ds(pl.multiple_of(s * HALF, 16), n * HALF), :]

    with scope("norm"):
        inputs[0].wait()
        inputs[1].wait()
        t = tok[...].astype(f32)
        scale = lax.rsqrt(jnp.mean(t * t, axis=1, keepdims=True) + EPS)
        x[pl.ds(pl.multiple_of(c * ROWS, 16), ROWS), :] = (t * scale * gain[...]).astype(bf16)
    prod[0:8, :] = jnp.zeros((8, CH), f32)

    with scope("w_barrier"):
        for g, (lo, hi) in enumerate(groups):
            count = NTP - 1 + hi - lo - 1 + (1 if lo else 0)

            @pl.when(jnp.logical_and(in_group(g), jnp.logical_or(sp != lo, lo == 0)))
            def _(count=count):
                pl.semaphore_wait(barrier, count)

            if lo:

                @pl.when(sp == lo)
                def _(count=count):
                    pl.semaphore_wait(barrier, count + 1)

    def send(src, dst, ssem, rsem, peer):
        cp = pltpu.make_async_remote_copy(
            src_ref=src, dst_ref=dst, send_sem=ssem, recv_sem=rsem,
            device_id=(sp, peer), device_id_type=MESH,
        )
        cp.start()

    def got(dst, rsem, name="w"):
        with scope(name):
            pltpu.make_async_remote_copy(
                src_ref=dst, dst_ref=dst, send_sem=rsem, recv_sem=rsem,
                device_id=(sp, sib), device_id_type=MESH,
            ).wait_recv()

    def ag(src, dst, k, peer, n=1):
        send(slots(src, n), slots(dst, n), ag_s, ag_r.at[AG_SLOT[k]], peer)

    other = 1 - c
    ag(2 * c, 4 + c, 0, yn)
    ag(2 * c + 1, 6 + c, 3, yp)
    ag(2 * c + 1, 8 + c, 1, yn)
    ag(2 * c, 10 + c, 4, yp)
    ag(2 * c, 2 * c, 6, sib, 2)
    send(woc, woc_v.at[pl.ds(CH, CH), :], ow_s, ow_r, sib)
    send(wom, wom_v.at[pl.ds(VAL, VAL), :], ow_s, ow_r, sib)
    def tell(sem, p):
        pl.semaphore_signal(sem, inc=1, device_id=(p, me), device_id_type=MESH)

    for g, (lo, hi) in enumerate(groups):
        if lo:

            @pl.when(in_group(g))
            def _(g=g):
                tell(ready, preceding(g))

            @pl.when(sp == lo)
            def _():
                tell(ready_edge, sp - 1)

    for cp in inputs[2:]:
        cp.wait()
    gw = jnp.concatenate(
        [wi[...].astype(f32), wf[...].astype(f32), jnp.zeros((112, D), f32)], axis=0
    )
    w_all[:, 1280:1408] = gw.T.astype(bf16)
    with scope("w_weights"):
        pltpu.make_async_copy(w_all.at[:, 0:1280], w_all.at[:, 0:1280], wsem.at[0]).wait()

    def project_rows(xs, bases, n, parts):
        for lo, hi in parts:
            res = dot(xs, w_all[:, lo:hi])
            for k, base in enumerate(bases):
                rows = pl.ds(pl.multiple_of(base, 16), n)
                piece = res[k * n : (k + 1) * n]
                if lo == 512:
                    left = piece[:, :CH].astype(bf16).astype(f32)
                    right = piece[:, CH:].astype(bf16).astype(f32)
                    at = pl.ds(pl.multiple_of(base + 8, 8), n)
                    prod[at, :] = (left * right).astype(bf16).astype(f32)
                elif hi <= 1280:
                    proj[rows, lo:hi] = piece.astype(bf16)
                else:
                    gates[rows, :] = piece[:, 1280 - lo :]
                    if lo < 1280:
                        proj[rows, lo:1280] = piece[:, : 1280 - lo].astype(bf16)

    def project(stage, bases, parts):
        project_rows(x[stage * 192 : stage * 192 + 192, :], bases, HALF, parts)

    edge = pltpu.make_async_remote_copy(
        src_ref=eb, dst_ref=er, send_sem=ed_s, recv_sem=ed_r,
        device_id=(lax.rem(sp + 1, n_sp), me), device_id_type=MESH,
    )

    def send_edge(where):
        @pl.when(jnp.logical_and(y == where, sp < n_sp - 1))
        def _():
            eb[...] = prod[BLK - 8 :, :].astype(bf16)
            for lo, hi in groups[:-1]:

                @pl.when(sp == hi - 1)
                def _():
                    pl.semaphore_wait(ready_edge, 1)

            edge.start()

    def own(d):
        return pl.ds(pl.multiple_of((d * 2 + c) * ROWS, 16), ROWS)

    def his(d):
        return pl.ds(pl.multiple_of((d * 2 + 1 - c) * ROWS, 16), ROWS)

    order = (yo_y, yn_y, yp_y, y)

    def rs_part(n, a, w, xb, s_, r_, prepare):
        prepare(order[n], other)
        send(a.at[his(order[n])], xb.at[n], s_, r_.at[(0, 5, 1, 1)[n]], sib)
        prepare(order[n], c)

    def both(n, a, xb):
        return jnp.concatenate([a[own(order[n]), :], xb[n]], axis=1)

    def rs_first(cut, a, w, xb, fs, fr, gs, gr, kept, s_, r_):
        got(xb.at[0], r_.at[0], "w_x0")
        lhs = both(0, a, xb)
        for k, (lo, hi, peer) in enumerate(((0, cut, yn), (cut, D, yp))):
            fs[:, lo:hi] = dot(lhs, w[:, lo:hi]).astype(bf16)
            send(fs.at[:, lo:hi], fr.at[:, lo:hi], s_, r_.at[2 + k], peer)

    def rs_early(cut, a, w, xb, fs, fr, gs, gr, kept, s_, r_):
        got(xb.at[1], r_.at[5], "w_x1")
        gs[0, :, cut:] = dot(both(1, a, xb), w[:, cut:]).astype(bf16)
        send(gs.at[0, :, cut:], gr.at[0, :, cut:], s_, r_.at[4], yn)

    def rs_second(early, cut, a, w, xb, fs, fr, gs, gr, kept, s_, r_):
        if not early:
            got(xb.at[1], r_.at[5], "w_x1")
        got(xb.at[pl.ds(2, 2)], r_.at[1], "w_x23")
        low = jnp.concatenate([both(n, a, xb) for n in (2, 3, 1)], axis=0)
        res = dot(low[: 2 * ROWS] if early else low, w[:, cut:])
        if not early:
            gs[0, :, cut:] = res[2 * ROWS :].astype(bf16)
            send(gs.at[0, :, cut:], gr.at[0, :, cut:], s_, r_.at[4], yn)
        part[:, cut:] = res[0:ROWS]
        kept[:, cut:] = res[ROWS : 2 * ROWS]
        res = dot(low, w[:, :cut])
        gs[1, :, :cut] = res[0:ROWS].astype(bf16)
        send(gs.at[1, :, :cut], gr.at[1, :, :cut], s_, r_.at[4], yp)
        kept[:, :cut] = res[ROWS : 2 * ROWS]
        part[:, :cut] = res[2 * ROWS :]

    def rs_mid(cut, a, w, xb, fs, fr, gs, gr, kept, s_, r_):
        for k, (lo, hi, peer) in enumerate(((0, cut, yn), (cut, D, yp))):
            got(fr.at[:, lo:hi], r_.at[2 + k], "w_f")
            gs[k, :, lo:hi] = (part[:, lo:hi] + fr[:, lo:hi].astype(f32)).astype(bf16)
            send(gs.at[k, :, lo:hi], gr.at[k, :, lo:hi], s_, r_.at[4], peer)

    def filtered(d, core):
        @pl.when(jnp.logical_and(jnp.logical_and(d == 0, core == 0), sp > 0))
        def _():
            with scope("w_edge"):
                edge.wait_recv()
            prod[0:8, :] = er[8:16, :].astype(f32)

        at = (d * 2 + core) * ROWS
        rows = pl.ds(pl.multiple_of(at, 16), ROWS)
        mine = pl.ds(pl.multiple_of(me * CH, CH), CH)
        near = prod[pl.ds(pl.multiple_of(at, 16), ROWS + 8), :]
        f = taps[0:1, mine] * near[6 : 6 + ROWS]
        f = f + taps[1:2, mine] * near[7 : 7 + ROWS]
        f = f + taps[2:3, mine] * near[8 : 8 + ROWS]
        cbr[rows, :] = (proj[rows, 1024:1280].astype(f32) * f).astype(bf16)

    conv_set = (CUT, cbr, woc_v, x_c, fs_c, fr_c, gs_c, gr_c, own_c, rc_s, rc_r)
    head_set = (COLS, mob, wom_v, x_h, fs_h, fr_h, gs_h, gr_h, own_h, rh_s, rh_r)

    def conv_part(n):
        rs_part(n, cbr, woc_v, x_c, rc_s, rc_r, filtered)

    every = ((0, 512), (512, 1024), (1024, 1408))
    got(slots(2 * other, 2), ag_r.at[6], "w_ag6")
    with scope("proj_0"):
        project(0, [y * 192 + HALF * k for k in range(4)], every)
        send_edge(3)
    got(slots(4 + c), ag_r.at[0], "w_ag0")
    ag(4 + c, 12 + 2 * c, 2, yn)
    ag(4 + c, 4 + c, 7, sib)
    got(slots(6 + c), ag_r.at[3], "w_ag3")
    ag(6 + c, 13 + 2 * c, 5, yp)
    ag(6 + c, 6 + c, 8, sib)
    got(slots(0, 2), ag_r.at[7], "w_ag7")
    with scope("proj_1"):
        project(
            1,
            [yp_y * 192, yp_y * 192 + ROWS, yn_y * 192 + HALF, yn_y * 192 + ROWS + HALF],
            every,
        )
        send_edge(2)
    got(slots(8 + c), ag_r.at[1], "w_ag1")
    ag(8 + c, 8 + c, 9, sib)
    got(slots(10 + c), ag_r.at[4], "w_ag4")
    ag(10 + c, 10 + c, 10, sib)
    got(slots(0, 2), ag_r.at[8], "w_ag9")
    with scope("proj_2"):
        project(
            2,
            [yp_y * 192 + HALF, yp_y * 192 + ROWS + HALF, yn_y * 192, yn_y * 192 + ROWS],
            every,
        )
        send_edge(0)
    with scope("conv_early"):
        conv_part(1)
    got(slots(12 + 2 * c), ag_r.at[2], "w_ag2")
    ag(12 + 2 * c, 12 + 2 * c, 11, sib)
    got(slots(13 + 2 * c), ag_r.at[5], "w_ag5")
    ag(13 + 2 * c, 13 + 2 * c, 12, sib)
    keys, rest = ((1280, 1408), (0, 512)), ((512, 1024), (1024, 1280))

    def project_last(core, parts):
        xs = x[pl.ds(pl.multiple_of(576 + core * ROWS, 16), ROWS), :]
        project_rows(xs, [yo_y * 192 + core * ROWS], ROWS, parts)

    with scope("proj_3own"):
        project_last(c, keys + rest)
        pltpu.make_async_copy(woc_v, woc_v, wsem.at[1]).wait()
        got(woc_v, ow_r)
        rs_early(*conv_set)
    got(slots(0, 2), ag_r.at[9], "w_ag12")
    with scope("proj_3"):
        project_last(other, keys)

    with scope("state"):
        g_t = gates[...].T
        sub = lax.broadcasted_iota(jnp.int32, (8, BLK), 0)
        lane = lax.broadcasted_iota(jnp.int32, (8, BLK), 1)
        in_row = jnp.sum(jnp.where(sub == me, g_t[0:8], 0.0), axis=0, keepdims=True)
        f_row = jnp.sum(jnp.where(sub == me, g_t[8:16], 0.0), axis=0, keepdims=True)
        lane8 = lax.broadcasted_iota(jnp.int32, (1, NTP), 1)
        f_row = f_row + jnp.sum(jnp.where(lane8 == me, bias[...], 0.0), axis=1, keepdims=True)
        log_forget = (
            jnp.minimum(f_row, 0.0) - jnp.log1p(jnp.exp(-jnp.abs(f_row))) + fextra[...]
        )

        def stacked(row):
            parts = [row[:, 128 * k : 128 * k + 128] for k in range(6)]
            return jnp.concatenate(parts + [jnp.zeros((2, 128), f32)], axis=0)

        lf6 = stacked(log_forget)
        l_1 = lf6.astype(bf16).astype(f32)
        l_2 = (lf6 - l_1).astype(bf16).astype(f32)
        l_3 = lf6 - l_1 - l_2
        upto = lax.broadcasted_iota(jnp.int32, (128, 128), 0) <= lax.broadcasted_iota(
            jnp.int32, (128, 128), 1
        )
        sums = dot(
            jnp.concatenate([l_1, l_2, l_3, jnp.zeros((8, 128), f32)], axis=0).astype(bf16),
            jnp.where(upto, 1.0, 0.0).astype(bf16),
        )
        inside = sums[0:8] + sums[8:16] + sums[16:24]
        sub8 = lax.broadcasted_iota(jnp.int32, (8, 128), 0)
        ends = jnp.broadcast_to(inside[:, 127:128], (8, 128))
        before = jnp.where(sub8 >= 1, pltpu.roll(ends, 1, 0), 0.0)
        for s in (1, 2, 4):
            before = before + jnp.where(sub8 >= s, pltpu.roll(before, s, 0), 0.0)
        cum6 = inside + before
        u6 = jnp.where(sub8 < 6, stacked(in_row) - cum6, -jnp.inf)
        u_max = jnp.max(jnp.max(u6, axis=1, keepdims=True), axis=0, keepdims=True)
        decay = cum6[5:6, 127:128]

        def unstacked(a):
            return jnp.concatenate([a[k : k + 1] for k in range(6)], axis=1)

        u_row = unstacked(u6)
        k_t = proj[:, 0:128].astype(f32).T
        keyed = k_t * jnp.exp(u_row - u_max)
        mem = dot(keyed.astype(bf16), proj[:, 256:512])
        norm_col = jnp.sum(keyed, axis=1, keepdims=True)
        block_norm = jnp.broadcast_to(norm_col, (128, 128)).T[0:1]
        d_lanes = jnp.broadcast_to(decay, (1, 128))
        m_lanes = jnp.broadcast_to(decay + u_max, (1, 128))
        aux[sp] = jnp.concatenate([d_lanes, m_lanes, block_norm], axis=1)
        for p in range(TILES):
            i, j = p // 2, p % 2
            st[p] = mem[16 * i : 16 * i + 16, 128 * j : 128 * j + 128].astype(bf16)

    def start_state(g, p):
        lo, hi = groups[g]
        n = TILES // (hi - lo)
        pltpu.make_async_remote_copy(
            src_ref=st.at[pl.ds((p - lo) * n, n)], dst_ref=rv.at[sp - lo, pl.ds(0, n)],
            send_sem=st_s, recv_sem=st_r, device_id=(p, me), device_id_type=MESH,
        ).start()
        pltpu.make_async_remote_copy(
            src_ref=aux.at[sp], dst_ref=aux.at[sp], send_sem=aux_s, recv_sem=aux_r,
            device_id=(p, me), device_id_type=MESH,
        ).start()

    with scope("send_state"):
        for g, (lo, hi) in enumerate(groups):

            @pl.when(in_group(g))
            def _(g=g, lo=lo, hi=hi):
                mates(g, functools.partial(start_state, g))
                n = TILES // (hi - lo)
                for k in range(n):
                    rv[sp - lo, k] = st[(sp - lo) * n + k]

    with scope("proj_lrg"):
        project_last(other, rest)
        send_edge(1)

    def start_carry(g, p):
        lo, hi = groups[g]
        n = TILES // (hi - lo)
        pltpu.make_async_remote_copy(
            src_ref=cv.at[p - lo, pl.ds(0, n)], dst_ref=cr.at[pl.ds((sp - lo) * n, n)],
            send_sem=cr_s, recv_sem=cr_r, device_id=(p, me), device_id_type=MESH,
        ).start()

    def pass_on(g):
        lo, hi = groups[g]
        out_ = []
        for q, p in enumerate(following(g)):
            n = TILES // (groups[g + 1][1] - groups[g + 1][0])
            out_ += [
                pltpu.make_async_remote_copy(
                    src_ref=ex.at[pl.ds(q * n, n)], dst_ref=px.at[pl.ds(0, n)],
                    send_sem=ex_s.at[q], recv_sem=px_r, device_id=(p, me), device_id_type=MESH,
                ),
                pltpu.make_async_remote_copy(
                    src_ref=ea, dst_ref=pa, send_sem=ea_s.at[q], recv_sem=pa_r,
                    device_id=(p, me), device_id_type=MESH,
                ),
            ]
        return out_

    def recurrence(g):
        lo, hi = groups[g]
        n = TILES // (hi - lo)
        with scope("w_state"):
            if hi - lo > 1:
                got(aux.at[pl.ds(0, hi - lo - 1)], aux_r)
                got(rv.at[pl.ds(0, hi - lo - 1), pl.ds(0, n)], st_r)
        if lo:
            with scope("w_prefix"):
                got(px.at[pl.ds(0, n)], px_r)
                got(pa, pa_r)
            tiles = [px[k] for k in range(n)]
            run_m = pa[:, 0:128]
            run_n = pa[:, 128:256]
        else:
            tiles = []
            for k in range(n):
                p = (sp - lo) * n + k
                r_i = pl.ds(pl.multiple_of((p // 2) * 16, 16), 16)
                c_i = pl.ds(pl.multiple_of(lax.rem(p, 2) * 128, 128), 128)
                tiles.append(fmem[r_i, c_i])
            run_m = jnp.zeros((1, 128), f32)
            run_n = fnorm[...]
        last_one = hi == n_sp
        for b in range(lo, hi):
            for k in range(n):
                cv[b - lo, k] = tiles[k].astype(bf16)
            mh[b - lo] = run_m
            nh[b - lo] = run_n
            if b < hi - 1 or not last_one:
                row = aux[b]
                new_m = jnp.maximum(run_m + row[:, 0:128], row[:, 128:256])
                old = jnp.exp(run_m + row[:, 0:128] - new_m)
                new = jnp.exp(row[:, 128:256] - new_m)
                tiles = [old * tiles[k] + new * rv[b - lo, k].astype(f32) for k in range(n)]
                run_n = old * run_n + new * row[:, 256:384]
                run_m = new_m
        if not last_one:
            for k in range(n):
                ex[k] = tiles[k]
            ea[...] = jnp.concatenate([run_m, run_n], axis=1)
            with scope("w_ready"):
                pl.semaphore_wait(ready, len(following(g)))
            for cp in pass_on(g):
                cp.start()
        with scope("send_carry"):
            mates(g, functools.partial(start_carry, g))
        for k in range(n):
            cr[(sp - lo) * n + k] = cv[sp - lo, k]
        m_at[...] = mh[sp - lo]
        n_at[...] = nh[sp - lo]

    def take(g):
        @pl.when(in_group(g))
        def _():
            recurrence(g)

    with scope("rs_first_conv"):
        conv_part(0)
        conv_part(3)
        top = jnp.broadcast_to(u_row, (8, BLK))
        urow[...] = top
        for s in (1, 2, 4, 8, 16, 32, 64, 128, 256, 512):
            top = jnp.maximum(top, jnp.where(lane >= s, pltpu.roll(top, s, 1), -jnp.inf))
        cols = jnp.concatenate([top, jnp.zeros((120, BLK), f32)], axis=0).T
        cmcol[...] = jnp.broadcast_to(cols[:, 0:1], (BLK, 128))
        rs_first(*conv_set)
    def mixing():
        for rb in range(3):
            r0 = rb * 256
            q = proj[r0 : r0 + 256, 128:256]
            cm = cmcol[r0 : r0 + 256, 0:1]
            acc = jnp.zeros((256, VAL), f32)
            tot = jnp.zeros((256, 1), f32)
            for cb in range(rb + 1):
                c0 = cb * 256
                mix = nt_dot(q, proj[c0 : c0 + 256, 0:128]) * SCALE
                mix = mix * jnp.exp(urow[0:1, c0 : c0 + 256] - cm)
                if cb == rb:
                    ri = lax.broadcasted_iota(jnp.int32, (256, 256), 0)
                    ci = lax.broadcasted_iota(jnp.int32, (256, 256), 1)
                    mix = jnp.where(ri >= ci, mix, 0.0)
                tot = tot + jnp.sum(mix, axis=1, keepdims=True)
                acc = acc + dot(mix.astype(bf16), proj[c0 : c0 + 256, 256:512])
            pv[r0 : r0 + 256, :] = acc
            rs[r0 : r0 + 256, :] = jnp.broadcast_to(tot, (256, 128))

    last_group = in_group(len(groups) - 1)
    for g in range(len(groups) - 1):
        take(g)

    @pl.when(last_group)
    def _():
        with scope("mixing"):
            mixing()

    with scope("rs_second_conv"):
        conv_part(2)
        rs_second(True, *conv_set)

    @pl.when(jnp.logical_not(last_group))
    def _():
        with scope("mixing"):
            mixing()

    take(len(groups) - 1)
    with scope("rs_mid_conv"):
        rs_mid(*conv_set)

    for g, (lo, hi) in enumerate(groups):

        @pl.when(in_group(g))
        def _(lo=lo, hi=hi):
            got(cr.at[pl.ds(0, TILES - TILES // (hi - lo))], cr_r, "w_carry")

    with scope("carry"):
        for p in range(TILES):
            i, j = p // 2, p % 2
            cmem[16 * i : 16 * i + 16, 128 * j : 128 * j + 128] = cr[p]
        carry = cmem[...]
        m_in = m_at[:, 0:1]
        n_in = n_at[...]
        n_1 = n_in.astype(bf16).astype(f32)
        n_2 = (n_in - n_1).astype(bf16).astype(f32)
        n_3 = n_in - n_1 - n_2
        sub16 = lax.broadcasted_iota(jnp.int32, (16, 128), 0)
        n_rows = jnp.where(
            sub16 == 0, n_1, jnp.where(sub16 == 1, n_2, jnp.where(sub16 == 2, n_3, 0.0))
        ).astype(bf16)

    def heads(d, core):
        rows = pl.ds(pl.multiple_of((d * 2 + core) * ROWS, 16), ROWS)
        q = proj[rows, 128:256]
        cm = cmcol[rows, 0:1]
        peak = jnp.maximum(cm, m_in)
        f_in = jnp.exp(cm - peak)
        f_carry = jnp.exp(m_in - peak)
        from_memory = dot(q, carry) * SCALE
        from_norm = jnp.sum(nt_dot(q, n_rows), axis=1, keepdims=True) * SCALE
        num = f_in * pv[rows, :] + f_carry * from_memory
        den = f_in * rs[rows, 0:1] + f_carry * from_norm
        memory_out = num / jnp.maximum(jnp.abs(den), 1.0)
        squares = jnp.sum(memory_out * memory_out, axis=1, keepdims=True)
        sqcol[rows, :] = jnp.broadcast_to(squares, (ROWS, 128))
        mob[rows, :] = memory_out.astype(bf16)

    with scope("rs_first_head"):
        for n in (0, 1):
            rs_part(n, mob, wom_v, x_h, rh_s, rh_r, heads)
        rs_first(*head_set)
    with scope("rs_second_head"):
        for n in (2, 3):
            rs_part(n, mob, wom_v, x_h, rh_s, rh_r, heads)
        rs_second(False, *head_set)
    ss[me] = sqcol[...].T[0:1]
    for k in range(1, NTP):
        send(ss.at[me], ss.at[me], ss_s, ss_r, lax.rem(me + k, NTP))
    with scope("rs_mid_head"):
        rs_mid(*head_set)
    got(ss.at[pl.ds(0, NTP - 1)], ss_r, "w_ss")
    total = ss[0]
    for k in range(1, NTP):
        total = total + ss[k]
    factor = lax.rsqrt(total / (NTP * VAL) + EPS)
    scol[...] = jnp.broadcast_to(factor, (128, BLK)).T
    got(gr_c, rc_r.at[4], "w_gc")
    factor = scol[pl.ds(pl.multiple_of(me * ROWS, 8), ROWS), 0:1]
    for k in range(2):
        cs = slice(k * COLS, (k + 1) * COLS)
        conv_sum = own_c[:, cs] + gr_c[0, :, cs].astype(f32) + gr_c[1, :, cs].astype(f32)
        own_c[:, cs] = conv_sum + factor * own_h[:, cs]
    got(gr_h, rh_r.at[4], "w_gh")
    outs = []
    with scope("final"):
        for k in range(2):
            cs = slice(k * COLS, (k + 1) * COLS)
            rest_sum = gr_h[0, :, cs].astype(f32) + gr_h[1, :, cs].astype(f32)
            out[:, cs] = (own_c[:, cs] + factor * rest_sum).astype(bf16)
            outs.append(pltpu.make_async_copy(out.at[:, cs], out_h.at[:, cs], out_s.at[k]))
            outs[k].start()

    def sent(ref, sem):
        pltpu.make_async_remote_copy(
            src_ref=ref, dst_ref=ref, send_sem=sem, recv_sem=sem,
            device_id=(sp, sib), device_id_type=MESH,
        ).wait_send()

    with scope("w_sends"):
        sent(x.at[pl.ds(0, 14 * HALF), :], ag_s)
        sent(woc_v, ow_s)
        sent(x.at[pl.ds(0, 336), :], rc_s)
        sent(x.at[pl.ds(0, 336), :], rh_s)
        sent(ss.at[pl.ds(0, NTP - 1)], ss_s)

    @pl.when(sp < n_sp - 1)
    def _():
        edge.wait_send()

    for g, (lo, hi) in enumerate(groups):

        @pl.when(in_group(g))
        def _(g=g, lo=lo, hi=hi):
            if hi - lo > 1:
                rest = pl.ds(0, TILES - TILES // (hi - lo))
                sent(st.at[rest], st_s)
                sent(aux.at[pl.ds(0, hi - lo - 1)], aux_s)
                sent(cr.at[rest], cr_s)
            for cp in pass_on(g):
                cp.wait_send()

    with scope("w_out"):
        for cp in outs:
            cp.wait()


def solution(mesh):
    n_sp = mesh.shape["sp"]
    groups = groups_of(n_sp)
    gmax = max(hi - lo for lo, hi in groups)
    tmax = max(TILES // (hi - lo) for lo, hi in groups)
    hbm = pl.BlockSpec(memory_space=pl.ANY)
    dma = pltpu.SemaphoreType.DMA

    def rs_bufs():
        return [
            pltpu.VMEM((4, ROWS, CH), bf16),
            pltpu.VMEM((ROWS, D), bf16),
            pltpu.VMEM((ROWS, D), bf16),
            pltpu.VMEM((2, ROWS, D), bf16),
            pltpu.VMEM((2, ROWS, D), bf16),
        ]

    scratch = [
        pltpu.VMEM((ROWS, D), bf16),
        pltpu.VMEM((1, D), f32),
        pltpu.VMEM((NTP, D), bf16),
        pltpu.VMEM((NTP, D), bf16),
        pltpu.VMEM((1, NTP), f32),
        pltpu.VMEM((1, BLK), f32),
        pltpu.VMEM((3, NTP * CH), f32),
        pltpu.VMEM((KEY, VAL), f32),
        pltpu.VMEM((1, KEY), f32),
        pltpu.VMEM((BLK, D), bf16),
        pltpu.VMEM((D, 1408), bf16),
        pltpu.VMEM((2 * VAL, D), bf16),
        pltpu.VMEM((2 * CH, D), bf16),
        pltpu.VMEM((BLK, 1280), bf16),
        pltpu.VMEM((BLK, 128), f32),
        pltpu.VMEM((8, BLK), f32),
        pltpu.VMEM((BLK, 128), f32),
        pltpu.VMEM((TILES, 16, 128), bf16),
        pltpu.VMEM((gmax, tmax, 16, 128), bf16),
        pltpu.VMEM((n_sp, 1, 384), f32),
        pltpu.VMEM((gmax, tmax, 16, 128), bf16),
        pltpu.VMEM((TILES, 16, 128), bf16),
        pltpu.VMEM((gmax, 1, 128), f32),
        pltpu.VMEM((gmax, 1, 128), f32),
        pltpu.VMEM((1, 128), f32),
        pltpu.VMEM((1, 128), f32),
        pltpu.VMEM((tmax, 16, 128), f32),
        pltpu.VMEM((1, 256), f32),
        pltpu.VMEM((tmax, 16, 128), f32),
        pltpu.VMEM((1, 256), f32),
        pltpu.VMEM((KEY, VAL), bf16),
        pltpu.VMEM((BLK, VAL), f32),
        pltpu.VMEM((BLK, 128), f32),
        pltpu.VMEM((BLK, VAL), bf16),
        pltpu.VMEM((BLK, CH), bf16),
        pltpu.VMEM((BLK + 8, CH), f32),
        pltpu.VMEM((16, CH), bf16),
        pltpu.VMEM((16, CH), bf16),
        pltpu.VMEM((NTP, 1, BLK), f32),
        pltpu.VMEM((BLK, 128), f32),
        pltpu.VMEM((BLK, 128), f32),
        pltpu.VMEM((ROWS, D), f32),
        pltpu.VMEM((ROWS, D), f32),
        pltpu.VMEM((ROWS, D), f32),
        pltpu.VMEM((ROWS, D), bf16),
        *rs_bufs(),
        *rs_bufs(),
        dma((2,)),
        dma((9,)),
        dma(()),
        dma((10,)),
        *[dma(()) for _ in range(8)],
        dma(()),
        dma(()),
        dma(()),
        dma((6,)),
        dma(()),
        dma((6,)),
        dma((2,)),
        dma(()),
        dma((2,)),
        dma(()),
        pltpu.SemaphoreType.REGULAR,
        pltpu.SemaphoreType.REGULAR,
        dma(()),
        dma(()),
        dma((2,)),
    ]

    def per_device(
        tokens, in_gain, w_query, w_key, w_value, w_input_gate, w_forget_gate, forget_bias,
        forget_extra, w_conv_gate, w_conv_left, w_conv_right, conv_taps, first_memory,
        first_norm, w_out_memory, w_out_conv,
    ):
        return pl.pallas_call(
            functools.partial(kernel, n_sp),
            out_shape=jax.ShapeDtypeStruct((ROWS, D), bf16),
            in_specs=[hbm] * 17,
            out_specs=hbm,
            scratch_shapes=scratch,
            compiler_params=pltpu.CompilerParams(
                collective_id=0, has_side_effects=True, vmem_limit_bytes=60 * 1024 * 1024
            ),
        )(
            tokens, in_gain.reshape(1, D), w_input_gate.T, w_forget_gate.T,
            forget_bias.reshape(1, NTP),
            forget_extra.reshape(1, BLK), conv_taps, first_memory.reshape(KEY, VAL), first_norm,
            w_query, w_key, w_value, w_conv_gate, w_conv_left, w_conv_right,
            w_out_memory, w_out_conv,
        )

    placed = (
        P(("sp", "tp"), None),
        P(),
        P(None, "tp"),
        P(None, "tp"),
        P(None, "tp"),
        P(),
        P(),
        P(),
        P("sp", "tp"),
        P(None, "tp"),
        P(None, "tp"),
        P(None, "tp"),
        P(),
        P("tp", None, None),
        P("tp", None),
        P("tp", None),
        P("tp", None),
    )
    return jax.shard_map(
        per_device, mesh=mesh, in_specs=placed, out_specs=P(("sp", "tp"), None), check_vma=False
    )
```
